512 devices in a mesh: ep: 32 (over z, core), tp: 16 (over y, x).
Axes of the slice: x: 4, y: 4, z: 16, core: 2. Of those that a mesh axis runs over, the one named last changes fastest.
Arguments:
- attn_rows: bfloat16 [4096, 2048], P('ep'), may hold values from -6 to 6
- attn_gain: float32 [2048], replicated, may hold values from 0.1 to 1.9
- query_weight: bfloat16 [2048, 1024], P(None, 'tp'), may hold values from -0.125 to 0.125
- key_weight: bfloat16 [2048, 1024], P(None, 'tp'), may hold values from -0.125 to 0.125
- value_weight: bfloat16 [2048, 1024], P(None, 'tp'), may hold values from -0.125 to 0.125
- key_bias: bfloat16 [16, 4096], P('tp', 'ep'), may hold values from -14 to 0
- out_weight: bfloat16 [1024, 2048], P(None, 'tp'), may hold values from -0.75 to 0.75
- expert_rows: bfloat16 [4096, 2048], P('ep'), may hold values from -6 to 6
- expert_gain: float32 [2048], replicated, may hold values from 0.1 to 1.9
- expert_ids: int32 [4096, 2], P('ep'), may hold values from 0 to 31, all different within a row; in each aligned block of 128 rows (0 to 127, 128 to 255, ...) at most 16 rows name the same one
- group_logits: float32 [4096, 4], P('ep'), may hold values from -6 to 6
- pair_logits: float32 [4096, 2], P('ep'), may hold values from -6 to 6
- gate_weight: bfloat16 [32, 2048, 2048], P('ep', None, 'tp'), may hold values from -0.125 to 0.125
- up_weight: bfloat16 [32, 2048, 2048], P('ep', None, 'tp'), may hold values from -0.125 to 0.125
- down_weight: bfloat16 [32, 2048, 2048], P('ep', None, 'tp'), may hold values from -0.125 to 0.125
Outputs:
- mixed: bfloat16 [4096, 2048], P('ep', 'tp')
- expert_out: bfloat16 [4096, 2048], P('ep', 'tp')
The draws below stay inside these ranges and needn't reach their ends.
Inputs may be any that keep to these rules, and one draw needn't show every extreme that they name: `expert_ids`: each row names two different experts; in every aligned block of 128 rows no expert is named more than 16 times.
All inputs are finite; a program needn't handle non-finite values.
Results may differ from the reference program's by a relative error of at most 0.0083.
Values may be sent and summed in bfloat16 or wider, within the bound.
No kernel may reach another device: no remote copies, remote signals or barrier semaphores. Data moves between devices by JAX's collectives and lax.ppermute only.
A program may use at most 64 MiB of HBM per device.

```python
import math
import jax
import jax.numpy as jnp
import numpy as np
from jax import lax

D = 2048
ATTENTION_HEADS = 16
HEAD_DIM = 64
FF = 2048
EXPERTS = 32
GROUPS = 4
GROUP_SIZE = 8
TOK_DEV = 128
MICRO_TOKENS = 4096
CAP = 16
N_EP = 32


def draw_key_bias(key, part):
    parallel_lanes = jax.random.split(jax.random.fold_in(key, 17), 7)
    blocks = MICRO_TOKENS // TOK_DEV
    slow_share = 0.5
    slow = jax.random.uniform(parallel_lanes[0], (ATTENTION_HEADS, 1, 1)) < slow_share
    shift = jax.random.uniform(parallel_lanes[1], (ATTENTION_HEADS, blocks, 1), minval=-0.7, maxval=0.7)
    rough = 0.3 * jax.random.normal(parallel_lanes[2], (ATTENTION_HEADS, blocks, TOK_DEV))
    base = jnp.where(slow, -11.0, -4.2) + shift + rough
    spot = jax.random.randint(parallel_lanes[3], (ATTENTION_HEADS, blocks, 1), 0, TOK_DEV)
    strong = jax.random.uniform(parallel_lanes[4], (ATTENTION_HEADS, blocks, 1), minval=-4.0, maxval=-3.2)
    marked = jnp.arange(TOK_DEV)[None, None, :] == spot
    base = jnp.where(slow & marked, strong, base)
    flattened = base.reshape(ATTENTION_HEADS, MICRO_TOKENS)
    surge_position = jax.random.randint(parallel_lanes[5], (ATTENTION_HEADS, 2), 0, MICRO_TOKENS)
    surge_value = jax.random.uniform(parallel_lanes[6], (ATTENTION_HEADS, 2), minval=-1.4, maxval=-0.2)
    match_count = jnp.arange(MICRO_TOKENS)[None, None, :] == surge_position[:, :, None]
    surge_total_sum = jnp.sum(jnp.where(match_count, surge_value[:, :, None], 0.0), axis=1)
    flattened = jnp.where(jnp.any(match_count, axis=1), surge_total_sum, flattened)
    return jnp.clip(flattened, -14.0, 0.0).astype(jnp.float32).astype(jnp.bfloat16)


def block_levels(key, dims, cuts, least, largest):
    level, own = 1.0, jax.random.fold_in(key, 6)
    for dim, parts in cuts:
        heights = jnp.exp(jax.random.uniform(jax.random.fold_in(own, dim), (parts,), jnp.float32, least / len(cuts), largest / len(cuts)))
        level = level * jnp.repeat(heights, dims[dim] // parts).reshape([-1 if axis == dim else 1 for axis in range(len(dims))])
    return level


def assign_block(rng, own, number, rows, count, top, reach, slope):
    sequence = jax.random.permutation(rng, count)
    packed, common = load_shares(count, rows * top, reach, slope, True), load_shares(count, rows * top, reach, slope, False)
    places = jnp.arange(count)

    def named(lengths, turn):
        used = int((lengths > 0).sum())
        fixed = max(1, used // 4)
        moved = fixed + (places - fixed + turn * (used - fixed)) % max(1, count - fixed)
        return jnp.zeros((count,), jnp.int32).at[sequence[jnp.where(places < fixed, places, moved)]].set(jnp.asarray(lengths, jnp.int32))

    lengths = jnp.where(number % 4 == 0, named(packed, number // 4), named(common, number - number // 4 - 1))
    mixed = jax.random.permutation(jax.random.fold_in(own, 3), count)
    donor, sink = mixed[0:count // 2 * 2:2], mixed[1:count // 2 * 2:2]
    room = jnp.minimum(lengths[donor] - 1, reach - lengths[sink]) // 2
    room = jnp.where((donor == sequence[0]) | (sink == sequence[0]) | (lengths[sink] == 0), 0, jnp.maximum(room, 0))
    moved = jax.random.randint(jax.random.fold_in(own, 4), (count // 2,), 0, 1 << 20) % (room + 1)
    lengths = lengths.at[donor].add(-moved).at[sink].add(moved)
    labels = jnp.searchsorted(jnp.cumsum(lengths), jnp.arange(rows * top), side="right").astype(jnp.int32)
    table = labels.reshape(top, rows).T
    table = table[jax.random.permutation(jax.random.fold_in(own, 1), rows)]
    turn = jax.random.randint(jax.random.fold_in(own, 2), (rows, 1), 0, top)
    return jnp.take_along_axis(table, (jnp.arange(top)[None, :] + turn) % top, axis=1)


def load_shares(count, total, most, skew, full):
    portions = [(1 << 20) // math.isqrt(grade ** skew) + 1 for grade in range(1, count + 1)]
    largest = most if full else min(most, max(-(-total // count), total * portions[0] // sum(portions)))
    least = 1 if total - largest >= count - 1 else 0
    holding, spare = [largest] + [least] * (count - 1), total - largest - least * (count - 1)
    while spare > 0:
        free = [i for i in range(1, count) if holding[i] < largest] or [i for i in range(1, count) if holding[i] < most]
        whole, remaining = sum([portions[i] for i in free]), spare
        for i in free:
            addition = min(most - holding[i], max(1, remaining * portions[i] // whole), spare)
            holding[i] = holding[i] + addition
            spare = spare - addition
    return np.array(holding)


def gaussian(rng, extent, deviation, most, cuts=(), kind=jnp.bfloat16):
    values = deviation * jax.random.normal(rng, extent, jnp.float32)
    if cuts:
        values = values * block_levels(rng, extent, cuts, -0.22, 0.18)
    return jnp.clip(values, -most, most).astype(kind)


def setup_inputs(seed: int = 0) -> dict:
    arg_keys = jax.random.split(jax.random.key(seed), 16)
    attn_rows = gaussian(arg_keys[0], (MICRO_TOKENS, D), 1.0, 6.0, ((0, 32),))
    attn_gain = jnp.clip(1.0 + 0.18 * jax.random.normal(arg_keys[1], (D,), jnp.float32), 0.1, 1.9)
    query_weight = gaussian(arg_keys[2], (D, ATTENTION_HEADS * HEAD_DIM), D ** -0.5, 0.125, ((1, 16),))
    key_weight = gaussian(arg_keys[3], (D, ATTENTION_HEADS * HEAD_DIM), D ** -0.5, 0.125, ((1, 16),))
    value_weight = gaussian(arg_keys[4], (D, ATTENTION_HEADS * HEAD_DIM), D ** -0.5, 0.125, ((1, 16),))
    key_bias = draw_key_bias(jax.random.fold_in(arg_keys[15], 71), 0)
    out_weight = gaussian(arg_keys[6], (ATTENTION_HEADS * HEAD_DIM, D), (ATTENTION_HEADS * HEAD_DIM // 16) ** -0.5, 0.75, ((1, 16),))
    expert_rows = gaussian(arg_keys[7], (MICRO_TOKENS, D), 1.0, 6.0, ((0, 32),))
    expert_gain = jnp.clip(1.0 + 0.18 * jax.random.normal(arg_keys[8], (D,), jnp.float32), 0.1, 1.9)
    expert_ids_keys = jax.random.split(jax.random.fold_in(arg_keys[9], 1), MICRO_TOKENS // TOK_DEV)
    expert_ids_turns = jax.random.permutation(jax.random.fold_in(arg_keys[9], 3), MICRO_TOKENS // TOK_DEV)
    expert_ids = jax.vmap(lambda own, number: assign_block(jax.random.fold_in(arg_keys[9], 2), own, number, TOK_DEV, EXPERTS, 2, CAP, 2))(expert_ids_keys, expert_ids_turns).reshape((MICRO_TOKENS, 2))
    group_logits = gaussian(arg_keys[10], (MICRO_TOKENS, GROUPS), 1.5, 6.0, ((0, 32),), jnp.float32)
    pair_logits = gaussian(arg_keys[11], (MICRO_TOKENS, 2), 1.5, 6.0, ((0, 32),), jnp.float32)
    gate_weight = gaussian(arg_keys[12], (EXPERTS, D, FF), D ** -0.5, 0.125, ((0, 32), (2, 16)))
    up_weight = gaussian(arg_keys[13], (EXPERTS, D, FF), D ** -0.5, 0.125, ((0, 32), (2, 16)))
    down_weight = gaussian(arg_keys[14], (EXPERTS, FF, D), FF ** -0.5, 0.125, ((0, 32), (2, 16)))
    return {"attn_rows": attn_rows, "attn_gain": attn_gain, "query_weight": query_weight, "key_weight": key_weight, "value_weight": value_weight, "key_bias": key_bias, "out_weight": out_weight, "expert_rows": expert_rows, "expert_gain": expert_gain, "expert_ids": expert_ids, "group_logits": group_logits, "pair_logits": pair_logits, "gate_weight": gate_weight, "up_weight": up_weight, "down_weight": down_weight}


epsilon = 1e-06

def norm_rows(rows, gain):
    values = rows.astype(jnp.float32)
    scaled = values * lax.rsqrt(lax.optimization_barrier(jnp.mean(values * values, axis=-1, keepdims=True)) + epsilon)
    return (scaled * gain.astype(jnp.float32)).astype(jnp.bfloat16)

def attention_part(attn_rows, attn_gain, query_weight, key_weight, value_weight, key_bias, out_weight):
    normed = norm_rows(attn_rows, attn_gain)
    queries = jnp.dot(normed, query_weight, preferred_element_type=jnp.float32).astype(jnp.bfloat16)
    keys = jnp.dot(normed, key_weight, preferred_element_type=jnp.float32).astype(jnp.bfloat16)
    values = jnp.dot(normed, value_weight, preferred_element_type=jnp.float32).astype(jnp.bfloat16)
    q_blocks = queries.reshape(N_EP, TOK_DEV, ATTENTION_HEADS, HEAD_DIM).astype(jnp.float32)
    k_blocks = keys.reshape(N_EP, TOK_DEV, ATTENTION_HEADS, HEAD_DIM).astype(jnp.float32)
    v_blocks = values.reshape(N_EP, TOK_DEV, ATTENTION_HEADS, HEAD_DIM).astype(jnp.float32)
    bias_blocks = key_bias.astype(jnp.float32).reshape(ATTENTION_HEADS, N_EP, TOK_DEV)
    scale = HEAD_DIM ** (-0.5)
    local = jnp.arange(TOK_DEV, dtype=jnp.int32)

    def query_block(index):
        query = q_blocks[index]
        query_pos = index * TOK_DEV + local

        def key_block(carry, other):
            key_part = k_blocks[other]
            scores = jnp.einsum('thd,shd->hts', query, key_part) * scale + bias_blocks[:, other][:, None, :]
            causal = (other * TOK_DEV + local)[None, :] < query_pos[:, None]
            log_keep = jnp.where(causal, jax.nn.log_sigmoid(-scores), 0.0)
            suffix = lax.cumsum(log_keep, axis=2, reverse=True) - log_keep
            weights = jnp.where(causal, jnp.exp(jax.nn.log_sigmoid(scores) + suffix), 0.0).astype(jnp.bfloat16)
            block_out = jnp.einsum('hts,shd->htd', weights.astype(jnp.float32), v_blocks[other])
            return (carry, (lax.optimization_barrier(jnp.sum(log_keep, axis=2)), block_out))
        _, (totals, outputs) = lax.scan(key_block, jnp.zeros((), jnp.float32), jnp.arange(N_EP, dtype=jnp.int32))
        later = lax.cumsum(totals, axis=0, reverse=True) - totals
        merged = lax.optimization_barrier(jnp.sum(jnp.exp(later)[..., None] * outputs, axis=0))
        return jnp.transpose(merged, (1, 0, 2)).reshape(TOK_DEV, ATTENTION_HEADS * HEAD_DIM)
    attended = lax.map(query_block, jnp.arange(N_EP, dtype=jnp.int32))
    attended = attended.reshape(MICRO_TOKENS, ATTENTION_HEADS * HEAD_DIM).astype(jnp.bfloat16)
    return jnp.dot(attended, out_weight, preferred_element_type=jnp.float32).astype(jnp.bfloat16)

def route_shares(expert_ids, group_logits, pair_logits):
    shares = jnp.exp(group_logits)
    shares = shares / lax.optimization_barrier(jnp.sum(shares, axis=1, keepdims=True))
    groups = expert_ids // GROUP_SIZE
    marks = (groups[:, :, None] == jnp.arange(GROUPS, dtype=jnp.int32)[None, None, :]).astype(jnp.float32)
    chosen = lax.optimization_barrier(jnp.sum(shares[:, None, :] * marks, axis=2))
    spread = pair_logits[:, 0] - pair_logits[:, 1]
    pair_share = jnp.stack([jax.nn.sigmoid(spread), jax.nn.sigmoid(-spread)], axis=1)
    return chosen * pair_share

def expert_part(expert_rows, expert_gain, expert_ids, group_logits, pair_logits, gate_weight, up_weight, down_weight):
    normed = norm_rows(expert_rows, expert_gain)
    route_weights = route_shares(expert_ids, group_logits, pair_logits)
    flattened = expert_ids.astype(jnp.int32).reshape(N_EP, TOK_DEV * 2)
    marks = (flattened[:, :, None] == jnp.arange(EXPERTS, dtype=jnp.int32)[None, None, :]).astype(jnp.int32)
    position = lax.optimization_barrier(jnp.sum((jnp.cumsum(marks, axis=1) - marks) * marks, axis=2)).astype(jnp.int32)
    source = jnp.broadcast_to(jnp.arange(N_EP, dtype=jnp.int32)[:, None], flattened.shape)
    row_index = (jnp.arange(MICRO_TOKENS * 2, dtype=jnp.int32) // 2).astype(jnp.int32)
    flat_ids = flattened.reshape(-1)
    flat_src = source.reshape(-1)
    flat_pos = position.reshape(-1)
    buffer = jnp.zeros((EXPERTS, N_EP, CAP, D), jnp.bfloat16).at[flat_ids, flat_src, flat_pos].set(normed[row_index])

    def one_expert(args):
        rows, gate_w, up_w, down_w = args
        rows = rows.reshape(N_EP * CAP, D)
        gate = jnp.dot(rows, gate_w, preferred_element_type=jnp.float32)
        up = jnp.dot(rows, up_w, preferred_element_type=jnp.float32)
        hidden = (jax.nn.silu(gate) * up).astype(jnp.bfloat16)
        return jnp.dot(hidden, down_w, preferred_element_type=jnp.float32).astype(jnp.bfloat16)
    results = lax.map(one_expert, (buffer, gate_weight, up_weight, down_weight))
    picked = results[flat_ids, (flat_src * CAP + flat_pos).astype(jnp.int32)].reshape(MICRO_TOKENS, 2, D)
    combined = lax.optimization_barrier(jnp.sum(route_weights[:, :, None] * picked.astype(jnp.float32), axis=1))
    return combined.astype(jnp.bfloat16)

def reference(attn_rows, attn_gain, query_weight, key_weight, value_weight, key_bias, out_weight, expert_rows, expert_gain, expert_ids, group_logits, pair_logits, gate_weight, up_weight, down_weight):
    mixed = attention_part(attn_rows, attn_gain, query_weight, key_weight, value_weight, key_bias, out_weight)
    expert_out = expert_part(expert_rows, expert_gain, expert_ids, group_logits, pair_logits, gate_weight, up_weight, down_weight)
    return (mixed, expert_out)
```

```python
import jax
import jax.numpy as jnp
from jax import lax
from jax.experimental import pallas as pl
from jax.experimental.pallas import tpu as pltpu
from jax.sharding import PartitionSpec as P


EXPERTS = 32
GROUPS = 4
GROUP_SIZE = 8
CAP = 16
BLOCK = 128
HEAD = 64
SLOTS = EXPERTS * CAP
MSG = 144

epsilon = 1e-06
f32 = jnp.float32
bf16 = jnp.bfloat16
i32 = jnp.int32

SMEM = pl.BlockSpec(memory_space=pltpu.SMEM)


def call(body, n_scalar, n_in, outs, flops, mib=16):
    return pl.pallas_call(
        body,
        out_shape=outs,
        in_specs=[SMEM] * n_scalar + [pl.BlockSpec()] * n_in,
        cost_estimate=pl.CostEstimate(flops=flops, bytes_accessed=1 << 20, transcendentals=0),
        compiler_params=pltpu.CompilerParams(vmem_limit_bytes=mib << 20),
    )


def nn(a, b):
    return lax.dot_general(a, b, (((1,), (0,)), ((), ())), preferred_element_type=f32)


def nt(a, b):
    return lax.dot_general(a, b, (((1,), (1,)), ((), ())), preferred_element_type=f32)


def iota(shape, dim):
    return lax.broadcasted_iota(i32, shape, dim)


def ones_where(mask):
    return jnp.where(mask, 1.0, 0.0).astype(f32)


def places(first, second):
    expert = iota((EXPERTS, BLOCK), 0)
    mark0 = ones_where(first == expert)
    mark1 = ones_where(second == expert)
    earlier = ones_where(iota((BLOCK, BLOCK), 0) < iota((BLOCK, BLOCK), 1)).astype(bf16)
    before = nn((mark0 + mark1).astype(bf16), earlier)
    place0 = jnp.sum(mark0 * before, axis=0, keepdims=True)
    place1 = jnp.sum(mark1 * before, axis=0, keepdims=True)
    return place0.astype(i32), place1.astype(i32)


def dispatch_body(tp_ref, rows_ref, gain_ref, ids_ref, out_ref):
    x = rows_ref[...].astype(f32)
    inv = lax.rsqrt(jnp.mean(x * x, axis=-1, keepdims=True) + epsilon)
    at = pl.multiple_of(tp_ref[0] * BLOCK, BLOCK)
    own = rows_ref[:, pl.ds(at, BLOCK)].astype(f32)
    own = (own * inv * gain_ref[:, pl.ds(at, BLOCK)]).astype(bf16)
    ids = ids_ref[...]
    first, second = ids[0:1, :], ids[1:2, :]
    place0, place1 = places(first, second)
    slot = iota((SLOTS, BLOCK), 0)
    hit = (slot == first * CAP + place0) | (slot == second * CAP + place1)
    out_ref[...] = nn(ones_where(hit).astype(bf16), own).astype(bf16)


def project_body(rows_ref, gain_ref, wq_ref, wk_ref, wv_ref, bias_ref, q_ref, msg_ref):
    x = rows_ref[...].astype(f32)
    inv = lax.rsqrt(jnp.mean(x * x, axis=-1, keepdims=True) + epsilon)
    normed = (x * inv * gain_ref[...]).astype(bf16)
    q = nt(normed, wq_ref[...]).astype(bf16)
    q_ref[...] = (q.astype(f32) * (HEAD**-0.5)).astype(bf16)
    kv = jnp.concatenate([wk_ref[...], wv_ref[...]], axis=0)
    msg_ref[0:BLOCK, :] = nt(kv, normed).astype(bf16)
    msg_ref[BLOCK:MSG, :] = jnp.broadcast_to(bias_ref[...], (MSG - BLOCK, BLOCK))


def copies_body(x_ref, out_ref):
    x = x_ref[...]
    for k in range(out_ref.shape[0]):
        out_ref[k] = x


def hidden_body(x_ref, gate_ref, up_ref, out_ref):
    parts = x_ref.shape[0]
    weights = jnp.concatenate([gate_ref[...], up_ref[...]], axis=1)
    rows = 256
    for m in range(SLOTS // rows):
        span = slice(m * rows, (m + 1) * rows)
        x = jnp.concatenate([x_ref[k, span, :] for k in range(parts)], axis=1)
        both = nn(x, weights)
        gate, up = both[:, :BLOCK], both[:, BLOCK:]
        hidden = (gate * jax.nn.sigmoid(gate) * up).astype(bf16)
        for k in range(parts):
            out_ref[k, span, :] = hidden


def down_body(x_ref, w_ref, out_ref):
    parts = x_ref.shape[0]
    rows = 256
    for m in range(SLOTS // rows):
        span = slice(m * rows, (m + 1) * rows)
        x = jnp.concatenate([x_ref[k, span, :] for k in range(parts)], axis=1)
        out_ref[span, :] = nn(x, w_ref[...]).astype(bf16)


def attend_body(pos_ref, q_ref, own_ref, other_ref, out_ref):
    here = pos_ref[0]
    core = here % 2
    chips = own_ref.shape[0] // MSG
    q = q_ref[...]
    wide = (2 * BLOCK, 2 * BLOCK)
    row, col = iota(wide, 0), iota(wide, 1)
    row = jnp.where(row >= BLOCK, row - BLOCK, row)
    tail = ones_where((col >= BLOCK) | (row >= col)).astype(bf16)
    t, s = iota((BLOCK, BLOCK), 0), iota((BLOCK, BLOCK), 1)

    def block(msg, number, later, total):
        scores = nn(q, msg[0:HEAD, :]) + msg[BLOCK : BLOCK + 1, :].astype(f32)
        causal = s + (number - here) * BLOCK < t
        keep = -(jnp.maximum(scores, 0.0) + jnp.log1p(jnp.exp(-jnp.abs(scores))))
        keep = jnp.where(causal, keep, 0.0)
        high = keep.astype(bf16)
        low = (keep - high.astype(f32)).astype(bf16)
        sums = nn(jnp.concatenate([high, low], axis=1), tail)
        weights = jnp.where(causal, jnp.exp(scores + sums[:, :BLOCK]), 0.0).astype(bf16)
        out = nt(weights, msg[HEAD:BLOCK, :])
        total = total + jnp.exp(later) * out
        return later + sums[:, BLOCK : BLOCK + HEAD], total

    def chip(k, carry):
        later, total = carry
        z = chips - 1 - k
        at = pl.multiple_of(z * MSG, MSG)
        own = own_ref[pl.ds(at, MSG), :]
        other = other_ref[pl.ds(at, MSG), :]
        upper = jnp.where(core == 1, own, other)
        lower = jnp.where(core == 1, other, own)
        later, total = block(upper, 2 * z + 1, later, total)
        return block(lower, 2 * z, later, total)

    zeros = jnp.zeros((BLOCK, HEAD), f32)
    _, total = lax.fori_loop(0, chips, chip, (zeros, zeros), unroll=2)
    out_ref[...] = jnp.transpose(total).astype(bf16)


def mix_body(x_ref, w_ref, out_ref):
    x = jnp.transpose(x_ref[...].astype(f32)).astype(bf16)
    out_ref[...] = nn(x, w_ref[...]).astype(bf16)


def combine_body(ids_ref, group_ref, pair_ref, back_ref, out_ref):
    ids = ids_ref[...]
    first, second = ids[0:1, :], ids[1:2, :]
    place0, place1 = places(first, second)
    shares = jnp.exp(group_ref[...])
    shares = shares / jnp.sum(shares, axis=0, keepdims=True)
    group = iota((GROUPS, BLOCK), 0)
    chosen0 = jnp.sum(jnp.where(first // GROUP_SIZE == group, shares, 0.0), axis=0, keepdims=True)
    chosen1 = jnp.sum(jnp.where(second // GROUP_SIZE == group, shares, 0.0), axis=0, keepdims=True)
    spread = pair_ref[0:1, :] - pair_ref[1:2, :]
    weight0 = chosen0 * jax.nn.sigmoid(spread)
    weight1 = chosen1 * jax.nn.sigmoid(-spread)
    slots = [(first * CAP + place0).astype(f32), (second * CAP + place1).astype(f32)]
    table = jnp.concatenate(slots + [weight0, weight1], axis=0)
    table = jnp.concatenate([table, jnp.zeros((BLOCK - 4, BLOCK), f32)], axis=0)
    table = jnp.transpose(table)
    slot = iota((BLOCK, SLOTS), 1)
    back = back_ref[...]
    pick0 = nn(ones_where(slot == table[:, 0:1].astype(i32)).astype(bf16), back)
    pick1 = nn(ones_where(slot == table[:, 1:2].astype(i32)).astype(bf16), back)
    out_ref[...] = (table[:, 2:3] * pick0 + table[:, 3:4] * pick1).astype(bf16)


def shards(
    attn_rows,
    attn_gain,
    query_weight,
    key_weight,
    value_weight,
    key_bias,
    out_weight,
    expert_rows,
    expert_gain,
    expert_ids,
    group_logits,
    pair_logits,
    gate_weight,
    up_weight,
    down_weight,
):
    ep, tp = lax.axis_size("ep"), lax.axis_size("tp")
    chips = ep // 2
    here = lax.axis_index("ep")
    same_core = [[z * 2 + c for z in range(chips)] for c in range(2)]
    partner = [(e, e ^ 1) for e in range(ep)]
    struct = jax.ShapeDtypeStruct

    def exchange(x, axis):
        return lax.all_to_all(x, axis, split_axis=0, concat_axis=0, tiled=True)

    slots = struct((SLOTS, BLOCK), bf16)
    copies = struct((tp, SLOTS, BLOCK), bf16)
    square = struct((BLOCK, BLOCK), bf16)
    ids = expert_ids.T
    column = lax.axis_index("tp").reshape(1)
    send = call(dispatch_body, 1, 3, slots, 1 << 27)(
        column, expert_rows, expert_gain[None, :], ids
    )
    routed = exchange(send.reshape(ep, CAP, BLOCK), "ep").reshape(SLOTS, BLOCK)
    outs = (struct((BLOCK, HEAD), bf16), struct((MSG, BLOCK), bf16))
    query, message = call(project_body, 0, 6, outs, 1 << 28)(
        attn_rows,
        attn_gain[None, :],
        query_weight.T,
        key_weight.T,
        value_weight.T,
        key_bias,
    )
    routed = call(copies_body, 0, 1, copies, 1 << 24)(routed)
    routed = exchange(routed, "tp")
    own = lax.all_gather(message, "ep", axis=0, tiled=True, axis_index_groups=same_core)
    other = lax.ppermute(own, "ep", partner)
    hidden = call(hidden_body, 0, 3, copies, 1 << 29)(routed, gate_weight[0], up_weight[0])
    hidden = exchange(hidden, "tp")
    attended = call(attend_body, 1, 3, struct((HEAD, BLOCK), bf16), 1 << 30)(
        here.reshape(1), query, own, other
    )
    result = call(down_body, 0, 2, slots, 1 << 28)(hidden, down_weight[0])
    back = exchange(result.reshape(ep, CAP, BLOCK), "ep").reshape(SLOTS, BLOCK)
    attended = lax.all_gather(attended, "tp", axis=0, tiled=True)
    mixed = call(mix_body, 0, 2, square, 1 << 26)(attended, out_weight)
    expert_out = call(combine_body, 0, 4, square, 1 << 27)(
        ids, group_logits.T, pair_logits.T, back
    )
    return (mixed, expert_out)


def solution(mesh):
    placed = (
        P("ep", None),
        P(),
        P(None, "tp"),
        P(None, "tp"),
        P(None, "tp"),
        P("tp", "ep"),
        P(None, "tp"),
        P("ep", None),
        P(),
        P("ep", None),
        P("ep", None),
        P("ep", None),
        P("ep", None, "tp"),
        P("ep", None, "tp"),
        P("ep", None, "tp"),
    )
    return jax.shard_map(
        shards,
        mesh=mesh,
        in_specs=placed,
        out_specs=(P("ep", "tp"), P("ep", "tp")),
        check_vma=False,
    )
```

```python
import jax
import jax.numpy as jnp
from jax import lax
from jax.experimental import pallas as pl
from jax.experimental.pallas import tpu as pltpu
from jax.sharding import PartitionSpec as P


EXPERTS = 32
GROUPS = 4
GROUP_SIZE = 8
CAP = 16
BLOCK = 128
HEAD = 64
SLOTS = EXPERTS * CAP
ROWS = SLOTS // 2
MSG = 144
BEHIND = 4

epsilon = 1e-06
f32 = jnp.float32
bf16 = jnp.bfloat16
i32 = jnp.int32

SMEM = pl.BlockSpec(memory_space=pltpu.SMEM)


def call(body, n_scalar, n_in, outs, flops, mib=16, hbm=(), **more):
    def run(*args):
        args = [
            pltpu.with_memory_space_constraint(a, pltpu.HBM) if k in hbm else a
            for k, a in enumerate(args)
        ]
        return kernel(*args)

    kernel = pl.pallas_call(
        body,
        out_shape=outs,
        in_specs=[SMEM] * n_scalar + [pl.BlockSpec()] * n_in,
        cost_estimate=pl.CostEstimate(flops=flops, bytes_accessed=1 << 20, transcendentals=0),
        compiler_params=pltpu.CompilerParams(vmem_limit_bytes=mib << 20),
        **more,
    )
    return run


def call_out(body, n_scalar, n_in, out, flops, scratch):
    copies = [pltpu.SemaphoreType.DMA((out.shape[0],))]
    more = {"out_specs": pl.BlockSpec(memory_space=pltpu.HBM), "scratch_shapes": scratch + copies}
    return call(body, n_scalar, n_in, out, flops, **more)


def packed(*pieces):
    def body(*refs):
        at = 0
        for ref in refs[:-1]:
            refs[-1][at : at + ref.shape[0], :] = ref[...]
            at += ref.shape[0]

    rows = sum(p.shape[0] for p in pieces)
    out = jax.ShapeDtypeStruct((rows, BLOCK), bf16)
    return call(body, 0, len(pieces), out, 1 << 22)(*pieces)


def nn(a, b):
    return lax.dot_general(a, b, (((1,), (0,)), ((), ())), preferred_element_type=f32)


def nt(a, b):
    return lax.dot_general(a, b, (((1,), (1,)), ((), ())), preferred_element_type=f32)


def iota(shape, dim):
    return lax.broadcasted_iota(i32, shape, dim)


def ones_where(mask):
    return jnp.where(mask, 1.0, 0.0).astype(f32)


def places(first, second):
    expert = iota((EXPERTS, BLOCK), 0)
    mark0 = ones_where(first == expert)
    mark1 = ones_where(second == expert)
    earlier = ones_where(iota((BLOCK, BLOCK), 0) < iota((BLOCK, BLOCK), 1)).astype(bf16)
    before = nn((mark0 + mark1).astype(bf16), earlier)
    place0 = jnp.sum(mark0 * before, axis=0, keepdims=True)
    place1 = jnp.sum(mark1 * before, axis=0, keepdims=True)
    return place0.astype(i32), place1.astype(i32)


def packed_seven(behind, middle, ahead):
    def body(behind_ref, middle_ref, ahead_ref, out_ref):
        out_ref[0 : 2 * MSG, :] = behind_ref[MSG:, :]
        out_ref[2 * MSG : 5 * MSG, :] = middle_ref[...]
        out_ref[5 * MSG :, :] = ahead_ref[: 2 * MSG, :]

    out = jax.ShapeDtypeStruct((7 * MSG, BLOCK), bf16)
    return call(body, 0, 3, out, 1 << 22)(behind, middle, ahead)


def dispatch_body(tp_ref, rows_ref, gain_ref, ids_ref, out_ref):
    x = rows_ref[...].astype(f32)
    inv = lax.rsqrt(jnp.mean(x * x, axis=-1, keepdims=True) + epsilon)
    at = pl.multiple_of(tp_ref[0] * BLOCK, BLOCK)
    own = rows_ref[:, pl.ds(at, BLOCK)].astype(f32)
    own = (own * inv * gain_ref[:, pl.ds(at, BLOCK)]).astype(bf16)
    ids = ids_ref[...]
    first, second = ids[0:1, :], ids[1:2, :]
    place0, place1 = places(first, second)
    slot = iota((SLOTS, BLOCK), 0)
    hit = (slot == first * CAP + place0) | (slot == second * CAP + place1)
    out_ref[...] = nn(ones_where(hit).astype(bf16), own).astype(bf16)


def project_body(rows_ref, gain_ref, wq_ref, wk_ref, wv_ref, bias_ref, q_ref, msg_ref):
    x = rows_ref[...].astype(f32)
    inv = lax.rsqrt(jnp.mean(x * x, axis=-1, keepdims=True) + epsilon)
    normed = (x * inv * gain_ref[...]).astype(bf16)
    q = nt(normed, wq_ref[...]).astype(bf16)
    q_ref[...] = (q.astype(f32) * (HEAD**-0.5)).astype(bf16)
    kv = jnp.concatenate([wk_ref[...], wv_ref[...]], axis=0)
    msg_ref[0:BLOCK, :] = nt(kv, normed).astype(bf16)
    msg_ref[BLOCK:MSG, :] = jnp.broadcast_to(bias_ref[...], (MSG - BLOCK, BLOCK))


def halves_body(x_ref, out_ref, sems):
    copies = []
    for k in range(out_ref.shape[0]):
        half = k % 2
        source = x_ref.at[half * ROWS : (half + 1) * ROWS, :]
        copies.append(pltpu.make_async_copy(source, out_ref.at[k], sems.at[k]))
        copies[-1].start()
    for copy in copies:
        copy.wait()


def hidden_body(tp_ref, x_ref, gate_ref, up_ref, other_ref, out_ref, hidden_ref, sems):
    parts = x_ref.shape[0]
    even = tp_ref[0] % 2 == 0
    depth = gate_ref.shape[0]
    x = jnp.concatenate([x_ref[k] for k in range(parts)], axis=1)
    own = nn(x, jnp.concatenate([gate_ref[...], up_ref[...]], axis=1))
    other = nn(x, jnp.concatenate([other_ref[:depth, :], other_ref[depth:, :]], axis=1))

    def gated(both):
        gate, up = both[:, :BLOCK], both[:, BLOCK:]
        return (gate * jax.nn.sigmoid(gate) * up).astype(bf16).astype(f32)

    own, other = gated(own), gated(other)
    first = jnp.where(even, own, other).astype(bf16)
    second = jnp.where(even, other, own).astype(bf16)
    hidden_ref[0:ROWS, :] = first
    hidden_ref[ROWS:SLOTS, :] = second
    copies = [pltpu.make_async_copy(hidden_ref, out_ref.at[k], sems.at[k]) for k in range(parts)]
    for copy in copies:
        copy.start()
    for copy in copies:
        copy.wait()


def down_body(x_ref, w_ref, out_ref):
    parts = x_ref.shape[0]
    for half in range(2):
        x = jnp.concatenate(
            [
                x_ref[k, e * ROWS : (e + 1) * ROWS, :]
                for k in range(half, parts, 2)
                for e in range(2)
            ],
            axis=1,
        )
        out_ref[half * ROWS : (half + 1) * ROWS, :] = nn(x, w_ref[...]).astype(bf16)


def attend_body(pos_ref, q_ref, own_ref, other_ref, out_ref):
    here = pos_ref[0]
    core = here % 2
    chip_here = here // 2
    chips = own_ref.shape[0] // MSG
    q = q_ref[...]
    wide = (2 * BLOCK, 2 * BLOCK)
    row, col = iota(wide, 0), iota(wide, 1)
    row = jnp.where(row >= BLOCK, row - BLOCK, row)
    tail = ones_where((col >= BLOCK) | (row >= col)).astype(bf16)
    t, s = iota((BLOCK, BLOCK), 0), iota((BLOCK, BLOCK), 1)

    def block(msg, number, later, total):
        scores = nn(q, msg[0:HEAD, :]) + msg[BLOCK : BLOCK + 1, :].astype(f32)
        causal = s + (number - here) * BLOCK < t
        keep = -(jnp.maximum(scores, 0.0) + jnp.log1p(jnp.exp(-jnp.abs(scores))))
        keep = jnp.where(causal, keep, 0.0)
        high = keep.astype(bf16)
        low = (keep - high.astype(f32)).astype(bf16)
        sums = nn(jnp.concatenate([high, low], axis=1), tail)
        weights = jnp.where(causal, jnp.exp(scores + sums[:, :BLOCK]), 0.0).astype(bf16)
        out = nt(weights, msg[HEAD:BLOCK, :])
        total = total + jnp.exp(later) * out
        return later + sums[:, BLOCK : BLOCK + HEAD], total

    def chip(k, carry):
        later, total = carry
        z = chips - 1 - k
        at = pl.multiple_of(((z - chip_here + BEHIND + chips) % chips) * MSG, 16)
        own = own_ref[pl.ds(at, MSG), :]
        other = other_ref[pl.ds(at, MSG), :]
        upper = jnp.where(core == 1, own, other)
        lower = jnp.where(core == 1, other, own)
        later, total = block(upper, 2 * z + 1, later, total)
        return block(lower, 2 * z, later, total)

    zeros = jnp.zeros((BLOCK, HEAD), f32)
    _, total = lax.fori_loop(0, chips, chip, (zeros, zeros), unroll=2)
    out_ref[...] = jnp.transpose(total).astype(bf16)


def mix_body(x_ref, w_ref, out_ref):
    x = jnp.transpose(x_ref[...].astype(f32)).astype(bf16)
    out_ref[...] = nn(x, w_ref[...]).astype(bf16)


def combine_body(ids_ref, group_ref, pair_ref, back_ref, out_ref):
    ids = ids_ref[...]
    first, second = ids[0:1, :], ids[1:2, :]
    place0, place1 = places(first, second)
    shares = jnp.exp(group_ref[...])
    shares = shares / jnp.sum(shares, axis=0, keepdims=True)
    group = iota((GROUPS, BLOCK), 0)
    chosen0 = jnp.sum(jnp.where(first // GROUP_SIZE == group, shares, 0.0), axis=0, keepdims=True)
    chosen1 = jnp.sum(jnp.where(second // GROUP_SIZE == group, shares, 0.0), axis=0, keepdims=True)
    spread = pair_ref[0:1, :] - pair_ref[1:2, :]
    weight0 = chosen0 * jax.nn.sigmoid(spread)
    weight1 = chosen1 * jax.nn.sigmoid(-spread)
    slots = [(first * CAP + place0).astype(f32), (second * CAP + place1).astype(f32)]
    table = jnp.concatenate(slots + [weight0, weight1], axis=0)
    table = jnp.concatenate([table, jnp.zeros((BLOCK - 4, BLOCK), f32)], axis=0)
    table = jnp.transpose(table)
    slot = iota((BLOCK, SLOTS), 1)
    back = back_ref[...]
    pick0 = nn(ones_where(slot == table[:, 0:1].astype(i32)).astype(bf16), back)
    pick1 = nn(ones_where(slot == table[:, 1:2].astype(i32)).astype(bf16), back)
    out_ref[...] = (table[:, 2:3] * pick0 + table[:, 3:4] * pick1).astype(bf16)


def shards(
    attn_rows,
    attn_gain,
    query_weight,
    key_weight,
    value_weight,
    key_bias,
    out_weight,
    expert_rows,
    expert_gain,
    expert_ids,
    group_logits,
    pair_logits,
    gate_weight,
    up_weight,
    down_weight,
):
    ep, tp = lax.axis_size("ep"), lax.axis_size("tp")
    chips = ep // 2
    here = lax.axis_index("ep")
    side = tp // 4
    along_x = [[y * 4 + x for x in range(4)] for y in range(side)]
    along_y = [[y * 4 + x for y in range(side)] for x in range(4)]
    struct = jax.ShapeDtypeStruct

    def exchange(x, axis):
        return lax.all_to_all(x, axis, split_axis=0, concat_axis=0, tiled=True)

    slots = struct((SLOTS, BLOCK), bf16)
    copies = struct((tp, SLOTS, BLOCK), bf16)
    square = struct((BLOCK, BLOCK), bf16)
    ids = expert_ids.T
    column = lax.axis_index("tp").reshape(1)

    def from_chip(x, step):
        moves = [((((z + step) % chips) * 2 + c), z * 2 + c) for z in range(chips) for c in range(2)]
        return lax.ppermute(x, "ep", moves)

    send = call(dispatch_body, 1, 3, slots, 1 << 27, hbm=(1, 2, 3))(
        column, expert_rows, expert_gain[None, :], ids
    )
    routed = exchange(send.reshape(ep, CAP, BLOCK), "ep").reshape(SLOTS, BLOCK)
    outs = (struct((BLOCK, HEAD), bf16), struct((MSG, BLOCK), bf16))
    query, message = call(project_body, 0, 6, outs, 1 << 28, hbm=range(6))(
        attn_rows,
        attn_gain[None, :],
        query_weight.T,
        key_weight.T,
        value_weight.T,
        key_bias,
    )
    behind1 = from_chip(message, -1)
    ahead1 = from_chip(message, 1)
    swaps = [(k, k ^ 1) for k in range(tp)]
    other_weights = lax.ppermute(
        jnp.concatenate([gate_weight[0], up_weight[0]], axis=0), "tp", swaps
    )
    three = packed(behind1, message, ahead1)
    behind3 = from_chip(three, -3)
    ahead3 = from_chip(three, 3)
    routed = call_out(halves_body, 0, 1, struct((tp, ROWS, BLOCK), bf16), 1 << 24, [])(routed)
    routed = exchange(routed, "tp")
    seven = packed_seven(behind3, three, ahead3)
    far = from_chip(seven, 8)
    own_hidden = [pltpu.VMEM((SLOTS, BLOCK), bf16)]
    hidden = call_out(hidden_body, 1, 4, copies, 1 << 29, own_hidden)(
        column, routed, gate_weight[0], up_weight[0], other_weights
    )
    hidden = exchange(hidden, "tp")
    own = packed(behind3, three, ahead3, far)
    other = lax.ppermute(own, "ep", [(e, e ^ 1) for e in range(ep)])
    attended = call(attend_body, 1, 3, struct((HEAD, BLOCK), bf16), 1 << 30)(
        here.reshape(1), query, own, other
    )
    attended = lax.all_gather(attended, "tp", axis=0, tiled=True, axis_index_groups=along_x)
    result = call(down_body, 0, 2, slots, 1 << 28)(hidden, down_weight[0])
    back = exchange(result.reshape(ep, CAP, BLOCK), "ep").reshape(SLOTS, BLOCK)
    attended = lax.all_gather(attended, "tp", axis=0, tiled=True, axis_index_groups=along_y)
    mixed = call(mix_body, 0, 2, square, 1 << 26)(attended, out_weight)
    expert_out = call(combine_body, 0, 4, square, 1 << 27)(ids, group_logits.T, pair_logits.T, back)
    return (mixed, expert_out)


def solution(mesh):
    placed = (
        P("ep", None),
        P(),
        P(None, "tp"),
        P(None, "tp"),
        P(None, "tp"),
        P("tp", "ep"),
        P(None, "tp"),
        P("ep", None),
        P(),
        P("ep", None),
        P("ep", None),
        P("ep", None),
        P("ep", None, "tp"),
        P("ep", None, "tp"),
        P("ep", None, "tp"),
    )
    return jax.shard_map(
        shards,
        mesh=mesh,
        in_specs=placed,
        out_specs=(P("ep", "tp"), P("ep", "tp")),
        check_vma=False,
    )
```

```python
import jax
import jax.numpy as jnp
from jax import lax
from jax.experimental import pallas as pl
from jax.experimental.pallas import tpu as pltpu
from jax.sharding import PartitionSpec as P


EXPERTS = 32
GROUPS = 4
GROUP_SIZE = 8
CAP = 16
BLOCK = 128
HEAD = 64
SLOTS = EXPERTS * CAP
ROWS = SLOTS // 2
MSG = 144
WIDTH = 4

epsilon = 1e-06
f32 = jnp.float32
bf16 = jnp.bfloat16
i32 = jnp.int32

SMEM = pl.BlockSpec(memory_space=pltpu.SMEM)


def call(body, n_scalar, n_in, outs, flops, mib=16, hbm=(), **more):
    def run(*args):
        args = [
            pltpu.with_memory_space_constraint(a, pltpu.HBM) if k in hbm else a
            for k, a in enumerate(args)
        ]
        return kernel(*args)

    kernel = pl.pallas_call(
        body,
        out_shape=outs,
        in_specs=[SMEM] * n_scalar + [pl.BlockSpec()] * n_in,
        cost_estimate=pl.CostEstimate(flops=flops, bytes_accessed=1 << 20, transcendentals=0),
        compiler_params=pltpu.CompilerParams(vmem_limit_bytes=mib << 20),
        **more,
    )
    return run


def call_out(body, n_scalar, n_in, out, flops, scratch):
    copies = [pltpu.SemaphoreType.DMA((out.shape[0],))]
    more = {"out_specs": pl.BlockSpec(memory_space=pltpu.HBM), "scratch_shapes": scratch + copies}
    return call(body, n_scalar, n_in, pltpu.HBM(out.shape, out.dtype), flops, **more)


def nn(a, b):
    return lax.dot_general(a, b, (((1,), (0,)), ((), ())), preferred_element_type=f32)


def nt(a, b):
    return lax.dot_general(a, b, (((1,), (1,)), ((), ())), preferred_element_type=f32)


def iota(shape, dim):
    return lax.broadcasted_iota(i32, shape, dim)


def ones_where(mask):
    return jnp.where(mask, 1.0, 0.0).astype(f32)


def places(first, second):
    expert = iota((EXPERTS, BLOCK), 0)
    mark0 = ones_where(first == expert)
    mark1 = ones_where(second == expert)
    earlier = ones_where(iota((BLOCK, BLOCK), 0) < iota((BLOCK, BLOCK), 1)).astype(bf16)
    before = nn((mark0 + mark1).astype(bf16), earlier)
    place0 = jnp.sum(mark0 * before, axis=0, keepdims=True)
    place1 = jnp.sum(mark1 * before, axis=0, keepdims=True)
    return place0.astype(i32), place1.astype(i32)


def dispatch_body(tp_ref, rows_ref, gain_ref, ids_ref, out_ref):
    x = rows_ref[...].astype(f32)
    inv = lax.rsqrt(jnp.mean(x * x, axis=-1, keepdims=True) + epsilon)
    at = pl.multiple_of(tp_ref[0] * BLOCK, BLOCK)
    own = rows_ref[:, pl.ds(at, BLOCK)].astype(f32)
    own = (own * inv * gain_ref[:, pl.ds(at, BLOCK)]).astype(bf16)
    ids = ids_ref[...]
    first, second = ids[0:1, :], ids[1:2, :]
    place0, place1 = places(first, second)
    slot = iota((SLOTS, BLOCK), 0)
    hit = (slot == first * CAP + place0) | (slot == second * CAP + place1)
    out_ref[...] = nn(ones_where(hit).astype(bf16), own).astype(bf16)


def project_body(rows_ref, gain_ref, wq_ref, wk_ref, wv_ref, bias_ref, q_ref, msg_ref):
    x = rows_ref[...].astype(f32)
    inv = lax.rsqrt(jnp.mean(x * x, axis=-1, keepdims=True) + epsilon)
    normed = (x * inv * gain_ref[...]).astype(bf16)
    q = nt(normed, wq_ref[...]).astype(bf16)
    q_ref[...] = (q.astype(f32) * (HEAD**-0.5)).astype(bf16)
    kv = jnp.concatenate([wk_ref[...], wv_ref[...]], axis=0)
    msg_ref[0:BLOCK, :] = nt(kv, normed).astype(bf16)
    msg_ref[BLOCK:MSG, :] = jnp.broadcast_to(bias_ref[...], (MSG - BLOCK, BLOCK))


def halves_body(x_ref, out_ref, sems):
    copies = []
    for k in range(out_ref.shape[0]):
        half = k % 2
        source = x_ref.at[half * ROWS : (half + 1) * ROWS, :]
        copies.append(pltpu.make_async_copy(source, out_ref.at[k], sems.at[k]))
        copies[-1].start()
    for copy in copies:
        copy.wait()


def hidden_body(tp_ref, x_ref, g0_ref, u0_ref, g1_ref, u1_ref, out_ref, hidden_ref, sems):
    parts = x_ref.shape[0]
    even = tp_ref[0] % 2 == 0
    x = jnp.concatenate([x_ref[k] for k in range(parts)], axis=1)
    own = nn(x, jnp.concatenate([g0_ref[...], u0_ref[...]], axis=1))
    other = nn(x, jnp.concatenate([g1_ref[...], u1_ref[...]], axis=1))

    def gated(both):
        gate, up = both[:, :BLOCK], both[:, BLOCK:]
        return (gate * jax.nn.sigmoid(gate) * up).astype(bf16).astype(f32)

    own, other = gated(own), gated(other)
    first = jnp.where(even, own, other).astype(bf16)
    second = jnp.where(even, other, own).astype(bf16)
    hidden_ref[0:ROWS, :] = first
    hidden_ref[ROWS:SLOTS, :] = second
    copies = [pltpu.make_async_copy(hidden_ref, out_ref.at[k], sems.at[k]) for k in range(parts)]
    for copy in copies:
        copy.start()
    for copy in copies:
        copy.wait()


def down_body(x_ref, w_ref, out_ref):
    parts = x_ref.shape[0]
    for half in range(2):
        x = jnp.concatenate(
            [
                x_ref[k, e * ROWS : (e + 1) * ROWS, :]
                for k in range(half, parts, 2)
                for e in range(2)
            ],
            axis=1,
        )
        out_ref[half * ROWS : (half + 1) * ROWS, :] = nn(x, w_ref[...]).astype(bf16)


def attend_body(pos_ref, q_ref, own_ref, other_ref, out_ref):
    here = pos_ref[0]
    core = here % 2
    chips = own_ref.shape[0] // MSG
    q = q_ref[...]
    wide = (2 * BLOCK, 2 * BLOCK)
    row, col = iota(wide, 0), iota(wide, 1)
    row = jnp.where(row >= BLOCK, row - BLOCK, row)
    tail = ones_where((col >= BLOCK) | (row >= col)).astype(bf16)
    t, s = iota((BLOCK, BLOCK), 0), iota((BLOCK, BLOCK), 1)

    offset = s - t

    def step(k, carry):
        later, total = carry
        messages, starts = [], []
        for w in range(WIDTH):
            z = chips - 1 - (k * WIDTH + w)
            at = pl.multiple_of(((z % 4) * (chips // 4) + z // 4) * MSG, 16)
            own = own_ref[pl.ds(at, MSG), :]
            other = other_ref[pl.ds(at, MSG), :]
            messages += [jnp.where(core == 1, own, other), jnp.where(core == 1, other, own)]
            starts += [(here - 2 * z - 1) * BLOCK, (here - 2 * z) * BLOCK]
        scores = [nn(q, m[0:HEAD, :]) + m[BLOCK : BLOCK + 1, :].astype(f32) for m in messages]
        causal = [offset < start for start in starts]
        logs = [jnp.log(1.0 + jnp.exp(-jnp.abs(x))) for x in scores]
        keep = [-(jnp.maximum(x, 0.0) + y) for x, y in zip(scores, logs)]
        keep = [jnp.where(c, x, 0.0) for c, x in zip(causal, keep)]
        high = [x.astype(bf16) for x in keep]
        low = [(x - y.astype(f32)).astype(bf16) for x, y in zip(keep, high)]
        sums = [nn(jnp.concatenate([x, y], axis=1), tail) for x, y in zip(high, low)]
        weights = [jnp.exp(x + y[:, :BLOCK]) for x, y in zip(scores, sums)]
        weights = [jnp.where(c, x, 0.0).astype(bf16) for c, x in zip(causal, weights)]
        outs = [nt(x, m[HEAD:BLOCK, :]) for x, m in zip(weights, messages)]
        for x, y in zip(outs, sums):
            total = total + jnp.exp(later) * x
            later = later + y[:, BLOCK : BLOCK + HEAD]
        return later, total

    zeros = jnp.zeros((BLOCK, HEAD), f32)
    _, total = lax.fori_loop(0, chips // WIDTH, step, (zeros, zeros))
    out_ref[...] = jnp.transpose(total).astype(bf16)


def mix_body(x_ref, w_ref, out_ref):
    x = jnp.transpose(x_ref[...].astype(f32)).astype(bf16)
    out_ref[...] = nn(x, w_ref[...]).astype(bf16)


def combine_body(ids_ref, group_ref, pair_ref, back_ref, out_ref):
    ids = ids_ref[...]
    first, second = ids[0:1, :], ids[1:2, :]
    place0, place1 = places(first, second)
    shares = jnp.exp(group_ref[...])
    shares = shares / jnp.sum(shares, axis=0, keepdims=True)
    group = iota((GROUPS, BLOCK), 0)
    chosen0 = jnp.sum(jnp.where(first // GROUP_SIZE == group, shares, 0.0), axis=0, keepdims=True)
    chosen1 = jnp.sum(jnp.where(second // GROUP_SIZE == group, shares, 0.0), axis=0, keepdims=True)
    spread = pair_ref[0:1, :] - pair_ref[1:2, :]
    weight0 = chosen0 * jax.nn.sigmoid(spread)
    weight1 = chosen1 * jax.nn.sigmoid(-spread)
    slots = [(first * CAP + place0).astype(f32), (second * CAP + place1).astype(f32)]
    table = jnp.concatenate(slots + [weight0, weight1], axis=0)
    table = jnp.concatenate([table, jnp.zeros((BLOCK - 4, BLOCK), f32)], axis=0)
    table = jnp.transpose(table)
    slot = iota((BLOCK, SLOTS), 1)
    back = back_ref[...]
    pick0 = nn(ones_where(slot == table[:, 0:1].astype(i32)).astype(bf16), back)
    pick1 = nn(ones_where(slot == table[:, 1:2].astype(i32)).astype(bf16), back)
    out_ref[...] = (table[:, 2:3] * pick0 + table[:, 3:4] * pick1).astype(bf16)


def shards(
    attn_rows,
    attn_gain,
    query_weight,
    key_weight,
    value_weight,
    key_bias,
    out_weight,
    expert_rows,
    expert_gain,
    expert_ids,
    group_logits,
    pair_logits,
    gate_weight,
    up_weight,
    down_weight,
):
    ep, tp = lax.axis_size("ep"), lax.axis_size("tp")
    chips = ep // 2
    here = lax.axis_index("ep")
    run = chips // 4
    strided = [[(m + 4 * k) * 2 + c for k in range(run)] for m in range(4) for c in range(2)]
    nearby = [[(m + 4 * k) * 2 + c for m in range(4)] for k in range(run) for c in range(2)]
    side = tp // 4
    along_x = [[y * 4 + x for x in range(4)] for y in range(side)]
    along_y = [[y * 4 + x for y in range(side)] for x in range(4)]
    struct = jax.ShapeDtypeStruct

    def exchange(x, axis):
        return lax.all_to_all(x, axis, split_axis=0, concat_axis=0, tiled=True)

    slots = struct((SLOTS, BLOCK), bf16)
    copies = struct((tp, SLOTS, BLOCK), bf16)
    square = struct((BLOCK, BLOCK), bf16)
    ids = expert_ids.T
    column = lax.axis_index("tp").reshape(1)

    send = call(dispatch_body, 1, 3, slots, 1 << 27, hbm=(1, 2, 3))(
        column, expert_rows, expert_gain[None, :], ids
    )
    routed = exchange(send.reshape(ep, CAP, BLOCK), "ep").reshape(SLOTS, BLOCK)
    outs = (struct((BLOCK, HEAD), bf16), struct((MSG, BLOCK), bf16))
    query, message = call(project_body, 0, 6, outs, 1 << 28, hbm=range(6))(
        attn_rows,
        attn_gain[None, :],
        query_weight.T,
        key_weight.T,
        value_weight.T,
        key_bias,
    )
    swaps = [(k, k ^ 1) for k in range(tp)]
    other_gate = lax.ppermute(gate_weight[0], "tp", swaps)
    other_up = lax.ppermute(up_weight[0], "tp", swaps)
    keys = lax.all_gather(message, "ep", axis=0, tiled=True, axis_index_groups=strided)
    routed = call_out(halves_body, 0, 1, struct((tp, ROWS, BLOCK), bf16), 1 << 24, [])(routed)
    routed = exchange(routed, "tp")
    own = lax.all_gather(keys, "ep", axis=0, tiled=True, axis_index_groups=nearby)
    own_hidden = [pltpu.VMEM((SLOTS, BLOCK), bf16)]
    hidden = call_out(hidden_body, 1, 5, copies, 1 << 29, own_hidden)(
        column, routed, gate_weight[0], up_weight[0], other_gate, other_up
    )
    hidden = exchange(hidden, "tp")
    other = lax.ppermute(own, "ep", [(e, e ^ 1) for e in range(ep)])
    attended = call(attend_body, 1, 3, struct((HEAD, BLOCK), bf16), 1 << 30)(
        here.reshape(1), query, own, other
    )
    attended = lax.all_gather(attended, "tp", axis=0, tiled=True, axis_index_groups=along_x)
    result = call(down_body, 0, 2, slots, 1 << 28)(hidden, down_weight[0])
    back = exchange(result.reshape(ep, CAP, BLOCK), "ep").reshape(SLOTS, BLOCK)
    attended = lax.all_gather(attended, "tp", axis=0, tiled=True, axis_index_groups=along_y)
    mixed = call(mix_body, 0, 2, square, 1 << 26)(attended, out_weight)
    expert_out = call(combine_body, 0, 4, square, 1 << 27)(ids, group_logits.T, pair_logits.T, back)
    return (mixed, expert_out)


def solution(mesh):
    placed = (
        P("ep", None),
        P(),
        P(None, "tp"),
        P(None, "tp"),
        P(None, "tp"),
        P("tp", "ep"),
        P(None, "tp"),
        P("ep", None),
        P(),
        P("ep", None),
        P("ep", None),
        P("ep", None),
        P("ep", None, "tp"),
        P("ep", None, "tp"),
        P("ep", None, "tp"),
    )
    return jax.shard_map(
        shards,
        mesh=mesh,
        in_specs=placed,
        out_specs=(P("ep", "tp"), P("ep", "tp")),
        check_vma=False,
    )
```

```python
import jax
import jax.numpy as jnp
from jax import lax
from jax.experimental import pallas as pl
from jax.experimental.pallas import tpu as pltpu
from jax.sharding import PartitionSpec as P


EXPERTS = 32
GROUPS = 4
GROUP_SIZE = 8
CAP = 16
BLOCK = 128
HEAD = 64
SLOTS = EXPERTS * CAP
ROWS = SLOTS // 2
MSG = 144
WIDTH = 4

epsilon = 1e-06
f32 = jnp.float32
bf16 = jnp.bfloat16
i32 = jnp.int32

SMEM = pl.BlockSpec(memory_space=pltpu.SMEM)


def call(body, n_scalar, n_in, outs, flops, mib=16, hbm=(), **more):
    def run(*args):
        args = [
            pltpu.with_memory_space_constraint(a, pltpu.HBM) if k in hbm else a
            for k, a in enumerate(args)
        ]
        return kernel(*args)

    kernel = pl.pallas_call(
        body,
        out_shape=outs,
        in_specs=[SMEM] * n_scalar + [pl.BlockSpec()] * n_in,
        cost_estimate=pl.CostEstimate(flops=flops, bytes_accessed=1 << 20, transcendentals=0),
        compiler_params=pltpu.CompilerParams(vmem_limit_bytes=mib << 20),
        **more,
    )
    return run


def call_out(body, n_scalar, n_in, out, flops, scratch, copies):
    copies = [pltpu.SemaphoreType.DMA((copies,))]
    more = {"out_specs": pl.BlockSpec(memory_space=pltpu.HBM), "scratch_shapes": scratch + copies}
    return call(body, n_scalar, n_in, pltpu.HBM(out.shape, out.dtype), flops, **more)


def nn(a, b):
    return lax.dot_general(a, b, (((1,), (0,)), ((), ())), preferred_element_type=f32)


def nt(a, b):
    return lax.dot_general(a, b, (((1,), (1,)), ((), ())), preferred_element_type=f32)


def iota(shape, dim):
    return lax.broadcasted_iota(i32, shape, dim)


def ones_where(mask):
    return jnp.where(mask, 1.0, 0.0).astype(f32)


def places(first, second):
    expert = iota((EXPERTS, BLOCK), 0)
    mark0 = ones_where(first == expert)
    mark1 = ones_where(second == expert)
    earlier = ones_where(iota((BLOCK, BLOCK), 0) < iota((BLOCK, BLOCK), 1)).astype(bf16)
    before = nn((mark0 + mark1).astype(bf16), earlier)
    place0 = jnp.sum(mark0 * before, axis=0, keepdims=True)
    place1 = jnp.sum(mark1 * before, axis=0, keepdims=True)
    return place0.astype(i32), place1.astype(i32)


def dispatch_body(tp_ref, rows_ref, gain_ref, ids_ref, out_ref):
    x = rows_ref[...].astype(f32)
    inv = lax.rsqrt(jnp.mean(x * x, axis=-1, keepdims=True) + epsilon)
    at = pl.multiple_of(tp_ref[0] * BLOCK, BLOCK)
    own = rows_ref[:, pl.ds(at, BLOCK)].astype(f32)
    own = (own * inv * gain_ref[:, pl.ds(at, BLOCK)]).astype(bf16)
    ids = ids_ref[...]
    first, second = ids[0:1, :], ids[1:2, :]
    place0, place1 = places(first, second)
    slot = iota((SLOTS, BLOCK), 0)
    hit = (slot == first * CAP + place0) | (slot == second * CAP + place1)
    out_ref[...] = nn(ones_where(hit).astype(bf16), own).astype(bf16)


def project_body(rows_ref, gain_ref, wq_ref, wk_ref, wv_ref, bias_ref, q_ref, msg_ref):
    x = rows_ref[...].astype(f32)
    inv = lax.rsqrt(jnp.mean(x * x, axis=-1, keepdims=True) + epsilon)
    normed = (x * inv * gain_ref[...]).astype(bf16)
    q = nt(normed, wq_ref[...]).astype(bf16)
    q_ref[...] = (q.astype(f32) * (HEAD**-0.5)).astype(bf16)
    kv = jnp.concatenate([wk_ref[...], wv_ref[...]], axis=0)
    msg_ref[0:BLOCK, :] = nt(kv, normed).astype(bf16)
    msg_ref[BLOCK:MSG, :] = jnp.broadcast_to(bias_ref[...], (MSG - BLOCK, BLOCK))


def halves_body(x_ref, out_ref, sems):
    copies = []
    for k in range(out_ref.shape[0]):
        half = k % 2
        source = x_ref.at[half * ROWS : (half + 1) * ROWS, :]
        copies.append(pltpu.make_async_copy(source, out_ref.at[k], sems.at[k]))
        copies[-1].start()
    for copy in copies:
        copy.wait()


def hidden_body(tp_ref, x_ref, g0_ref, u0_ref, g1_ref, u1_ref, out_ref, hidden_ref, sems):
    parts = x_ref.shape[0]
    even = tp_ref[0] % 2 == 0
    own_weights = jnp.concatenate([g0_ref[...], u0_ref[...]], axis=1)
    other_weights = jnp.concatenate([g1_ref[...], u1_ref[...]], axis=1)

    def gated(both):
        gate, up = both[:, :BLOCK], both[:, BLOCK:]
        return gate * jax.nn.sigmoid(gate) * up

    copies = []
    for m in range(2):
        x = [x_ref[k, m * BLOCK : (m + 1) * BLOCK, :] for k in range(parts)]
        x = jnp.concatenate(x, axis=1)
        own, other = gated(nn(x, own_weights)), gated(nn(x, other_weights))
        span = slice(m * ROWS, (m + 1) * ROWS)
        hidden_ref[m * ROWS : m * ROWS + BLOCK, :] = jnp.where(even, own, other).astype(bf16)
        hidden_ref[m * ROWS + BLOCK : (m + 1) * ROWS, :] = jnp.where(even, other, own).astype(bf16)
        for k in range(parts):
            target = out_ref.at[k, span, :]
            copies.append(
                pltpu.make_async_copy(hidden_ref.at[span, :], target, sems.at[m * parts + k])
            )
            copies[-1].start()
    for copy in copies:
        copy.wait()


def down_body(x_ref, w_ref, out_ref):
    parts = x_ref.shape[0]
    for half in range(2):
        for m in range(2):
            at = m * ROWS
            x = jnp.concatenate(
                [
                    x_ref[k, at + e * BLOCK : at + (e + 1) * BLOCK, :]
                    for k in range(half, parts, 2)
                    for e in range(2)
                ],
                axis=1,
            )
            at = half * ROWS + m * BLOCK
            out_ref[at : at + BLOCK, :] = nn(x, w_ref[...]).astype(bf16)


def attend_body(pos_ref, q_ref, own_ref, other_ref, out_ref):
    here = pos_ref[0]
    core = here % 2
    chips = own_ref.shape[0] // MSG
    q = q_ref[...]
    wide = (2 * BLOCK, 2 * BLOCK)
    row, col = iota(wide, 0), iota(wide, 1)
    row = jnp.where(row >= BLOCK, row - BLOCK, row)
    tail = ones_where((col >= BLOCK) | (row >= col)).astype(bf16)
    t, s = iota((BLOCK, BLOCK), 0), iota((BLOCK, BLOCK), 1)

    offset = s - t

    def step(k, carry):
        later, total = carry
        messages, starts = [], []
        for w in range(WIDTH):
            z = chips - 1 - (k * WIDTH + w)
            at = pl.multiple_of(((z % 4) * (chips // 4) + z // 4) * MSG, 16)
            own = own_ref[pl.ds(at, MSG), :]
            other = other_ref[pl.ds(at, MSG), :]
            messages += [jnp.where(core == 1, own, other), jnp.where(core == 1, other, own)]
            starts += [(here - 2 * z - 1) * BLOCK, (here - 2 * z) * BLOCK]
        scores = [nn(q, m[0:HEAD, :]) + m[BLOCK : BLOCK + 1, :].astype(f32) for m in messages]
        causal = [offset < start for start in starts]
        logs = [jnp.log(1.0 + jnp.exp(-jnp.abs(x))) for x in scores]
        keep = [-(jnp.maximum(x, 0.0) + y) for x, y in zip(scores, logs)]
        keep = [jnp.where(c, x, 0.0) for c, x in zip(causal, keep)]
        high = [x.astype(bf16) for x in keep]
        low = [(x - y.astype(f32)).astype(bf16) for x, y in zip(keep, high)]
        sums = [nn(jnp.concatenate([x, y], axis=1), tail) for x, y in zip(high, low)]
        weights = [jnp.exp(x + y[:, :BLOCK]) for x, y in zip(scores, sums)]
        weights = [jnp.where(c, x, 0.0).astype(bf16) for c, x in zip(causal, weights)]
        outs = [nt(x, m[HEAD:BLOCK, :]) for x, m in zip(weights, messages)]
        for x, y in zip(outs, sums):
            total = total + jnp.exp(later) * x
            later = later + y[:, BLOCK : BLOCK + HEAD]
        return later, total

    zeros = jnp.zeros((BLOCK, HEAD), f32)
    _, total = lax.fori_loop(0, chips // WIDTH, step, (zeros, zeros))
    out_ref[...] = jnp.transpose(total).astype(bf16)


def mix_body(x_ref, w_ref, out_ref):
    x = jnp.transpose(x_ref[...].astype(f32)).astype(bf16)
    out_ref[...] = nn(x, w_ref[...]).astype(bf16)


def combine_body(ids_ref, group_ref, pair_ref, back_ref, out_ref):
    ids = ids_ref[...]
    first, second = ids[0:1, :], ids[1:2, :]
    place0, place1 = places(first, second)
    shares = jnp.exp(group_ref[...])
    shares = shares / jnp.sum(shares, axis=0, keepdims=True)
    group = iota((GROUPS, BLOCK), 0)
    chosen0 = jnp.sum(jnp.where(first // GROUP_SIZE == group, shares, 0.0), axis=0, keepdims=True)
    chosen1 = jnp.sum(jnp.where(second // GROUP_SIZE == group, shares, 0.0), axis=0, keepdims=True)
    spread = pair_ref[0:1, :] - pair_ref[1:2, :]
    weight0 = chosen0 * jax.nn.sigmoid(spread)
    weight1 = chosen1 * jax.nn.sigmoid(-spread)
    slots = [(first * CAP + place0).astype(f32), (second * CAP + place1).astype(f32)]
    table = jnp.concatenate(slots + [weight0, weight1], axis=0)
    table = jnp.concatenate([table, jnp.zeros((BLOCK - 4, BLOCK), f32)], axis=0)
    table = jnp.transpose(table)
    slot = iota((BLOCK, SLOTS), 1)
    back = back_ref[...]
    pick0 = nn(ones_where(slot == table[:, 0:1].astype(i32)).astype(bf16), back)
    pick1 = nn(ones_where(slot == table[:, 1:2].astype(i32)).astype(bf16), back)
    out_ref[...] = (table[:, 2:3] * pick0 + table[:, 3:4] * pick1).astype(bf16)


def shards(
    attn_rows,
    attn_gain,
    query_weight,
    key_weight,
    value_weight,
    key_bias,
    out_weight,
    expert_rows,
    expert_gain,
    expert_ids,
    group_logits,
    pair_logits,
    gate_weight,
    up_weight,
    down_weight,
):
    ep, tp = lax.axis_size("ep"), lax.axis_size("tp")
    chips = ep // 2
    here = lax.axis_index("ep")
    run = chips // 4
    strided = [[(m + 4 * k) * 2 + c for k in range(run)] for m in range(4) for c in range(2)]
    nearby = [[(m + 4 * k) * 2 + c for m in range(4)] for k in range(run) for c in range(2)]
    struct = jax.ShapeDtypeStruct

    def exchange(x, axis):
        return lax.all_to_all(x, axis, split_axis=0, concat_axis=0, tiled=True)

    slots = struct((SLOTS, BLOCK), bf16)
    copies = struct((tp, SLOTS, BLOCK), bf16)
    square = struct((BLOCK, BLOCK), bf16)
    ids = expert_ids.T
    column = lax.axis_index("tp").reshape(1)

    send = call(dispatch_body, 1, 3, slots, 1 << 27, hbm=(1, 2, 3))(
        column, expert_rows, expert_gain[None, :], ids
    )
    routed = exchange(send.reshape(ep, CAP, BLOCK), "ep").reshape(SLOTS, BLOCK)
    outs = (struct((BLOCK, HEAD), bf16), struct((MSG, BLOCK), bf16))
    query, message = call(project_body, 0, 6, outs, 1 << 28, hbm=range(6))(
        attn_rows,
        attn_gain[None, :],
        query_weight.T,
        key_weight.T,
        value_weight.T,
        key_bias,
    )
    swaps = [(k, k ^ 1) for k in range(tp)]
    other_gate = lax.ppermute(gate_weight[0], "tp", swaps)
    other_up = lax.ppermute(up_weight[0], "tp", swaps)
    keys = lax.all_gather(message, "ep", axis=0, tiled=True, axis_index_groups=strided)
    routed = call_out(halves_body, 0, 1, struct((tp, ROWS, BLOCK), bf16), 1 << 24, [], tp)(routed)
    routed = exchange(routed, "tp")
    own = lax.all_gather(keys, "ep", axis=0, tiled=True, axis_index_groups=nearby)
    own_hidden = [pltpu.VMEM((SLOTS, BLOCK), bf16)]
    hidden = call_out(hidden_body, 1, 5, copies, 1 << 29, own_hidden, 2 * tp)(
        column, routed, gate_weight[0], up_weight[0], other_gate, other_up
    )
    hidden = exchange(hidden, "tp")
    other = lax.ppermute(own, "ep", [(e, e ^ 1) for e in range(ep)])
    attended = call(attend_body, 1, 3, struct((HEAD, BLOCK), bf16), 1 << 30)(
        here.reshape(1), query, own, other
    )
    result = call(down_body, 0, 2, slots, 1 << 28)(hidden, down_weight[0])
    back = exchange(result.reshape(ep, CAP, BLOCK), "ep").reshape(SLOTS, BLOCK)
    attended = lax.all_gather(attended, "tp", axis=0, tiled=True)
    mixed = call(mix_body, 0, 2, square, 1 << 26)(attended, out_weight)
    expert_out = call(combine_body, 0, 4, square, 1 << 27)(ids, group_logits.T, pair_logits.T, back)
    return (mixed, expert_out)


def solution(mesh):
    placed = (
        P("ep", None),
        P(),
        P(None, "tp"),
        P(None, "tp"),
        P(None, "tp"),
        P("tp", "ep"),
        P(None, "tp"),
        P("ep", None),
        P(),
        P("ep", None),
        P("ep", None),
        P("ep", None),
        P("ep", None, "tp"),
        P("ep", None, "tp"),
        P("ep", None, "tp"),
    )
    return jax.shard_map(
        shards,
        mesh=mesh,
        in_specs=placed,
        out_specs=(P("ep", "tp"), P("ep", "tp")),
        check_vma=False,
    )
```

```python
import jax
import jax.numpy as jnp
from jax import lax
from jax.experimental import pallas as pl
from jax.experimental.pallas import tpu as pltpu
from jax.sharding import PartitionSpec as P


EXPERTS = 32
GROUPS = 4
GROUP_SIZE = 8
CAP = 16
BLOCK = 128
HEAD = 64
SLOTS = EXPERTS * CAP
ROWS = SLOTS // 2
MSG = 144
WIDTH = 4

epsilon = 1e-06
f32 = jnp.float32
bf16 = jnp.bfloat16
i32 = jnp.int32

SMEM = pl.BlockSpec(memory_space=pltpu.SMEM)


def call(body, n_scalar, n_in, outs, flops, mib=16, hbm=(), **more):
    def run(*args):
        args = [
            pltpu.with_memory_space_constraint(a, pltpu.HBM) if k in hbm else a
            for k, a in enumerate(args)
        ]
        return kernel(*args)

    kernel = pl.pallas_call(
        body,
        out_shape=outs,
        in_specs=[SMEM] * n_scalar + [pl.BlockSpec()] * n_in,
        cost_estimate=pl.CostEstimate(flops=flops, bytes_accessed=1 << 20, transcendentals=0),
        compiler_params=pltpu.CompilerParams(vmem_limit_bytes=mib << 20),
        **more,
    )
    return run


def call_out(body, n_scalar, n_in, out, flops, scratch, copies):
    copies = [pltpu.SemaphoreType.DMA((copies,))]
    more = {"out_specs": pl.BlockSpec(memory_space=pltpu.HBM), "scratch_shapes": scratch + copies}
    return call(body, n_scalar, n_in, pltpu.HBM(out.shape, out.dtype), flops, **more)


def nn(a, b):
    return lax.dot_general(a, b, (((1,), (0,)), ((), ())), preferred_element_type=f32)


def nt(a, b):
    return lax.dot_general(a, b, (((1,), (1,)), ((), ())), preferred_element_type=f32)


def iota(shape, dim):
    return lax.broadcasted_iota(i32, shape, dim)


def ones_where(mask):
    return jnp.where(mask, 1.0, 0.0).astype(f32)


def places(first, second):
    expert = iota((EXPERTS, BLOCK), 0)
    mark0 = ones_where(first == expert)
    mark1 = ones_where(second == expert)
    earlier = ones_where(iota((BLOCK, BLOCK), 0) < iota((BLOCK, BLOCK), 1)).astype(bf16)
    before = nn((mark0 + mark1).astype(bf16), earlier)
    place0 = jnp.sum(mark0 * before, axis=0, keepdims=True)
    place1 = jnp.sum(mark1 * before, axis=0, keepdims=True)
    return place0.astype(i32), place1.astype(i32)


def dispatch_body(tp_ref, rows_ref, gain_ref, ids_ref, out_ref):
    x = rows_ref[...].astype(f32)
    inv = lax.rsqrt(jnp.mean(x * x, axis=-1, keepdims=True) + epsilon)
    at = pl.multiple_of(tp_ref[0] * BLOCK, BLOCK)
    own = rows_ref[:, pl.ds(at, BLOCK)].astype(f32)
    own = (own * inv * gain_ref[:, pl.ds(at, BLOCK)]).astype(bf16)
    ids = ids_ref[...]
    first, second = ids[0:1, :], ids[1:2, :]
    place0, place1 = places(first, second)
    slot = iota((SLOTS, BLOCK), 0)
    hit = (slot == first * CAP + place0) | (slot == second * CAP + place1)
    out_ref[...] = nn(ones_where(hit).astype(bf16), own).astype(bf16)


def project_body(rows_ref, gain_ref, wq_ref, wk_ref, wv_ref, bias_ref, q_ref, msg_ref):
    x = rows_ref[...].astype(f32)
    inv = lax.rsqrt(jnp.mean(x * x, axis=-1, keepdims=True) + epsilon)
    normed = (x * inv * gain_ref[...]).astype(bf16)
    q = nt(normed, wq_ref[...]).astype(bf16)
    q_ref[...] = (q.astype(f32) * (HEAD**-0.5)).astype(bf16)
    kv = jnp.concatenate([wk_ref[...], wv_ref[...]], axis=0)
    msg_ref[0:BLOCK, :] = nt(kv, normed).astype(bf16)
    msg_ref[BLOCK:MSG, :] = jnp.broadcast_to(bias_ref[...], (MSG - BLOCK, BLOCK))


def halves_body(x_ref, out_ref, sems):
    copies = []
    for k in range(out_ref.shape[0]):
        half = k % 2
        source = x_ref.at[half * ROWS : (half + 1) * ROWS, :]
        copies.append(pltpu.make_async_copy(source, out_ref.at[k], sems.at[k]))
        copies[-1].start()
    for copy in copies:
        copy.wait()


def hidden_body(tp_ref, x_ref, g0_ref, u0_ref, g1_ref, u1_ref, out_ref, hidden_ref, sems):
    parts = x_ref.shape[0]
    even = tp_ref[0] % 2 == 0
    own_weights = jnp.concatenate([g0_ref[...], u0_ref[...]], axis=1)
    other_weights = jnp.concatenate([g1_ref[...], u1_ref[...]], axis=1)

    def gated(both):
        gate, up = both[:, :BLOCK], both[:, BLOCK:]
        return gate * jax.nn.sigmoid(gate) * up

    copies = []
    for m in range(2):
        x = [x_ref[k, m * BLOCK : (m + 1) * BLOCK, :] for k in range(parts)]
        x = jnp.concatenate(x, axis=1)
        own, other = gated(nn(x, own_weights)), gated(nn(x, other_weights))
        span = slice(m * ROWS, (m + 1) * ROWS)
        hidden_ref[m * ROWS : m * ROWS + BLOCK, :] = jnp.where(even, own, other).astype(bf16)
        hidden_ref[m * ROWS + BLOCK : (m + 1) * ROWS, :] = jnp.where(even, other, own).astype(bf16)
        for k in range(parts):
            target = out_ref.at[k, span, :]
            copies.append(
                pltpu.make_async_copy(hidden_ref.at[span, :], target, sems.at[m * parts + k])
            )
            copies[-1].start()
    for copy in copies:
        copy.wait()


def down_body(x_ref, w_ref, out_ref):
    parts = x_ref.shape[0]
    for half in range(2):
        for m in range(2):
            at = m * ROWS
            x = jnp.concatenate(
                [
                    x_ref[k, at + e * BLOCK : at + (e + 1) * BLOCK, :]
                    for k in range(half, parts, 2)
                    for e in range(2)
                ],
                axis=1,
            )
            at = half * ROWS + m * BLOCK
            out_ref[at : at + BLOCK, :] = nn(x, w_ref[...]).astype(bf16)


def attend_body(pos_ref, q_ref, own_ref, other_ref, far_ref, far_other_ref, out_ref):
    here = pos_ref[0]
    core = here % 2
    chips = 2 * own_ref.shape[0] // MSG
    odd = (here // 2) % 2
    q = q_ref[...]
    wide = (2 * BLOCK, 2 * BLOCK)
    row, col = iota(wide, 0), iota(wide, 1)
    row = jnp.where(row >= BLOCK, row - BLOCK, row)
    tail = ones_where((col >= BLOCK) | (row >= col)).astype(bf16)
    t, s = iota((BLOCK, BLOCK), 0), iota((BLOCK, BLOCK), 1)

    offset = s - t

    def step(k, carry):
        later, total = carry
        messages, starts = [], []
        for w in range(WIDTH):
            z = chips - 1 - (k * WIDTH + w)
            at = pl.ds(pl.multiple_of((z // 2) * MSG, 16), MSG)
            near = odd == (WIDTH - 1 - w) % 2
            own = jnp.where(near, own_ref[at, :], far_ref[at, :])
            other = jnp.where(near, other_ref[at, :], far_other_ref[at, :])
            messages += [jnp.where(core == 1, own, other), jnp.where(core == 1, other, own)]
            starts += [(here - 2 * z - 1) * BLOCK, (here - 2 * z) * BLOCK]
        scores = [nn(q, m[0:HEAD, :]) + m[BLOCK : BLOCK + 1, :].astype(f32) for m in messages]
        causal = [offset < start for start in starts]
        logs = [jnp.log(1.0 + jnp.exp(-jnp.abs(x))) for x in scores]
        keep = [-(jnp.maximum(x, 0.0) + y) for x, y in zip(scores, logs)]
        keep = [jnp.where(c, x, 0.0) for c, x in zip(causal, keep)]
        high = [x.astype(bf16) for x in keep]
        low = [(x - y.astype(f32)).astype(bf16) for x, y in zip(keep, high)]
        sums = [nn(jnp.concatenate([x, y], axis=1), tail) for x, y in zip(high, low)]
        weights = [jnp.exp(x + y[:, :BLOCK]) for x, y in zip(scores, sums)]
        weights = [jnp.where(c, x, 0.0).astype(bf16) for c, x in zip(causal, weights)]
        outs = [nt(x, m[HEAD:BLOCK, :]) for x, m in zip(weights, messages)]
        for x, y in zip(outs, sums):
            total = total + jnp.exp(later) * x
            later = later + y[:, BLOCK : BLOCK + HEAD]
        return later, total

    zeros = jnp.zeros((BLOCK, HEAD), f32)
    _, total = lax.fori_loop(0, chips // WIDTH, step, (zeros, zeros))
    out_ref[...] = jnp.transpose(total).astype(bf16)


def mix_body(x_ref, w_ref, out_ref):
    x = jnp.transpose(x_ref[...].astype(f32)).astype(bf16)
    out_ref[...] = nn(x, w_ref[...]).astype(bf16)


def combine_body(ids_ref, group_ref, pair_ref, back_ref, out_ref):
    ids = ids_ref[...]
    first, second = ids[0:1, :], ids[1:2, :]
    place0, place1 = places(first, second)
    shares = jnp.exp(group_ref[...])
    shares = shares / jnp.sum(shares, axis=0, keepdims=True)
    group = iota((GROUPS, BLOCK), 0)
    chosen0 = jnp.sum(jnp.where(first // GROUP_SIZE == group, shares, 0.0), axis=0, keepdims=True)
    chosen1 = jnp.sum(jnp.where(second // GROUP_SIZE == group, shares, 0.0), axis=0, keepdims=True)
    spread = pair_ref[0:1, :] - pair_ref[1:2, :]
    weight0 = chosen0 * jax.nn.sigmoid(spread)
    weight1 = chosen1 * jax.nn.sigmoid(-spread)
    slots = [(first * CAP + place0).astype(f32), (second * CAP + place1).astype(f32)]
    table = jnp.concatenate(slots + [weight0, weight1], axis=0)
    table = jnp.concatenate([table, jnp.zeros((BLOCK - 4, BLOCK), f32)], axis=0)
    table = jnp.transpose(table)
    slot = iota((BLOCK, SLOTS), 1)
    back = back_ref[...]
    pick0 = nn(ones_where(slot == table[:, 0:1].astype(i32)).astype(bf16), back)
    pick1 = nn(ones_where(slot == table[:, 1:2].astype(i32)).astype(bf16), back)
    out_ref[...] = (table[:, 2:3] * pick0 + table[:, 3:4] * pick1).astype(bf16)


def shards(
    attn_rows,
    attn_gain,
    query_weight,
    key_weight,
    value_weight,
    key_bias,
    out_weight,
    expert_rows,
    expert_gain,
    expert_ids,
    group_logits,
    pair_logits,
    gate_weight,
    up_weight,
    down_weight,
):
    ep, tp = lax.axis_size("ep"), lax.axis_size("tp")
    chips = ep // 2
    here = lax.axis_index("ep")
    run = chips // 4
    strided = [[(m + 4 * k) * 2 + c for k in range(run)] for m in range(4) for c in range(2)]
    pairs = [[(z + 2 * b) * 2 + c for b in range(2)] for z in range(chips) if z % 4 < 2 for c in range(2)]
    side = tp // 4
    along_x = [[y * 4 + x for x in range(4)] for y in range(side)]
    along_y = [[y * 4 + x for y in range(side)] for x in range(4)]
    struct = jax.ShapeDtypeStruct

    def exchange(x, axis):
        return lax.all_to_all(x, axis, split_axis=0, concat_axis=0, tiled=True)

    slots = struct((SLOTS, BLOCK), bf16)
    copies = struct((tp, SLOTS, BLOCK), bf16)
    square = struct((BLOCK, BLOCK), bf16)
    ids = expert_ids.T
    column = lax.axis_index("tp").reshape(1)

    send = call(dispatch_body, 1, 3, slots, 1 << 27, hbm=(1, 2, 3))(
        column, expert_rows, expert_gain[None, :], ids
    )
    routed = exchange(send.reshape(ep, CAP, BLOCK), "ep").reshape(SLOTS, BLOCK)
    outs = (struct((BLOCK, HEAD), bf16), struct((MSG, BLOCK), bf16))
    query, message = call(project_body, 0, 6, outs, 1 << 28, hbm=range(6))(
        attn_rows,
        attn_gain[None, :],
        query_weight.T,
        key_weight.T,
        value_weight.T,
        key_bias,
    )
    swaps = [(k, k ^ 1) for k in range(tp)]
    other_gate = lax.ppermute(gate_weight[0], "tp", swaps)
    other_up = lax.ppermute(up_weight[0], "tp", swaps)
    keys = lax.all_gather(message, "ep", axis=0, tiled=True, axis_index_groups=pairs)
    own = lax.all_gather(keys, "ep", axis=0, tiled=True, axis_index_groups=strided)
    far = lax.ppermute(own, "ep", [(e, e ^ 2) for e in range(ep)])
    routed = call_out(halves_body, 0, 1, struct((tp, ROWS, BLOCK), bf16), 1 << 24, [], tp)(routed)
    routed = exchange(routed, "tp")
    own_hidden = [pltpu.VMEM((SLOTS, BLOCK), bf16)]
    hidden = call_out(hidden_body, 1, 5, copies, 1 << 29, own_hidden, 2 * tp)(
        column, routed, gate_weight[0], up_weight[0], other_gate, other_up
    )
    hidden = exchange(hidden, "tp")
    cores = [(e, e ^ 1) for e in range(ep)]
    own_other = lax.ppermute(own, "ep", cores)
    far_other = lax.ppermute(far, "ep", cores)
    attended = call(attend_body, 1, 5, struct((HEAD, BLOCK), bf16), 1 << 30)(
        here.reshape(1), query, own, own_other, far, far_other
    )
    attended = lax.all_gather(attended, "tp", axis=0, tiled=True, axis_index_groups=along_x)
    result = call(down_body, 0, 2, slots, 1 << 28)(hidden, down_weight[0])
    back = exchange(result.reshape(ep, CAP, BLOCK), "ep").reshape(SLOTS, BLOCK)
    attended = lax.all_gather(attended, "tp", axis=0, tiled=True, axis_index_groups=along_y)
    mixed = call(mix_body, 0, 2, square, 1 << 26)(attended, out_weight)
    expert_out = call(combine_body, 0, 4, square, 1 << 27)(ids, group_logits.T, pair_logits.T, back)
    return (mixed, expert_out)


def solution(mesh):
    placed = (
        P("ep", None),
        P(),
        P(None, "tp"),
        P(None, "tp"),
        P(None, "tp"),
        P("tp", "ep"),
        P(None, "tp"),
        P("ep", None),
        P(),
        P("ep", None),
        P("ep", None),
        P("ep", None),
        P("ep", None, "tp"),
        P("ep", None, "tp"),
        P("ep", None, "tp"),
    )
    return jax.shard_map(
        shards,
        mesh=mesh,
        in_specs=placed,
        out_specs=(P("ep", "tp"), P("ep", "tp")),
        check_vma=False,
    )
```

```python
import jax
import jax.numpy as jnp
from jax import lax
from jax.experimental import pallas as pl
from jax.experimental.pallas import tpu as pltpu
from jax.sharding import PartitionSpec as P


EXPERTS = 32
GROUPS = 4
GROUP_SIZE = 8
CAP = 16
BLOCK = 128
HEAD = 64
SLOTS = EXPERTS * CAP
ROWS = SLOTS // 2
MSG = 144
WIDTH = 4
OFFSETS = (0, 1, 3, 2)

epsilon = 1e-06
f32 = jnp.float32
bf16 = jnp.bfloat16
i32 = jnp.int32

SMEM = pl.BlockSpec(memory_space=pltpu.SMEM)


def call(body, n_scalar, n_in, outs, flops, mib=16, hbm=(), **more):
    def run(*args):
        args = [
            pltpu.with_memory_space_constraint(a, pltpu.HBM) if k in hbm else a
            for k, a in enumerate(args)
        ]
        return kernel(*args)

    kernel = pl.pallas_call(
        body,
        out_shape=outs,
        in_specs=[SMEM] * n_scalar + [pl.BlockSpec()] * n_in,
        cost_estimate=pl.CostEstimate(flops=flops, bytes_accessed=1 << 20, transcendentals=0),
        compiler_params=pltpu.CompilerParams(vmem_limit_bytes=mib << 20),
        **more,
    )
    return run


def call_out(body, n_scalar, n_in, out, flops, scratch, copies):
    copies = [pltpu.SemaphoreType.DMA((copies,))]
    more = {"out_specs": pl.BlockSpec(memory_space=pltpu.HBM), "scratch_shapes": scratch + copies}
    return call(body, n_scalar, n_in, pltpu.HBM(out.shape, out.dtype), flops, **more)


def nn(a, b):
    return lax.dot_general(a, b, (((1,), (0,)), ((), ())), preferred_element_type=f32)


def nt(a, b):
    return lax.dot_general(a, b, (((1,), (1,)), ((), ())), preferred_element_type=f32)


def iota(shape, dim):
    return lax.broadcasted_iota(i32, shape, dim)


def ones_where(mask):
    return jnp.where(mask, 1.0, 0.0).astype(f32)


def places(first, second):
    expert = iota((EXPERTS, BLOCK), 0)
    mark0 = ones_where(first == expert)
    mark1 = ones_where(second == expert)
    earlier = ones_where(iota((BLOCK, BLOCK), 0) < iota((BLOCK, BLOCK), 1)).astype(bf16)
    before = nn((mark0 + mark1).astype(bf16), earlier)
    place0 = jnp.sum(mark0 * before, axis=0, keepdims=True)
    place1 = jnp.sum(mark1 * before, axis=0, keepdims=True)
    return place0.astype(i32), place1.astype(i32)


def dispatch_body(tp_ref, rows_ref, gain_ref, ids_ref, out_ref):
    x = rows_ref[...].astype(f32)
    inv = lax.rsqrt(jnp.mean(x * x, axis=-1, keepdims=True) + epsilon)
    at = pl.multiple_of(tp_ref[0] * BLOCK, BLOCK)
    own = rows_ref[:, pl.ds(at, BLOCK)].astype(f32)
    own = (own * inv * gain_ref[:, pl.ds(at, BLOCK)]).astype(bf16)
    ids = ids_ref[...]
    first, second = ids[0:1, :], ids[1:2, :]
    place0, place1 = places(first, second)
    slot = iota((SLOTS, BLOCK), 0)
    hit = (slot == first * CAP + place0) | (slot == second * CAP + place1)
    out_ref[...] = nn(ones_where(hit).astype(bf16), own).astype(bf16)


def project_body(rows_ref, gain_ref, wq_ref, wk_ref, wv_ref, bias_ref, q_ref, msg_ref):
    x = rows_ref[...].astype(f32)
    inv = lax.rsqrt(jnp.mean(x * x, axis=-1, keepdims=True) + epsilon)
    normed = (x * inv * gain_ref[...]).astype(bf16)
    q = nt(normed, wq_ref[...]).astype(bf16)
    q_ref[...] = (q.astype(f32) * (HEAD**-0.5)).astype(bf16)
    kv = jnp.concatenate([wk_ref[...], wv_ref[...]], axis=0)
    msg_ref[0:BLOCK, :] = nt(kv, normed).astype(bf16)
    msg_ref[BLOCK:MSG, :] = jnp.broadcast_to(bias_ref[...], (MSG - BLOCK, BLOCK))


def halves_body(x_ref, out_ref, sems):
    copies = []
    for k in range(out_ref.shape[0]):
        half = k % 2
        source = x_ref.at[half * ROWS : (half + 1) * ROWS, :]
        copies.append(pltpu.make_async_copy(source, out_ref.at[k], sems.at[k]))
        copies[-1].start()
    for copy in copies:
        copy.wait()


def hidden_body(tp_ref, x_ref, g0_ref, u0_ref, g1_ref, u1_ref, out_ref, hidden_ref, sems):
    parts = x_ref.shape[0]
    even = tp_ref[0] % 2 == 0
    own_weights = jnp.concatenate([g0_ref[...], u0_ref[...]], axis=1)
    other_weights = jnp.concatenate([g1_ref[...], u1_ref[...]], axis=1)

    def gated(both):
        gate, up = both[:, :BLOCK], both[:, BLOCK:]
        return gate * jax.nn.sigmoid(gate) * up

    copies = []
    for m in range(2):
        x = [x_ref[k, m * BLOCK : (m + 1) * BLOCK, :] for k in range(parts)]
        x = jnp.concatenate(x, axis=1)
        own, other = gated(nn(x, own_weights)), gated(nn(x, other_weights))
        span = slice(m * ROWS, (m + 1) * ROWS)
        hidden_ref[m * ROWS : m * ROWS + BLOCK, :] = jnp.where(even, own, other).astype(bf16)
        hidden_ref[m * ROWS + BLOCK : (m + 1) * ROWS, :] = jnp.where(even, other, own).astype(bf16)
        for k in range(parts):
            target = out_ref.at[k, span, :]
            copies.append(
                pltpu.make_async_copy(hidden_ref.at[span, :], target, sems.at[m * parts + k])
            )
            copies[-1].start()
    for copy in copies:
        copy.wait()


def down_body(x_ref, w_ref, out_ref):
    parts = x_ref.shape[0]
    for half in range(2):
        for m in range(2):
            at = m * ROWS
            x = jnp.concatenate(
                [
                    x_ref[k, at + e * BLOCK : at + (e + 1) * BLOCK, :]
                    for k in range(half, parts, 2)
                    for e in range(2)
                ],
                axis=1,
            )
            at = half * ROWS + m * BLOCK
            out_ref[at : at + BLOCK, :] = nn(x, w_ref[...]).astype(bf16)


def attend_body(pos_ref, q_ref, own_ref, other_ref, far_ref, far_other_ref, out_ref):
    here = pos_ref[0]
    core = here % 2
    chips = 2 * own_ref.shape[0] // MSG
    odd = (here // 2) % 2
    q = q_ref[...]
    wide = (2 * BLOCK, 2 * BLOCK)
    row, col = iota(wide, 0), iota(wide, 1)
    row = jnp.where(row >= BLOCK, row - BLOCK, row)
    tail = ones_where((col >= BLOCK) | (row >= col)).astype(bf16)
    t, s = iota((BLOCK, BLOCK), 0), iota((BLOCK, BLOCK), 1)

    offset = s - t

    def step(k, carry):
        later, total = carry
        messages, starts = [], []
        for w in range(WIDTH):
            z = chips - 1 - (k * WIDTH + w)
            at = pl.ds(pl.multiple_of((z // 2) * MSG, 16), MSG)
            near = odd == (WIDTH - 1 - w) % 2
            own = jnp.where(near, own_ref[at, :], far_ref[at, :])
            other = jnp.where(near, other_ref[at, :], far_other_ref[at, :])
            messages += [jnp.where(core == 1, own, other), jnp.where(core == 1, other, own)]
            starts += [(here - 2 * z - 1) * BLOCK, (here - 2 * z) * BLOCK]
        scores = [nn(q, m[0:HEAD, :]) + m[BLOCK : BLOCK + 1, :].astype(f32) for m in messages]
        causal = [offset < start for start in starts]
        logs = [jnp.log(1.0 + jnp.exp(-jnp.abs(x))) for x in scores]
        keep = [-(jnp.maximum(x, 0.0) + y) for x, y in zip(scores, logs)]
        keep = [jnp.where(c, x, 0.0) for c, x in zip(causal, keep)]
        high = [x.astype(bf16) for x in keep]
        low = [(x - y.astype(f32)).astype(bf16) for x, y in zip(keep, high)]
        sums = [nn(jnp.concatenate([x, y], axis=1), tail) for x, y in zip(high, low)]
        weights = [jnp.exp(x + y[:, :BLOCK]) for x, y in zip(scores, sums)]
        weights = [jnp.where(c, x, 0.0).astype(bf16) for c, x in zip(causal, weights)]
        outs = [nt(x, m[HEAD:BLOCK, :]) for x, m in zip(weights, messages)]
        for x, y in zip(outs, sums):
            total = total + jnp.exp(later) * x
            later = later + y[:, BLOCK : BLOCK + HEAD]
        return later, total

    zeros = jnp.zeros((BLOCK, HEAD), f32)
    _, total = lax.fori_loop(0, chips // WIDTH, step, (zeros, zeros))
    out_ref[...] = jnp.transpose(total).astype(bf16)


def pack_body(*refs):
    for k, ref in enumerate(refs[:-1]):
        refs[-1][k * HEAD : (k + 1) * HEAD, :] = ref[...]


def mix_body(tp_ref, x_ref, w_ref, out_ref):
    column = tp_ref[0] % 4
    weights = []
    for k in range(x_ref.shape[0] // HEAD):
        head = k - k % 4 + (column + OFFSETS[k % 4]) % 4
        weights.append(w_ref[pl.ds(pl.multiple_of(head * HEAD, HEAD), HEAD), :])
    x = jnp.transpose(x_ref[...].astype(f32)).astype(bf16)
    out_ref[...] = nn(x, jnp.concatenate(weights, axis=0)).astype(bf16)


def combine_body(ids_ref, group_ref, pair_ref, back_ref, out_ref):
    ids = ids_ref[...]
    first, second = ids[0:1, :], ids[1:2, :]
    place0, place1 = places(first, second)
    shares = jnp.exp(group_ref[...])
    shares = shares / jnp.sum(shares, axis=0, keepdims=True)
    group = iota((GROUPS, BLOCK), 0)
    chosen0 = jnp.sum(jnp.where(first // GROUP_SIZE == group, shares, 0.0), axis=0, keepdims=True)
    chosen1 = jnp.sum(jnp.where(second // GROUP_SIZE == group, shares, 0.0), axis=0, keepdims=True)
    spread = pair_ref[0:1, :] - pair_ref[1:2, :]
    weight0 = chosen0 * jax.nn.sigmoid(spread)
    weight1 = chosen1 * jax.nn.sigmoid(-spread)
    slots = [(first * CAP + place0).astype(f32), (second * CAP + place1).astype(f32)]
    table = jnp.concatenate(slots + [weight0, weight1], axis=0)
    table = jnp.concatenate([table, jnp.zeros((BLOCK - 4, BLOCK), f32)], axis=0)
    table = jnp.transpose(table)
    slot = iota((BLOCK, SLOTS), 1)
    back = back_ref[...]
    pick0 = nn(ones_where(slot == table[:, 0:1].astype(i32)).astype(bf16), back)
    pick1 = nn(ones_where(slot == table[:, 1:2].astype(i32)).astype(bf16), back)
    out_ref[...] = (table[:, 2:3] * pick0 + table[:, 3:4] * pick1).astype(bf16)


def shards(
    attn_rows,
    attn_gain,
    query_weight,
    key_weight,
    value_weight,
    key_bias,
    out_weight,
    expert_rows,
    expert_gain,
    expert_ids,
    group_logits,
    pair_logits,
    gate_weight,
    up_weight,
    down_weight,
):
    ep, tp = lax.axis_size("ep"), lax.axis_size("tp")
    chips = ep // 2
    here = lax.axis_index("ep")
    run = chips // 4
    strided = [[(m + 4 * k) * 2 + c for k in range(run)] for m in range(4) for c in range(2)]
    pairs = [[(z + 2 * b) * 2 + c for b in range(2)] for z in range(chips) if z % 4 < 2 for c in range(2)]
    side = tp // 4
    along_y = [[y * 4 + x for y in range(side)] for x in range(4)]
    struct = jax.ShapeDtypeStruct

    def exchange(x, axis):
        return lax.all_to_all(x, axis, split_axis=0, concat_axis=0, tiled=True)

    slots = struct((SLOTS, BLOCK), bf16)
    copies = struct((tp, SLOTS, BLOCK), bf16)
    square = struct((BLOCK, BLOCK), bf16)
    ids = expert_ids.T
    column = lax.axis_index("tp").reshape(1)

    send = call(dispatch_body, 1, 3, slots, 1 << 27, hbm=(1, 2, 3))(
        column, expert_rows, expert_gain[None, :], ids
    )
    routed = exchange(send.reshape(ep, CAP, BLOCK), "ep").reshape(SLOTS, BLOCK)
    outs = (struct((BLOCK, HEAD), bf16), struct((MSG, BLOCK), bf16))
    query, message = call(project_body, 0, 6, outs, 1 << 28, hbm=range(6))(
        attn_rows,
        attn_gain[None, :],
        query_weight.T,
        key_weight.T,
        value_weight.T,
        key_bias,
    )
    swaps = [(k, k ^ 1) for k in range(tp)]
    other_gate = lax.ppermute(gate_weight[0], "tp", swaps)
    other_up = lax.ppermute(up_weight[0], "tp", swaps)
    keys = lax.all_gather(message, "ep", axis=0, tiled=True, axis_index_groups=pairs)
    own = lax.all_gather(keys, "ep", axis=0, tiled=True, axis_index_groups=strided)
    far = lax.ppermute(own, "ep", [(e, e ^ 2) for e in range(ep)])
    routed = call_out(halves_body, 0, 1, struct((tp, ROWS, BLOCK), bf16), 1 << 24, [], tp)(routed)
    routed = exchange(routed, "tp")
    own_hidden = [pltpu.VMEM((SLOTS, BLOCK), bf16)]
    hidden = call_out(hidden_body, 1, 5, copies, 1 << 29, own_hidden, 2 * tp)(
        column, routed, gate_weight[0], up_weight[0], other_gate, other_up
    )
    hidden = exchange(hidden, "tp")
    cores = [(e, e ^ 1) for e in range(ep)]
    own_other = lax.ppermute(own, "ep", cores)
    far_other = lax.ppermute(far, "ep", cores)
    attended = call(attend_body, 1, 5, struct((HEAD, BLOCK), bf16), 1 << 30)(
        here.reshape(1), query, own, own_other, far, far_other
    )
    heads = [attended]
    for d in OFFSETS[1:]:
        moves = [(k - k % 4 + (k + d) % 4, k) for k in range(tp)]
        heads.append(lax.ppermute(attended, "tp", moves))
    stacked = struct((len(heads) * HEAD, BLOCK), bf16)
    attended = call(pack_body, 0, len(heads), stacked, 1 << 20)(*heads)
    result = call(down_body, 0, 2, slots, 1 << 28)(hidden, down_weight[0])
    back = exchange(result.reshape(ep, CAP, BLOCK), "ep").reshape(SLOTS, BLOCK)
    attended = lax.all_gather(attended, "tp", axis=0, tiled=True, axis_index_groups=along_y)
    mixed = call(mix_body, 1, 2, square, 1 << 26)(column, attended, out_weight)
    expert_out = call(combine_body, 0, 4, square, 1 << 27)(ids, group_logits.T, pair_logits.T, back)
    return (mixed, expert_out)


def solution(mesh):
    placed = (
        P("ep", None),
        P(),
        P(None, "tp"),
        P(None, "tp"),
        P(None, "tp"),
        P("tp", "ep"),
        P(None, "tp"),
        P("ep", None),
        P(),
        P("ep", None),
        P("ep", None),
        P("ep", None),
        P("ep", None, "tp"),
        P("ep", None, "tp"),
        P("ep", None, "tp"),
    )
    return jax.shard_map(
        shards,
        mesh=mesh,
        in_specs=placed,
        out_specs=(P("ep", "tp"), P("ep", "tp")),
        check_vma=False,
    )
```

```python
import jax
import jax.numpy as jnp
from jax import lax
from jax.experimental import pallas as pl
from jax.experimental.pallas import tpu as pltpu
from jax.sharding import PartitionSpec as P


EXPERTS = 32
GROUPS = 4
GROUP_SIZE = 8
CAP = 16
BLOCK = 128
HEAD = 64
SLOTS = EXPERTS * CAP
ROWS = SLOTS // 2
MSG = 144
WIDTH = 4
OFFSETS = (0, 1, 3, 2)

epsilon = 1e-06
f32 = jnp.float32
bf16 = jnp.bfloat16
i32 = jnp.int32

SMEM = pl.BlockSpec(memory_space=pltpu.SMEM)


def call(body, n_scalar, n_in, outs, flops, mib=16, hbm=(), **more):
    def run(*args):
        args = [
            pltpu.with_memory_space_constraint(a, pltpu.HBM) if k in hbm else a
            for k, a in enumerate(args)
        ]
        return kernel(*args)

    kernel = pl.pallas_call(
        body,
        out_shape=outs,
        in_specs=[SMEM] * n_scalar + [pl.BlockSpec()] * n_in,
        cost_estimate=pl.CostEstimate(flops=flops, bytes_accessed=1 << 20, transcendentals=0),
        compiler_params=pltpu.CompilerParams(vmem_limit_bytes=mib << 20),
        **more,
    )
    return run


def call_out(body, n_scalar, n_in, out, flops, scratch, copies):
    copies = [pltpu.SemaphoreType.DMA((copies,))]
    more = {"out_specs": pl.BlockSpec(memory_space=pltpu.HBM), "scratch_shapes": scratch + copies}
    return call(body, n_scalar, n_in, pltpu.HBM(out.shape, out.dtype), flops, **more)


def nn(a, b):
    return lax.dot_general(a, b, (((1,), (0,)), ((), ())), preferred_element_type=f32)


def nt(a, b):
    return lax.dot_general(a, b, (((1,), (1,)), ((), ())), preferred_element_type=f32)


def iota(shape, dim):
    return lax.broadcasted_iota(i32, shape, dim)


def ones_where(mask):
    return jnp.where(mask, 1.0, 0.0).astype(f32)


def places(first, second):
    expert = iota((EXPERTS, BLOCK), 0)
    mark0 = ones_where(first == expert)
    mark1 = ones_where(second == expert)
    earlier = ones_where(iota((BLOCK, BLOCK), 0) < iota((BLOCK, BLOCK), 1)).astype(bf16)
    before = nn((mark0 + mark1).astype(bf16), earlier)
    place0 = jnp.sum(mark0 * before, axis=0, keepdims=True)
    place1 = jnp.sum(mark1 * before, axis=0, keepdims=True)
    return place0.astype(i32), place1.astype(i32)


def dispatch_body(tp_ref, rows_ref, gain_ref, ids_ref, out_ref):
    x = rows_ref[...].astype(f32)
    inv = lax.rsqrt(jnp.mean(x * x, axis=-1, keepdims=True) + epsilon)
    at = pl.multiple_of(tp_ref[0] * BLOCK, BLOCK)
    own = rows_ref[:, pl.ds(at, BLOCK)].astype(f32)
    own = (own * inv * gain_ref[:, pl.ds(at, BLOCK)]).astype(bf16)
    ids = ids_ref[...]
    first, second = ids[0:1, :], ids[1:2, :]
    place0, place1 = places(first, second)
    slot = iota((SLOTS, BLOCK), 0)
    hit = (slot == first * CAP + place0) | (slot == second * CAP + place1)
    out_ref[...] = nn(ones_where(hit).astype(bf16), own).astype(bf16)


def project_body(rows_ref, gain_ref, wq_ref, wk_ref, wv_ref, bias_ref, q_ref, msg_ref):
    x = rows_ref[...].astype(f32)
    inv = lax.rsqrt(jnp.mean(x * x, axis=-1, keepdims=True) + epsilon)
    normed = (x * inv * gain_ref[...]).astype(bf16)
    q = nt(normed, wq_ref[...]).astype(bf16)
    q_ref[...] = (q.astype(f32) * (HEAD**-0.5)).astype(bf16)
    kv = jnp.concatenate([wk_ref[...], wv_ref[...]], axis=0)
    msg_ref[0:BLOCK, :] = nt(kv, normed).astype(bf16)
    msg_ref[BLOCK:MSG, :] = jnp.broadcast_to(bias_ref[...], (MSG - BLOCK, BLOCK))


def halves_body(x_ref, out_ref, sems):
    copies = []
    for k in range(out_ref.shape[0]):
        half = k % 2
        source = x_ref.at[half * ROWS : (half + 1) * ROWS, :]
        copies.append(pltpu.make_async_copy(source, out_ref.at[k], sems.at[k]))
        copies[-1].start()
    for copy in copies:
        copy.wait()


def hidden_body(tp_ref, x_ref, g0_ref, u0_ref, g1_ref, u1_ref, out_ref, hidden_ref, sems):
    parts = x_ref.shape[0]
    even = tp_ref[0] % 2 == 0
    own_weights = jnp.concatenate([g0_ref[...], u0_ref[...]], axis=1)
    other_weights = jnp.concatenate([g1_ref[...], u1_ref[...]], axis=1)

    def gated(both):
        gate, up = both[:, :BLOCK], both[:, BLOCK:]
        return gate * jax.nn.sigmoid(gate) * up

    copies = []
    for m in range(2):
        x = [x_ref[k, m * BLOCK : (m + 1) * BLOCK, :] for k in range(parts)]
        x = jnp.concatenate(x, axis=1)
        own, other = gated(nn(x, own_weights)), gated(nn(x, other_weights))
        span = slice(m * ROWS, (m + 1) * ROWS)
        hidden_ref[m * ROWS : m * ROWS + BLOCK, :] = jnp.where(even, own, other).astype(bf16)
        hidden_ref[m * ROWS + BLOCK : (m + 1) * ROWS, :] = jnp.where(even, other, own).astype(bf16)
        for k in range(parts):
            target = out_ref.at[k, span, :]
            copies.append(
                pltpu.make_async_copy(hidden_ref.at[span, :], target, sems.at[m * parts + k])
            )
            copies[-1].start()
    for copy in copies:
        copy.wait()


def down_body(x_ref, w_ref, out_ref):
    parts = x_ref.shape[0]
    rows = []
    for half in range(2):
        for m in range(2):
            at = m * ROWS
            pieces = [
                x_ref[k, at + e * BLOCK : at + (e + 1) * BLOCK, :]
                for k in range(half, parts, 2)
                for e in range(2)
            ]
            rows.append(jnp.concatenate(pieces, axis=1))
    out_ref[...] = nn(jnp.concatenate(rows, axis=0), w_ref[...]).astype(bf16)


def attend_body(pos_ref, q_ref, own_ref, other_ref, far_ref, far_other_ref, out_ref):
    here = pos_ref[0]
    core = here % 2
    chips = 2 * own_ref.shape[0] // MSG
    odd = (here // 2) % 2
    q = q_ref[...]
    wide = (2 * BLOCK, 2 * BLOCK)
    row, col = iota(wide, 0), iota(wide, 1)
    row = jnp.where(row >= BLOCK, row - BLOCK, row)
    tail = ones_where((col >= BLOCK) | (row >= col)).astype(bf16)
    t, s = iota((BLOCK, BLOCK), 0), iota((BLOCK, BLOCK), 1)

    offset = s - t

    def step(k, carry):
        later, total = carry
        messages, starts = [], []
        for w in range(WIDTH):
            z = chips - 1 - (k * WIDTH + w)
            at = pl.ds(pl.multiple_of((z // 2) * MSG, 16), MSG)
            near = odd == (WIDTH - 1 - w) % 2
            own = jnp.where(near, own_ref[at, :], far_ref[at, :])
            other = jnp.where(near, other_ref[at, :], far_other_ref[at, :])
            messages += [jnp.where(core == 1, own, other), jnp.where(core == 1, other, own)]
            starts += [(here - 2 * z - 1) * BLOCK, (here - 2 * z) * BLOCK]
        scores = [nn(q, m[0:HEAD, :]) + m[BLOCK : BLOCK + 1, :].astype(f32) for m in messages]
        causal = [offset < start for start in starts]
        logs = [jnp.log(1.0 + jnp.exp(-jnp.abs(x))) for x in scores]
        keep = [-(jnp.maximum(x, 0.0) + y) for x, y in zip(scores, logs)]
        keep = [jnp.where(c, x, 0.0) for c, x in zip(causal, keep)]
        high = [x.astype(bf16) for x in keep]
        low = [(x - y.astype(f32)).astype(bf16) for x, y in zip(keep, high)]
        sums = [nn(jnp.concatenate([x, y], axis=1), tail) for x, y in zip(high, low)]
        weights = [jnp.exp(x + y[:, :BLOCK]) for x, y in zip(scores, sums)]
        weights = [jnp.where(c, x, 0.0).astype(bf16) for c, x in zip(causal, weights)]
        outs = [nt(x, m[HEAD:BLOCK, :]) for x, m in zip(weights, messages)]
        for x, y in zip(outs, sums):
            total = total + jnp.exp(later) * x
            later = later + y[:, BLOCK : BLOCK + HEAD]
        return later, total

    zeros = jnp.zeros((BLOCK, HEAD), f32)
    _, total = lax.fori_loop(0, chips // WIDTH, step, (zeros, zeros))
    out_ref[...] = jnp.transpose(total).astype(bf16)


def pack_body(*refs):
    for k, ref in enumerate(refs[:-1]):
        refs[-1][k * HEAD : (k + 1) * HEAD, :] = ref[...]


def mix_body(tp_ref, x_ref, w_ref, out_ref):
    column = tp_ref[0] % 4
    weights = []
    for k in range(x_ref.shape[0] // HEAD):
        head = k - k % 4 + (column + OFFSETS[k % 4]) % 4
        weights.append(w_ref[pl.ds(pl.multiple_of(head * HEAD, HEAD), HEAD), :])
    x = jnp.transpose(x_ref[...].astype(f32)).astype(bf16)
    out_ref[...] = nn(x, jnp.concatenate(weights, axis=0)).astype(bf16)


def plan_body(ids_ref, group_ref, pair_ref, pick_ref, table_ref):
    ids = ids_ref[...]
    first, second = ids[0:1, :], ids[1:2, :]
    place0, place1 = places(first, second)
    shares = jnp.exp(group_ref[...])
    shares = shares / jnp.sum(shares, axis=0, keepdims=True)
    group = iota((GROUPS, BLOCK), 0)
    chosen0 = jnp.sum(jnp.where(first // GROUP_SIZE == group, shares, 0.0), axis=0, keepdims=True)
    chosen1 = jnp.sum(jnp.where(second // GROUP_SIZE == group, shares, 0.0), axis=0, keepdims=True)
    spread = pair_ref[0:1, :] - pair_ref[1:2, :]
    weight0 = chosen0 * jax.nn.sigmoid(spread)
    weight1 = chosen1 * jax.nn.sigmoid(-spread)
    slots = [(first * CAP + place0).astype(f32), (second * CAP + place1).astype(f32)]
    table = jnp.concatenate(slots + [weight0, weight1], axis=0)
    table = jnp.concatenate([table, jnp.zeros((BLOCK - 4, BLOCK), f32)], axis=0)
    table = jnp.transpose(table)
    slot = iota((BLOCK, SLOTS), 1)
    for k in range(2):
        hit = ones_where(slot == table[:, k : k + 1].astype(i32))
        pick_ref[k * BLOCK : (k + 1) * BLOCK, :] = hit.astype(bf16)
    table_ref[...] = table


def combine_body(pick_ref, table_ref, back_ref, out_ref):
    both = nn(pick_ref[...], back_ref[...])
    out = table_ref[:, 2:3] * both[:BLOCK] + table_ref[:, 3:4] * both[BLOCK:]
    out_ref[...] = out.astype(bf16)


def shards(
    attn_rows,
    attn_gain,
    query_weight,
    key_weight,
    value_weight,
    key_bias,
    out_weight,
    expert_rows,
    expert_gain,
    expert_ids,
    group_logits,
    pair_logits,
    gate_weight,
    up_weight,
    down_weight,
):
    ep, tp = lax.axis_size("ep"), lax.axis_size("tp")
    chips = ep // 2
    here = lax.axis_index("ep")
    run = chips // 4
    strided = [[(m + 4 * k) * 2 + c for k in range(run)] for m in range(4) for c in range(2)]
    pairs = [[(z + 2 * b) * 2 + c for b in range(2)] for z in range(chips) if z % 4 < 2 for c in range(2)]
    side = tp // 4
    along_y = [[y * 4 + x for y in range(side)] for x in range(4)]
    struct = jax.ShapeDtypeStruct

    def exchange(x, axis):
        return lax.all_to_all(x, axis, split_axis=0, concat_axis=0, tiled=True)

    slots = struct((SLOTS, BLOCK), bf16)
    copies = struct((tp, SLOTS, BLOCK), bf16)
    square = struct((BLOCK, BLOCK), bf16)
    ids = expert_ids.T
    column = lax.axis_index("tp").reshape(1)

    send = call(dispatch_body, 1, 3, slots, 1 << 27, hbm=(1, 2, 3))(
        column, expert_rows, expert_gain[None, :], ids
    )
    routed = exchange(send.reshape(ep, CAP, BLOCK), "ep").reshape(SLOTS, BLOCK)
    outs = (struct((BLOCK, HEAD), bf16), struct((MSG, BLOCK), bf16))
    query, message = call(project_body, 0, 6, outs, 1 << 28, hbm=range(6))(
        attn_rows,
        attn_gain[None, :],
        query_weight.T,
        key_weight.T,
        value_weight.T,
        key_bias,
    )
    swaps = [(k, k ^ 1) for k in range(tp)]
    other_gate = lax.ppermute(gate_weight[0], "tp", swaps)
    other_up = lax.ppermute(up_weight[0], "tp", swaps)
    keys = lax.all_gather(message, "ep", axis=0, tiled=True, axis_index_groups=pairs)
    own = lax.all_gather(keys, "ep", axis=0, tiled=True, axis_index_groups=strided)
    far = lax.ppermute(own, "ep", [(e, e ^ 2) for e in range(ep)])
    routed = call_out(halves_body, 0, 1, struct((tp, ROWS, BLOCK), bf16), 1 << 24, [], tp)(routed)
    routed = exchange(routed, "tp")
    own_hidden = [pltpu.VMEM((SLOTS, BLOCK), bf16)]
    hidden = call_out(hidden_body, 1, 5, copies, 1 << 29, own_hidden, 2 * tp)(
        column, routed, gate_weight[0], up_weight[0], other_gate, other_up
    )
    hidden = exchange(hidden, "tp")
    cores = [(e, e ^ 1) for e in range(ep)]
    own_other = lax.ppermute(own, "ep", cores)
    far_other = lax.ppermute(far, "ep", cores)
    attended = call(attend_body, 1, 5, struct((HEAD, BLOCK), bf16), 1 << 30)(
        here.reshape(1), query, own, own_other, far, far_other
    )
    heads = [attended]
    for d in OFFSETS[1:]:
        moves = [(k - k % 4 + (k + d) % 4, k) for k in range(tp)]
        heads.append(lax.ppermute(attended, "tp", moves))
    stacked = struct((len(heads) * HEAD, BLOCK), bf16)
    attended = call(pack_body, 0, len(heads), stacked, 1 << 20)(*heads)
    result = call(down_body, 0, 2, slots, 1 << 28)(hidden, down_weight[0])
    back = exchange(result.reshape(ep, CAP, BLOCK), "ep").reshape(SLOTS, BLOCK)
    tables = (struct((2 * BLOCK, SLOTS), bf16), struct((BLOCK, BLOCK), f32))
    picks, table = call(plan_body, 0, 3, tables, 1 << 26)(ids, group_logits.T, pair_logits.T)
    attended = lax.all_gather(attended, "tp", axis=0, tiled=True, axis_index_groups=along_y)
    mixed = call(mix_body, 1, 2, square, 1 << 26)(column, attended, out_weight)
    expert_out = call(combine_body, 0, 3, square, 1 << 27)(picks, table, back)
    return (mixed, expert_out)


def solution(mesh):
    placed = (
        P("ep", None),
        P(),
        P(None, "tp"),
        P(None, "tp"),
        P(None, "tp"),
        P("tp", "ep"),
        P(None, "tp"),
        P("ep", None),
        P(),
        P("ep", None),
        P("ep", None),
        P("ep", None),
        P("ep", None, "tp"),
        P("ep", None, "tp"),
        P("ep", None, "tp"),
    )
    return jax.shard_map(
        shards,
        mesh=mesh,
        in_specs=placed,
        out_specs=(P("ep", "tp"), P("ep", "tp")),
        check_vma=False,
    )
```

```python
import jax
import jax.numpy as jnp
from jax import lax
from jax.experimental import pallas as pl
from jax.experimental.pallas import tpu as pltpu
from jax.sharding import PartitionSpec as P


EXPERTS = 32
GROUPS = 4
GROUP_SIZE = 8
CAP = 16
BLOCK = 128
HEAD = 64
SLOTS = EXPERTS * CAP
ROWS = SLOTS // 2
MSG = 144
WIDTH = 4
OFFSETS = (0, 1, 3, 2)

epsilon = 1e-06
f32 = jnp.float32
bf16 = jnp.bfloat16
i32 = jnp.int32

SMEM = pl.BlockSpec(memory_space=pltpu.SMEM)


def call(body, n_scalar, n_in, outs, flops, mib=16, hbm=(), **more):
    def run(*args):
        args = [
            pltpu.with_memory_space_constraint(a, pltpu.HBM) if k in hbm else a
            for k, a in enumerate(args)
        ]
        return kernel(*args)

    kernel = pl.pallas_call(
        body,
        out_shape=outs,
        in_specs=[SMEM] * n_scalar + [pl.BlockSpec()] * n_in,
        cost_estimate=pl.CostEstimate(flops=flops, bytes_accessed=1 << 20, transcendentals=0),
        compiler_params=pltpu.CompilerParams(vmem_limit_bytes=mib << 20),
        **more,
    )
    return run


def call_out(body, n_scalar, n_in, out, flops, scratch, copies):
    copies = [pltpu.SemaphoreType.DMA((copies,))]
    more = {"out_specs": pl.BlockSpec(memory_space=pltpu.HBM), "scratch_shapes": scratch + copies}
    return call(body, n_scalar, n_in, pltpu.HBM(out.shape, out.dtype), flops, **more)


def nn(a, b):
    return lax.dot_general(a, b, (((1,), (0,)), ((), ())), preferred_element_type=f32)


def nt(a, b):
    return lax.dot_general(a, b, (((1,), (1,)), ((), ())), preferred_element_type=f32)


def iota(shape, dim):
    return lax.broadcasted_iota(i32, shape, dim)


def ones_where(mask):
    return jnp.where(mask, 1.0, 0.0).astype(f32)


def places(first, second):
    expert = iota((EXPERTS, BLOCK), 0)
    mark0 = ones_where(first == expert)
    mark1 = ones_where(second == expert)
    earlier = ones_where(iota((BLOCK, BLOCK), 0) < iota((BLOCK, BLOCK), 1)).astype(bf16)
    before = nn((mark0 + mark1).astype(bf16), earlier)
    place0 = jnp.sum(mark0 * before, axis=0, keepdims=True)
    place1 = jnp.sum(mark1 * before, axis=0, keepdims=True)
    return place0.astype(i32), place1.astype(i32)


def dispatch_body(tp_ref, rows_ref, gain_ref, ids_ref, out_ref):
    x = rows_ref[...].astype(f32)
    inv = lax.rsqrt(jnp.mean(x * x, axis=-1, keepdims=True) + epsilon)
    at = pl.multiple_of(tp_ref[0] * BLOCK, BLOCK)
    own = rows_ref[:, pl.ds(at, BLOCK)].astype(f32)
    own = (own * inv * gain_ref[:, pl.ds(at, BLOCK)]).astype(bf16)
    ids = ids_ref[...]
    first, second = ids[0:1, :], ids[1:2, :]
    place0, place1 = places(first, second)
    slot = iota((SLOTS, BLOCK), 0)
    hit = (slot == first * CAP + place0) | (slot == second * CAP + place1)
    out_ref[...] = nn(ones_where(hit).astype(bf16), own).astype(bf16)


def project_body(rows_ref, gain_ref, wq_ref, wk_ref, wv_ref, bias_ref, q_ref, msg_ref):
    x = rows_ref[...].astype(f32)
    inv = lax.rsqrt(jnp.mean(x * x, axis=-1, keepdims=True) + epsilon)
    normed = (x * inv * gain_ref[...]).astype(bf16)
    q = nt(normed, wq_ref[...]).astype(bf16)
    q_ref[...] = (q.astype(f32) * (HEAD**-0.5)).astype(bf16)
    kv = jnp.concatenate([wk_ref[...], wv_ref[...]], axis=0)
    msg_ref[0:BLOCK, :] = nt(kv, normed).astype(bf16)
    msg_ref[BLOCK:MSG, :] = jnp.broadcast_to(bias_ref[...], (MSG - BLOCK, BLOCK))


def halves_body(x_ref, out_ref, sems):
    copies = []
    for k in range(out_ref.shape[0]):
        half = k % 2
        source = x_ref.at[half * ROWS : (half + 1) * ROWS, :]
        copies.append(pltpu.make_async_copy(source, out_ref.at[k], sems.at[k]))
        copies[-1].start()
    for copy in copies:
        copy.wait()


def hidden_body(x_ref, g0_ref, u0_ref, g1_ref, u1_ref, out_ref, hidden_ref, sems):
    parts = x_ref.shape[0]
    x = jnp.concatenate([x_ref[k] for k in range(parts)], axis=1)
    copies = []
    for m, (g_ref, u_ref) in enumerate(((g0_ref, u0_ref), (g1_ref, u1_ref))):
        both = nn(x, jnp.concatenate([g_ref[...], u_ref[...]], axis=1))
        gate, up = both[:, :BLOCK], both[:, BLOCK:]
        span = slice(m * ROWS, (m + 1) * ROWS)
        hidden_ref[span, :] = (gate * jax.nn.sigmoid(gate) * up).astype(bf16)
        for k in range(parts):
            target = out_ref.at[k, span, :]
            copies.append(
                pltpu.make_async_copy(hidden_ref.at[span, :], target, sems.at[m * parts + k])
            )
            copies[-1].start()
    for copy in copies:
        copy.wait()


def down_body(x_ref, w_ref, out_ref):
    parts = x_ref.shape[0]
    rows = []
    for half in range(2):
        pieces = []
        for k in range(half, parts, 2):
            own, other = x_ref[k, 0:ROWS, :], x_ref[k, ROWS:SLOTS, :]
            pieces += [own, other] if half == 0 else [other, own]
        rows.append(jnp.concatenate(pieces, axis=1))
    out_ref[...] = nn(jnp.concatenate(rows, axis=0), w_ref[...]).astype(bf16)


def order_body(pos_ref, own_ref, other_ref, out_ref):
    core = pos_ref[0] % 2
    own, other = own_ref[...], other_ref[...]
    rows = own.shape[0]
    out_ref[0:rows, :] = jnp.where(core == 1, own, other)
    out_ref[rows:, :] = jnp.where(core == 1, other, own)


def attend_body(pos_ref, q_ref, near_ref, far_ref, far_other_ref, out_ref):
    here = pos_ref[0]
    core = here % 2
    rows = far_ref.shape[0]
    chips = 2 * rows // MSG
    odd = (here // 2) % 2
    q = q_ref[...]
    wide = (2 * BLOCK, 2 * BLOCK)
    row, col = iota(wide, 0), iota(wide, 1)
    row = jnp.where(row >= BLOCK, row - BLOCK, row)
    tail = ones_where((col >= BLOCK) | (row >= col)).astype(bf16)
    t, s = iota((BLOCK, BLOCK), 0), iota((BLOCK, BLOCK), 1)

    offset = s - t

    def step(k, carry):
        later, total = carry
        messages, starts = [], []
        for w in range(WIDTH):
            z = chips - 1 - (k * WIDTH + w)
            at = pl.multiple_of((z // 2) * MSG, 16)
            near = odd == (WIDTH - 1 - w) % 2
            far, other = far_ref[pl.ds(at, MSG), :], far_other_ref[pl.ds(at, MSG), :]
            upper = jnp.where(core == 1, far, other)
            lower = jnp.where(core == 1, other, far)
            messages.append(jnp.where(near, near_ref[pl.ds(at, MSG), :], upper))
            messages.append(jnp.where(near, near_ref[pl.ds(rows + at, MSG), :], lower))
            starts += [(here - 2 * z - 1) * BLOCK, (here - 2 * z) * BLOCK]
        scores = [nn(q, m[0:HEAD, :]) + m[BLOCK : BLOCK + 1, :].astype(f32) for m in messages]
        causal = [offset < start for start in starts]
        logs = [jnp.log(1.0 + jnp.exp(-jnp.abs(x))) for x in scores]
        keep = [-(jnp.maximum(x, 0.0) + y) for x, y in zip(scores, logs)]
        keep = [jnp.where(c, x, 0.0) for c, x in zip(causal, keep)]
        high = [x.astype(bf16) for x in keep]
        low = [(x - y.astype(f32)).astype(bf16) for x, y in zip(keep, high)]
        sums = [nn(jnp.concatenate([x, y], axis=1), tail) for x, y in zip(high, low)]
        weights = [jnp.exp(x + y[:, :BLOCK]) for x, y in zip(scores, sums)]
        weights = [jnp.where(c, x, 0.0).astype(bf16) for c, x in zip(causal, weights)]
        outs = [nt(x, m[HEAD:BLOCK, :]) for x, m in zip(weights, messages)]
        for x, y in zip(outs, sums):
            total = total + jnp.exp(later) * x
            later = later + y[:, BLOCK : BLOCK + HEAD]
        return later, total

    zeros = jnp.zeros((BLOCK, HEAD), f32)
    _, total = lax.fori_loop(0, chips // WIDTH, step, (zeros, zeros))
    out_ref[...] = jnp.transpose(total).astype(bf16)


def pack_body(*refs):
    for k, ref in enumerate(refs[:-1]):
        refs[-1][k * HEAD : (k + 1) * HEAD, :] = ref[...]


def mix_body(tp_ref, x_ref, w_ref, out_ref):
    column = tp_ref[0] % 4
    weights = []
    for k in range(x_ref.shape[0] // HEAD):
        head = k - k % 4 + (column + OFFSETS[k % 4]) % 4
        weights.append(w_ref[pl.ds(pl.multiple_of(head * HEAD, HEAD), HEAD), :])
    x = jnp.transpose(x_ref[...].astype(f32)).astype(bf16)
    out_ref[...] = nn(x, jnp.concatenate(weights, axis=0)).astype(bf16)


def plan_body(ids_ref, group_ref, pair_ref, pick_ref, table_ref):
    ids = ids_ref[...]
    first, second = ids[0:1, :], ids[1:2, :]
    place0, place1 = places(first, second)
    shares = jnp.exp(group_ref[...])
    shares = shares / jnp.sum(shares, axis=0, keepdims=True)
    group = iota((GROUPS, BLOCK), 0)
    chosen0 = jnp.sum(jnp.where(first // GROUP_SIZE == group, shares, 0.0), axis=0, keepdims=True)
    chosen1 = jnp.sum(jnp.where(second // GROUP_SIZE == group, shares, 0.0), axis=0, keepdims=True)
    spread = pair_ref[0:1, :] - pair_ref[1:2, :]
    weight0 = chosen0 * jax.nn.sigmoid(spread)
    weight1 = chosen1 * jax.nn.sigmoid(-spread)
    slots = [(first * CAP + place0).astype(f32), (second * CAP + place1).astype(f32)]
    table = jnp.concatenate(slots + [weight0, weight1], axis=0)
    table = jnp.concatenate([table, jnp.zeros((BLOCK - 4, BLOCK), f32)], axis=0)
    table = jnp.transpose(table)
    slot = iota((BLOCK, SLOTS), 1)
    for k in range(2):
        hit = ones_where(slot == table[:, k : k + 1].astype(i32))
        pick_ref[k * BLOCK : (k + 1) * BLOCK, :] = hit.astype(bf16)
    table_ref[...] = table


def combine_body(pick_ref, table_ref, back_ref, out_ref):
    both = nn(pick_ref[...], back_ref[...])
    out = table_ref[:, 2:3] * both[:BLOCK] + table_ref[:, 3:4] * both[BLOCK:]
    out_ref[...] = out.astype(bf16)


def shards(
    attn_rows,
    attn_gain,
    query_weight,
    key_weight,
    value_weight,
    key_bias,
    out_weight,
    expert_rows,
    expert_gain,
    expert_ids,
    group_logits,
    pair_logits,
    gate_weight,
    up_weight,
    down_weight,
):
    ep, tp = lax.axis_size("ep"), lax.axis_size("tp")
    chips = ep // 2
    here = lax.axis_index("ep")
    run = chips // 4
    strided = [[(m + 4 * k) * 2 + c for k in range(run)] for m in range(4) for c in range(2)]
    pairs = [[(z + 2 * b) * 2 + c for b in range(2)] for z in range(chips) if z % 4 < 2 for c in range(2)]
    side = tp // 4
    along_y = [[y * 4 + x for y in range(side)] for x in range(4)]
    struct = jax.ShapeDtypeStruct

    def exchange(x, axis):
        return lax.all_to_all(x, axis, split_axis=0, concat_axis=0, tiled=True)

    slots = struct((SLOTS, BLOCK), bf16)
    copies = struct((tp, SLOTS, BLOCK), bf16)
    square = struct((BLOCK, BLOCK), bf16)
    ids = expert_ids.T
    column = lax.axis_index("tp").reshape(1)

    send = call(dispatch_body, 1, 3, slots, 1 << 27, hbm=(1, 2, 3))(
        column, expert_rows, expert_gain[None, :], ids
    )
    routed = exchange(send.reshape(ep, CAP, BLOCK), "ep").reshape(SLOTS, BLOCK)
    outs = (struct((BLOCK, HEAD), bf16), struct((MSG, BLOCK), bf16))
    query, message = call(project_body, 0, 6, outs, 1 << 28, hbm=range(6))(
        attn_rows,
        attn_gain[None, :],
        query_weight.T,
        key_weight.T,
        value_weight.T,
        key_bias,
    )
    swaps = [(k, k ^ 1) for k in range(tp)]
    other_gate = lax.ppermute(gate_weight[0], "tp", swaps)
    other_up = lax.ppermute(up_weight[0], "tp", swaps)
    keys = lax.all_gather(message, "ep", axis=0, tiled=True, axis_index_groups=pairs)
    own = lax.all_gather(keys, "ep", axis=0, tiled=True, axis_index_groups=strided)
    far = lax.ppermute(own, "ep", [(e, e ^ 2) for e in range(ep)])
    routed = call_out(halves_body, 0, 1, struct((tp, ROWS, BLOCK), bf16), 1 << 24, [], tp)(routed)
    routed = exchange(routed, "tp")
    own_hidden = [pltpu.VMEM((SLOTS, BLOCK), bf16)]
    hidden = call_out(hidden_body, 0, 5, copies, 1 << 29, own_hidden, 2 * tp)(
        routed, gate_weight[0], up_weight[0], other_gate, other_up
    )
    hidden = exchange(hidden, "tp")
    cores = [(e, e ^ 1) for e in range(ep)]
    own_other = lax.ppermute(own, "ep", cores)
    ordered = struct((2 * own.shape[0], BLOCK), bf16)
    near = call(order_body, 1, 2, ordered, 1 << 22)(here.reshape(1), own, own_other)
    far_other = lax.ppermute(far, "ep", cores)
    attended = call(attend_body, 1, 4, struct((HEAD, BLOCK), bf16), 1 << 30)(
        here.reshape(1), query, near, far, far_other
    )
    heads = [attended]
    for d in OFFSETS[1:]:
        moves = [(k - k % 4 + (k + d) % 4, k) for k in range(tp)]
        heads.append(lax.ppermute(attended, "tp", moves))
    stacked = struct((len(heads) * HEAD, BLOCK), bf16)
    attended = call(pack_body, 0, len(heads), stacked, 1 << 20)(*heads)
    result = call(down_body, 0, 2, slots, 1 << 28)(hidden, down_weight[0])
    back = exchange(result.reshape(ep, CAP, BLOCK), "ep").reshape(SLOTS, BLOCK)
    tables = (struct((2 * BLOCK, SLOTS), bf16), struct((BLOCK, BLOCK), f32))
    picks, table = call(plan_body, 0, 3, tables, 1 << 26)(ids, group_logits.T, pair_logits.T)
    attended = lax.all_gather(attended, "tp", axis=0, tiled=True, axis_index_groups=along_y)
    mixed = call(mix_body, 1, 2, square, 1 << 26)(column, attended, out_weight)
    expert_out = call(combine_body, 0, 3, square, 1 << 27)(picks, table, back)
    return (mixed, expert_out)


def solution(mesh):
    placed = (
        P("ep", None),
        P(),
        P(None, "tp"),
        P(None, "tp"),
        P(None, "tp"),
        P("tp", "ep"),
        P(None, "tp"),
        P("ep", None),
        P(),
        P("ep", None),
        P("ep", None),
        P("ep", None),
        P("ep", None, "tp"),
        P("ep", None, "tp"),
        P("ep", None, "tp"),
    )
    return jax.shard_map(
        shards,
        mesh=mesh,
        in_specs=placed,
        out_specs=(P("ep", "tp"), P("ep", "tp")),
        check_vma=False,
    )
```

```python
import jax
import jax.numpy as jnp
from jax import lax
from jax.experimental import pallas as pl
from jax.experimental.pallas import tpu as pltpu
from jax.sharding import PartitionSpec as P


EXPERTS = 32
GROUPS = 4
GROUP_SIZE = 8
CAP = 16
BLOCK = 128
HEAD = 64
SLOTS = EXPERTS * CAP
ROWS = SLOTS // 2
MSG = 144
WIDTH = 4
PARTS = 4
OFFSETS = (0, 1, 3, 2)

epsilon = 1e-06
f32 = jnp.float32
bf16 = jnp.bfloat16
i32 = jnp.int32

SMEM = pl.BlockSpec(memory_space=pltpu.SMEM)


def call(body, n_scalar, n_in, outs, flops, mib=16, hbm=(), own=None, **more):
    def run(*args):
        args = [
            pltpu.with_memory_space_constraint(a, pltpu.HBM) if k in hbm else a
            for k, a in enumerate(args)
        ]
        return kernel(*args)

    raw = pl.BlockSpec(memory_space=pltpu.HBM)
    kernel = pl.pallas_call(
        body,
        out_shape=outs,
        in_specs=[SMEM] * n_scalar + [raw if k == own else pl.BlockSpec() for k in range(n_in)],
        cost_estimate=pl.CostEstimate(flops=flops, bytes_accessed=1 << 20, transcendentals=0),
        compiler_params=pltpu.CompilerParams(vmem_limit_bytes=mib << 20),
        **more,
    )
    return run


def call_out(body, n_scalar, n_in, out, flops, scratch, copies):
    copies = [pltpu.SemaphoreType.DMA((copies,))]
    more = {"out_specs": pl.BlockSpec(memory_space=pltpu.HBM), "scratch_shapes": scratch + copies}
    return call(body, n_scalar, n_in, pltpu.HBM(out.shape, out.dtype), flops, **more)


def nn(a, b):
    return lax.dot_general(a, b, (((1,), (0,)), ((), ())), preferred_element_type=f32)


def nt(a, b):
    return lax.dot_general(a, b, (((1,), (1,)), ((), ())), preferred_element_type=f32)


def iota(shape, dim):
    return lax.broadcasted_iota(i32, shape, dim)


def ones_where(mask):
    return jnp.where(mask, 1.0, 0.0).astype(f32)


def places(first, second):
    expert = iota((EXPERTS, BLOCK), 0)
    mark0 = ones_where(first == expert)
    mark1 = ones_where(second == expert)
    earlier = ones_where(iota((BLOCK, BLOCK), 0) < iota((BLOCK, BLOCK), 1)).astype(bf16)
    before = nn((mark0 + mark1).astype(bf16), earlier)
    place0 = jnp.sum(mark0 * before, axis=0, keepdims=True)
    place1 = jnp.sum(mark1 * before, axis=0, keepdims=True)
    return place0.astype(i32), place1.astype(i32)


def dispatch_body(tp_ref, rows_ref, gain_ref, ids_ref, out_ref, x_ref, sems):
    part = BLOCK // PARTS
    copies = []
    for k in range(PARTS):
        span = slice(k * part, (k + 1) * part)
        copies.append(pltpu.make_async_copy(rows_ref.at[span, :], x_ref.at[span, :], sems.at[k]))
        copies[-1].start()
    ids = ids_ref[...]
    first, second = ids[0:1, :], ids[1:2, :]
    place0, place1 = places(first, second)
    slot = iota((SLOTS, BLOCK), 0)
    hit = (slot == first * CAP + place0) | (slot == second * CAP + place1)
    hit = ones_where(hit).astype(bf16)
    at = pl.multiple_of(tp_ref[0] * BLOCK, BLOCK)
    gain = gain_ref[:, pl.ds(at, BLOCK)]
    owns = []
    for k in range(PARTS):
        copies[k].wait()
        span = slice(k * part, (k + 1) * part)
        x = x_ref[span, :].astype(f32)
        inv = lax.rsqrt(jnp.mean(x * x, axis=-1, keepdims=True) + epsilon)
        own = x_ref[span, pl.ds(at, BLOCK)].astype(f32)
        owns.append((own * inv * gain).astype(bf16))
    out_ref[...] = nn(hit, jnp.concatenate(owns, axis=0)).astype(bf16)


def project_body(rows_ref, gain_ref, wq_ref, wk_ref, wv_ref, bias_ref, q_ref, msg_ref):
    x = rows_ref[...].astype(f32)
    inv = lax.rsqrt(jnp.mean(x * x, axis=-1, keepdims=True) + epsilon)
    normed = (x * inv * gain_ref[...]).astype(bf16)
    q = nt(normed, wq_ref[...]).astype(bf16)
    q_ref[...] = (q.astype(f32) * (HEAD**-0.5)).astype(bf16)
    kv = jnp.concatenate([wk_ref[...], wv_ref[...]], axis=0)
    msg_ref[0:BLOCK, :] = nt(kv, normed).astype(bf16)
    msg_ref[BLOCK:MSG, :] = jnp.broadcast_to(bias_ref[...], (MSG - BLOCK, BLOCK))


def halves_body(x_ref, out_ref, sems):
    copies = []
    for k in range(out_ref.shape[0]):
        half = k % 2
        source = x_ref.at[half * ROWS : (half + 1) * ROWS, :]
        copies.append(pltpu.make_async_copy(source, out_ref.at[k], sems.at[k]))
        copies[-1].start()
    for copy in copies:
        copy.wait()


def hidden_body(x_ref, g0_ref, u0_ref, g1_ref, u1_ref, out_ref, hidden_ref, sems):
    parts = x_ref.shape[0]
    x = jnp.concatenate([x_ref[k] for k in range(parts)], axis=1)
    copies = []
    for m, (g_ref, u_ref) in enumerate(((g0_ref, u0_ref), (g1_ref, u1_ref))):
        both = nn(x, jnp.concatenate([g_ref[...], u_ref[...]], axis=1))
        gate, up = both[:, :BLOCK], both[:, BLOCK:]
        span = slice(m * ROWS, (m + 1) * ROWS)
        hidden_ref[span, :] = (gate * jax.nn.sigmoid(gate) * up).astype(bf16)
        for k in range(parts):
            target = out_ref.at[k, span, :]
            copies.append(
                pltpu.make_async_copy(hidden_ref.at[span, :], target, sems.at[m * parts + k])
            )
            copies[-1].start()
    for copy in copies:
        copy.wait()


def down_body(x_ref, w_ref, out_ref):
    parts = x_ref.shape[0]
    rows = []
    for half in range(2):
        pieces = []
        for k in range(half, parts, 2):
            own, other = x_ref[k, 0:ROWS, :], x_ref[k, ROWS:SLOTS, :]
            pieces += [own, other] if half == 0 else [other, own]
        rows.append(jnp.concatenate(pieces, axis=1))
    out_ref[...] = nn(jnp.concatenate(rows, axis=0), w_ref[...]).astype(bf16)


def order_body(pos_ref, own_ref, other_ref, out_ref):
    core = pos_ref[0] % 2
    own, other = own_ref[...], other_ref[...]
    rows = own.shape[0]
    out_ref[0:rows, :] = jnp.where(core == 1, own, other)
    out_ref[rows:, :] = jnp.where(core == 1, other, own)


def attend_body(pos_ref, q_ref, near_ref, far_ref, far_other_ref, out_ref):
    here = pos_ref[0]
    core = here % 2
    rows = far_ref.shape[0]
    chips = 2 * rows // MSG
    odd = (here // 2) % 2
    q = q_ref[...]
    wide = (2 * BLOCK, 2 * BLOCK)
    row, col = iota(wide, 0), iota(wide, 1)
    row = jnp.where(row >= BLOCK, row - BLOCK, row)
    tail = ones_where((col >= BLOCK) | (row >= col)).astype(bf16)
    t, s = iota((BLOCK, BLOCK), 0), iota((BLOCK, BLOCK), 1)

    offset = s - t

    def step(k, carry):
        later, total = carry
        messages, starts = [], []
        for w in range(WIDTH):
            z = chips - 1 - (k * WIDTH + w)
            at = pl.multiple_of((z // 2) * MSG, 16)
            near = odd == (WIDTH - 1 - w) % 2
            far, other = far_ref[pl.ds(at, MSG), :], far_other_ref[pl.ds(at, MSG), :]
            upper = jnp.where(core == 1, far, other)
            lower = jnp.where(core == 1, other, far)
            messages.append(jnp.where(near, near_ref[pl.ds(at, MSG), :], upper))
            messages.append(jnp.where(near, near_ref[pl.ds(rows + at, MSG), :], lower))
            starts += [(here - 2 * z - 1) * BLOCK, (here - 2 * z) * BLOCK]
        scores = [nn(q, m[0:HEAD, :]) + m[BLOCK : BLOCK + 1, :].astype(f32) for m in messages]
        causal = [offset < start for start in starts]
        logs = [jnp.log(1.0 + jnp.exp(-jnp.abs(x))) for x in scores]
        keep = [-(jnp.maximum(x, 0.0) + y) for x, y in zip(scores, logs)]
        keep = [jnp.where(c, x, 0.0) for c, x in zip(causal, keep)]
        high = [x.astype(bf16) for x in keep]
        low = [(x - y.astype(f32)).astype(bf16) for x, y in zip(keep, high)]
        sums = [nn(jnp.concatenate([x, y], axis=1), tail) for x, y in zip(high, low)]
        weights = [jnp.exp(x + y[:, :BLOCK]) for x, y in zip(scores, sums)]
        weights = [jnp.where(c, x, 0.0).astype(bf16) for c, x in zip(causal, weights)]
        outs = [nt(x, m[HEAD:BLOCK, :]) for x, m in zip(weights, messages)]
        for x, y in zip(outs, sums):
            total = total + jnp.exp(later) * x
            later = later + y[:, BLOCK : BLOCK + HEAD]
        return later, total

    zeros = jnp.zeros((BLOCK, HEAD), f32)
    _, total = lax.fori_loop(0, chips // WIDTH, step, (zeros, zeros))
    out_ref[...] = jnp.transpose(total).astype(bf16)


def pack_body(*refs):
    for k, ref in enumerate(refs[:-1]):
        refs[-1][k * HEAD : (k + 1) * HEAD, :] = ref[...]


def mix_body(tp_ref, x0_ref, x1_ref, x2_ref, x3_ref, w_ref, out_ref):
    line, column = tp_ref[0] // 4, tp_ref[0] % 4
    weights, pieces = [], []
    for d, x_ref in zip(OFFSETS, (x0_ref, x1_ref, x2_ref, x3_ref)):
        pieces.append(x_ref[...])
        for e in OFFSETS:
            head = (line + d) % 4 * 4 + (column + e) % 4
            weights.append(w_ref[pl.ds(pl.multiple_of(head * HEAD, HEAD), HEAD), :])
    x = jnp.transpose(jnp.concatenate(pieces, axis=0).astype(f32)).astype(bf16)
    out_ref[...] = nn(x, jnp.concatenate(weights, axis=0)).astype(bf16)


def plan_body(ids_ref, group_ref, pair_ref, pick_ref, table_ref):
    ids = ids_ref[...]
    first, second = ids[0:1, :], ids[1:2, :]
    place0, place1 = places(first, second)
    shares = jnp.exp(group_ref[...])
    shares = shares / jnp.sum(shares, axis=0, keepdims=True)
    group = iota((GROUPS, BLOCK), 0)
    chosen0 = jnp.sum(jnp.where(first // GROUP_SIZE == group, shares, 0.0), axis=0, keepdims=True)
    chosen1 = jnp.sum(jnp.where(second // GROUP_SIZE == group, shares, 0.0), axis=0, keepdims=True)
    spread = pair_ref[0:1, :] - pair_ref[1:2, :]
    weight0 = chosen0 * jax.nn.sigmoid(spread)
    weight1 = chosen1 * jax.nn.sigmoid(-spread)
    slots = [(first * CAP + place0).astype(f32), (second * CAP + place1).astype(f32)]
    table = jnp.concatenate(slots + [weight0, weight1], axis=0)
    table = jnp.concatenate([table, jnp.zeros((BLOCK - 4, BLOCK), f32)], axis=0)
    table = jnp.transpose(table)
    slot = iota((BLOCK, SLOTS), 1)
    for k in range(2):
        hit = ones_where(slot == table[:, k : k + 1].astype(i32))
        pick_ref[k * BLOCK : (k + 1) * BLOCK, :] = hit.astype(bf16)
    table_ref[...] = table


def combine_body(pick_ref, table_ref, back_ref, out_ref):
    both = nn(pick_ref[...], back_ref[...])
    out = table_ref[:, 2:3] * both[:BLOCK] + table_ref[:, 3:4] * both[BLOCK:]
    out_ref[...] = out.astype(bf16)


def shards(
    attn_rows,
    attn_gain,
    query_weight,
    key_weight,
    value_weight,
    key_bias,
    out_weight,
    expert_rows,
    expert_gain,
    expert_ids,
    group_logits,
    pair_logits,
    gate_weight,
    up_weight,
    down_weight,
):
    ep, tp = lax.axis_size("ep"), lax.axis_size("tp")
    chips = ep // 2
    here = lax.axis_index("ep")
    run = chips // 4
    strided = [[(m + 4 * k) * 2 + c for k in range(run)] for m in range(4) for c in range(2)]
    pairs = [[(z + 2 * b) * 2 + c for b in range(2)] for z in range(chips) if z % 4 < 2 for c in range(2)]
    row_moves = [[(k - k % 4 + (k + d) % 4, k) for k in range(tp)] for d in range(4)]
    column_moves = [[((k + 4 * d) % tp, k) for k in range(tp)] for d in range(4)]
    struct = jax.ShapeDtypeStruct

    def exchange(x, axis):
        return lax.all_to_all(x, axis, split_axis=0, concat_axis=0, tiled=True)

    slots = struct((SLOTS, BLOCK), bf16)
    copies = struct((tp, SLOTS, BLOCK), bf16)
    square = struct((BLOCK, BLOCK), bf16)
    ids = expert_ids.T
    column = lax.axis_index("tp").reshape(1)

    scratch = [pltpu.VMEM((BLOCK, expert_rows.shape[1]), bf16), pltpu.SemaphoreType.DMA((PARTS,))]
    more = {"own": 0, "scratch_shapes": scratch}
    send = call(dispatch_body, 1, 3, slots, 1 << 27, hbm=(1, 2, 3), **more)(
        column, expert_rows, expert_gain[None, :], ids
    )
    routed = exchange(send.reshape(ep, CAP, BLOCK), "ep").reshape(SLOTS, BLOCK)
    outs = (struct((BLOCK, HEAD), bf16), struct((MSG, BLOCK), bf16))
    query, message = call(project_body, 0, 6, outs, 1 << 28, hbm=range(6))(
        attn_rows,
        attn_gain[None, :],
        query_weight.T,
        key_weight.T,
        value_weight.T,
        key_bias,
    )
    swaps = [(k, k ^ 1) for k in range(tp)]
    other_gate = lax.ppermute(gate_weight[0], "tp", swaps)
    other_up = lax.ppermute(up_weight[0], "tp", swaps)
    keys = lax.all_gather(message, "ep", axis=0, tiled=True, axis_index_groups=pairs)
    own = lax.all_gather(keys, "ep", axis=0, tiled=True, axis_index_groups=strided)
    far = lax.ppermute(own, "ep", [(e, e ^ 2) for e in range(ep)])
    routed = call_out(halves_body, 0, 1, struct((tp, ROWS, BLOCK), bf16), 1 << 24, [], tp)(routed)
    routed = exchange(routed, "tp")
    own_hidden = [pltpu.VMEM((SLOTS, BLOCK), bf16)]
    hidden = call_out(hidden_body, 0, 5, copies, 1 << 29, own_hidden, 2 * tp)(
        routed, gate_weight[0], up_weight[0], other_gate, other_up
    )
    hidden = exchange(hidden, "tp")
    cores = [(e, e ^ 1) for e in range(ep)]
    own_other = lax.ppermute(own, "ep", cores)
    ordered = struct((2 * own.shape[0], BLOCK), bf16)
    near = call(order_body, 1, 2, ordered, 1 << 22)(here.reshape(1), own, own_other)
    far_other = lax.ppermute(far, "ep", cores)
    attended = call(attend_body, 1, 4, struct((HEAD, BLOCK), bf16), 1 << 30)(
        here.reshape(1), query, near, far, far_other
    )
    heads = [attended]
    for d in OFFSETS[1:3]:
        heads.append(lax.ppermute(attended, "tp", row_moves[d]))
    heads.append(lax.ppermute(attended, "tp", row_moves[OFFSETS[3]]))
    stacked = struct((len(heads) * HEAD, BLOCK), bf16)
    attended = call(pack_body, 0, len(heads), stacked, 1 << 20)(*heads)
    result = call(down_body, 0, 2, slots, 1 << 28)(hidden, down_weight[0])
    back = exchange(result.reshape(ep, CAP, BLOCK), "ep").reshape(SLOTS, BLOCK)
    tables = (struct((2 * BLOCK, SLOTS), bf16), struct((BLOCK, BLOCK), f32))
    picks, table = call(plan_body, 0, 3, tables, 1 << 26)(ids, group_logits.T, pair_logits.T)
    stacks = [attended]
    for d in OFFSETS[1:]:
        stacks.append(lax.ppermute(attended, "tp", column_moves[d]))
    mixed = call(mix_body, 1, 5, square, 1 << 26)(column, *stacks, out_weight)
    expert_out = call(combine_body, 0, 3, square, 1 << 27)(picks, table, back)
    return (mixed, expert_out)


def solution(mesh):
    placed = (
        P("ep", None),
        P(),
        P(None, "tp"),
        P(None, "tp"),
        P(None, "tp"),
        P("tp", "ep"),
        P(None, "tp"),
        P("ep", None),
        P(),
        P("ep", None),
        P("ep", None),
        P("ep", None),
        P("ep", None, "tp"),
        P("ep", None, "tp"),
        P("ep", None, "tp"),
    )
    return jax.shard_map(
        shards,
        mesh=mesh,
        in_specs=placed,
        out_specs=(P("ep", "tp"), P("ep", "tp")),
        check_vma=False,
    )
```

```python
import jax
import jax.numpy as jnp
from jax import lax
from jax.experimental import pallas as pl
from jax.experimental.pallas import tpu as pltpu
from jax.sharding import PartitionSpec as P


EXPERTS = 32
GROUPS = 4
GROUP_SIZE = 8
CAP = 16
BLOCK = 128
HEAD = 64
SLOTS = EXPERTS * CAP
ROWS = SLOTS // 2
MSG = 144
WIDTH = 4

epsilon = 1e-06
f32 = jnp.float32
bf16 = jnp.bfloat16
i32 = jnp.int32

SMEM = pl.BlockSpec(memory_space=pltpu.SMEM)


def call(body, n_scalar, n_in, outs, flops, mib=16, hbm=(), **more):
    def run(*args):
        args = [
            pltpu.with_memory_space_constraint(a, pltpu.HBM) if k in hbm else a
            for k, a in enumerate(args)
        ]
        return kernel(*args)

    kernel = pl.pallas_call(
        body,
        out_shape=outs,
        in_specs=[SMEM] * n_scalar + [pl.BlockSpec()] * n_in,
        cost_estimate=pl.CostEstimate(flops=flops, bytes_accessed=1 << 20, transcendentals=0),
        compiler_params=pltpu.CompilerParams(vmem_limit_bytes=mib << 20),
        **more,
    )
    return run


def call_out(body, n_scalar, n_in, out, flops, scratch, copies):
    copies = [pltpu.SemaphoreType.DMA((copies,))]
    more = {"out_specs": pl.BlockSpec(memory_space=pltpu.HBM), "scratch_shapes": scratch + copies}
    return call(body, n_scalar, n_in, pltpu.HBM(out.shape, out.dtype), flops, **more)


def nn(a, b):
    return lax.dot_general(a, b, (((1,), (0,)), ((), ())), preferred_element_type=f32)


def nt(a, b):
    return lax.dot_general(a, b, (((1,), (1,)), ((), ())), preferred_element_type=f32)


def iota(shape, dim):
    return lax.broadcasted_iota(i32, shape, dim)


def ones_where(mask):
    return jnp.where(mask, 1.0, 0.0).astype(f32)


def places(first, second):
    expert = iota((EXPERTS, BLOCK), 0)
    mark0 = ones_where(first == expert)
    mark1 = ones_where(second == expert)
    earlier = ones_where(iota((BLOCK, BLOCK), 0) < iota((BLOCK, BLOCK), 1)).astype(bf16)
    before = nn((mark0 + mark1).astype(bf16), earlier)
    place0 = jnp.sum(mark0 * before, axis=0, keepdims=True)
    place1 = jnp.sum(mark1 * before, axis=0, keepdims=True)
    return place0.astype(i32), place1.astype(i32)


def dispatch_body(tp_ref, rows_ref, gain_ref, ids_ref, out_ref):
    x = rows_ref[...].astype(f32)
    inv = lax.rsqrt(jnp.mean(x * x, axis=-1, keepdims=True) + epsilon)
    at = pl.multiple_of(tp_ref[0] * BLOCK, BLOCK)
    own = rows_ref[:, pl.ds(at, BLOCK)].astype(f32)
    own = (own * inv * gain_ref[:, pl.ds(at, BLOCK)]).astype(bf16)
    ids = ids_ref[...]
    first, second = ids[0:1, :], ids[1:2, :]
    place0, place1 = places(first, second)
    slot = iota((SLOTS, BLOCK), 0)
    hit = (slot == first * CAP + place0) | (slot == second * CAP + place1)
    out_ref[...] = nn(ones_where(hit).astype(bf16), own).astype(bf16)


def project_body(rows_ref, gain_ref, wq_ref, wk_ref, wv_ref, bias_ref, q_ref, msg_ref):
    x = rows_ref[...].astype(f32)
    inv = lax.rsqrt(jnp.mean(x * x, axis=-1, keepdims=True) + epsilon)
    normed = (x * inv * gain_ref[...]).astype(bf16)
    q = nt(normed, wq_ref[...]).astype(bf16)
    q_ref[...] = (q.astype(f32) * (HEAD**-0.5)).astype(bf16)
    kv = jnp.concatenate([wk_ref[...], wv_ref[...]], axis=0)
    msg_ref[0:BLOCK, :] = nt(kv, normed).astype(bf16)
    msg_ref[BLOCK:MSG, :] = jnp.broadcast_to(bias_ref[...], (MSG - BLOCK, BLOCK))


def halves_body(x_ref, out_ref, sems):
    copies = []
    for k in range(out_ref.shape[0]):
        half = k % 2
        source = x_ref.at[half * ROWS : (half + 1) * ROWS, :]
        copies.append(pltpu.make_async_copy(source, out_ref.at[k], sems.at[k]))
        copies[-1].start()
    for copy in copies:
        copy.wait()


def hidden_body(tp_ref, x_ref, g0_ref, u0_ref, g1_ref, u1_ref, out_ref, hidden_ref, sems):
    parts = x_ref.shape[0]
    even = tp_ref[0] % 2 == 0
    own_weights = jnp.concatenate([g0_ref[...], u0_ref[...]], axis=1)
    other_weights = jnp.concatenate([g1_ref[...], u1_ref[...]], axis=1)

    def gated(both):
        gate, up = both[:, :BLOCK], both[:, BLOCK:]
        return gate * jax.nn.sigmoid(gate) * up

    copies = []
    for m in range(2):
        x = [x_ref[k, m * BLOCK : (m + 1) * BLOCK, :] for k in range(parts)]
        x = jnp.concatenate(x, axis=1)
        own, other = gated(nn(x, own_weights)), gated(nn(x, other_weights))
        span = slice(m * ROWS, (m + 1) * ROWS)
        hidden_ref[m * ROWS : m * ROWS + BLOCK, :] = jnp.where(even, own, other).astype(bf16)
        hidden_ref[m * ROWS + BLOCK : (m + 1) * ROWS, :] = jnp.where(even, other, own).astype(bf16)
        for k in range(parts):
            target = out_ref.at[k, span, :]
            copies.append(
                pltpu.make_async_copy(hidden_ref.at[span, :], target, sems.at[m * parts + k])
            )
            copies[-1].start()
    for copy in copies:
        copy.wait()


def down_body(x_ref, w_ref, out_ref):
    parts = x_ref.shape[0]
    rows = []
    for half in range(2):
        for m in range(2):
            at = m * ROWS
            pieces = [
                x_ref[k, at + e * BLOCK : at + (e + 1) * BLOCK, :]
                for k in range(half, parts, 2)
                for e in range(2)
            ]
            rows.append(jnp.concatenate(pieces, axis=1))
    out_ref[...] = nn(jnp.concatenate(rows, axis=0), w_ref[...]).astype(bf16)


def order_body(pos_ref, own_ref, other_ref, out_ref):
    core = pos_ref[0] % 2
    own, other = own_ref[...], other_ref[...]
    rows = own.shape[0]
    out_ref[0:rows, :] = jnp.where(core == 1, own, other)
    out_ref[rows:, :] = jnp.where(core == 1, other, own)


def attend_body(pos_ref, q_ref, near_ref, far_ref, far_other_ref, out_ref):
    here = pos_ref[0]
    core = here % 2
    rows = far_ref.shape[0]
    chips = 2 * rows // MSG
    odd = (here // 2) % 2
    q = q_ref[...]
    wide = (2 * BLOCK, 2 * BLOCK)
    row, col = iota(wide, 0), iota(wide, 1)
    row = jnp.where(row >= BLOCK, row - BLOCK, row)
    tail = ones_where((col >= BLOCK) | (row >= col)).astype(bf16)
    t, s = iota((BLOCK, BLOCK), 0), iota((BLOCK, BLOCK), 1)

    offset = s - t

    def step(k, carry):
        later, total = carry
        messages, starts = [], []
        for w in range(WIDTH):
            z = chips - 1 - (k * WIDTH + w)
            at = pl.multiple_of((z // 2) * MSG, 16)
            near = odd == (WIDTH - 1 - w) % 2
            far, other = far_ref[pl.ds(at, MSG), :], far_other_ref[pl.ds(at, MSG), :]
            upper = jnp.where(core == 1, far, other)
            lower = jnp.where(core == 1, other, far)
            messages.append(jnp.where(near, near_ref[pl.ds(at, MSG), :], upper))
            messages.append(jnp.where(near, near_ref[pl.ds(rows + at, MSG), :], lower))
            starts += [(here - 2 * z - 1) * BLOCK, (here - 2 * z) * BLOCK]
        scores = [nn(q, m[0:HEAD, :]) + m[BLOCK : BLOCK + 1, :].astype(f32) for m in messages]
        causal = [offset < start for start in starts]
        logs = [jnp.log(1.0 + jnp.exp(-jnp.abs(x))) for x in scores]
        keep = [-(jnp.maximum(x, 0.0) + y) for x, y in zip(scores, logs)]
        keep = [jnp.where(c, x, 0.0) for c, x in zip(causal, keep)]
        high = [x.astype(bf16) for x in keep]
        low = [(x - y.astype(f32)).astype(bf16) for x, y in zip(keep, high)]
        sums = [nn(jnp.concatenate([x, y], axis=1), tail) for x, y in zip(high, low)]
        weights = [jnp.exp(x + y[:, :BLOCK]) for x, y in zip(scores, sums)]
        weights = [jnp.where(c, x, 0.0).astype(bf16) for c, x in zip(causal, weights)]
        outs = [nt(x, m[HEAD:BLOCK, :]) for x, m in zip(weights, messages)]
        for x, y in zip(outs, sums):
            total = total + jnp.exp(later) * x
            later = later + y[:, BLOCK : BLOCK + HEAD]
        return later, total

    zeros = jnp.zeros((BLOCK, HEAD), f32)
    _, total = lax.fori_loop(0, chips // WIDTH, step, (zeros, zeros))
    out_ref[...] = jnp.transpose(total).astype(bf16)


def pack_body(*refs):
    for k, ref in enumerate(refs[:-1]):
        refs[-1][k * HEAD : (k + 1) * HEAD, :] = ref[...]


def mix_body(tp_ref, x_ref, w_ref, out_ref):
    column = tp_ref[0] % 4
    weights = []
    for k in range(x_ref.shape[0] // HEAD):
        head = k - k % 4 + jnp.bitwise_xor(column, k % 4)
        weights.append(w_ref[pl.ds(pl.multiple_of(head * HEAD, HEAD), HEAD), :])
    x = jnp.transpose(x_ref[...].astype(f32)).astype(bf16)
    out_ref[...] = nn(x, jnp.concatenate(weights, axis=0)).astype(bf16)


def plan_body(ids_ref, group_ref, pair_ref, pick_ref, table_ref):
    ids = ids_ref[...]
    first, second = ids[0:1, :], ids[1:2, :]
    place0, place1 = places(first, second)
    shares = jnp.exp(group_ref[...])
    shares = shares / jnp.sum(shares, axis=0, keepdims=True)
    group = iota((GROUPS, BLOCK), 0)
    chosen0 = jnp.sum(jnp.where(first // GROUP_SIZE == group, shares, 0.0), axis=0, keepdims=True)
    chosen1 = jnp.sum(jnp.where(second // GROUP_SIZE == group, shares, 0.0), axis=0, keepdims=True)
    spread = pair_ref[0:1, :] - pair_ref[1:2, :]
    weight0 = chosen0 * jax.nn.sigmoid(spread)
    weight1 = chosen1 * jax.nn.sigmoid(-spread)
    slots = [(first * CAP + place0).astype(f32), (second * CAP + place1).astype(f32)]
    table = jnp.concatenate(slots + [weight0, weight1], axis=0)
    table = jnp.concatenate([table, jnp.zeros((BLOCK - 4, BLOCK), f32)], axis=0)
    table = jnp.transpose(table)
    slot = iota((BLOCK, SLOTS), 1)
    for k in range(2):
        hit = ones_where(slot == table[:, k : k + 1].astype(i32))
        pick_ref[k * BLOCK : (k + 1) * BLOCK, :] = hit.astype(bf16)
    table_ref[...] = table


def combine_body(pick_ref, table_ref, back_ref, out_ref):
    both = nn(pick_ref[...], back_ref[...])
    out = table_ref[:, 2:3] * both[:BLOCK] + table_ref[:, 3:4] * both[BLOCK:]
    out_ref[...] = out.astype(bf16)


def shards(
    attn_rows,
    attn_gain,
    query_weight,
    key_weight,
    value_weight,
    key_bias,
    out_weight,
    expert_rows,
    expert_gain,
    expert_ids,
    group_logits,
    pair_logits,
    gate_weight,
    up_weight,
    down_weight,
):
    ep, tp = lax.axis_size("ep"), lax.axis_size("tp")
    chips = ep // 2
    here = lax.axis_index("ep")
    run = chips // 4
    strided = [[(m + 4 * k) * 2 + c for k in range(run)] for m in range(4) for c in range(2)]
    pairs = [[(z + 2 * b) * 2 + c for b in range(2)] for z in range(chips) if z % 4 < 2 for c in range(2)]
    side = tp // 4
    along_y = [[y * 4 + x for y in range(side)] for x in range(4)]
    struct = jax.ShapeDtypeStruct

    def exchange(x, axis):
        return lax.all_to_all(x, axis, split_axis=0, concat_axis=0, tiled=True)

    slots = struct((SLOTS, BLOCK), bf16)
    copies = struct((tp, SLOTS, BLOCK), bf16)
    square = struct((BLOCK, BLOCK), bf16)
    ids = expert_ids.T
    column = lax.axis_index("tp").reshape(1)

    send = call(dispatch_body, 1, 3, slots, 1 << 27, hbm=(1, 2, 3))(
        column, expert_rows, expert_gain[None, :], ids
    )
    routed = exchange(send.reshape(ep, CAP, BLOCK), "ep").reshape(SLOTS, BLOCK)
    outs = (struct((BLOCK, HEAD), bf16), struct((MSG, BLOCK), bf16))
    query, message = call(project_body, 0, 6, outs, 1 << 28, hbm=range(6))(
        attn_rows,
        attn_gain[None, :],
        query_weight.T,
        key_weight.T,
        value_weight.T,
        key_bias,
    )
    swaps = [(k, k ^ 1) for k in range(tp)]
    other_gate = lax.ppermute(gate_weight[0], "tp", swaps)
    other_up = lax.ppermute(up_weight[0], "tp", swaps)
    keys = lax.all_gather(message, "ep", axis=0, tiled=True, axis_index_groups=pairs)
    own = lax.all_gather(keys, "ep", axis=0, tiled=True, axis_index_groups=strided)
    far = lax.ppermute(own, "ep", [(e, e ^ 2) for e in range(ep)])
    routed = call_out(halves_body, 0, 1, struct((tp, ROWS, BLOCK), bf16), 1 << 24, [], tp)(routed)
    routed = exchange(routed, "tp")
    own_hidden = [pltpu.VMEM((SLOTS, BLOCK), bf16)]
    hidden = call_out(hidden_body, 1, 5, copies, 1 << 29, own_hidden, 2 * tp)(
        column, routed, gate_weight[0], up_weight[0], other_gate, other_up
    )
    hidden = exchange(hidden, "tp")
    cores = [(e, e ^ 1) for e in range(ep)]
    own_other = lax.ppermute(own, "ep", cores)
    ordered = struct((2 * own.shape[0], BLOCK), bf16)
    near = call(order_body, 1, 2, ordered, 1 << 22)(here.reshape(1), own, own_other)
    far_other = lax.ppermute(far, "ep", cores)
    attended = call(attend_body, 1, 4, struct((HEAD, BLOCK), bf16), 1 << 30)(
        here.reshape(1), query, near, far, far_other
    )
    heads = [attended]
    for d in range(1, 4):
        heads.append(lax.ppermute(attended, "tp", [(k ^ d, k) for k in range(tp)]))
    stacked = struct((len(heads) * HEAD, BLOCK), bf16)
    attended = call(pack_body, 0, len(heads), stacked, 1 << 20)(*heads)
    result = call(down_body, 0, 2, slots, 1 << 28)(hidden, down_weight[0])
    back = exchange(result.reshape(ep, CAP, BLOCK), "ep").reshape(SLOTS, BLOCK)
    tables = (struct((2 * BLOCK, SLOTS), bf16), struct((BLOCK, BLOCK), f32))
    picks, table = call(plan_body, 0, 3, tables, 1 << 26)(ids, group_logits.T, pair_logits.T)
    attended = lax.all_gather(attended, "tp", axis=0, tiled=True, axis_index_groups=along_y)
    mixed = call(mix_body, 1, 2, square, 1 << 26)(column, attended, out_weight)
    expert_out = call(combine_body, 0, 3, square, 1 << 27)(picks, table, back)
    return (mixed, expert_out)


def solution(mesh):
    placed = (
        P("ep", None),
        P(),
        P(None, "tp"),
        P(None, "tp"),
        P(None, "tp"),
        P("tp", "ep"),
        P(None, "tp"),
        P("ep", None),
        P(),
        P("ep", None),
        P("ep", None),
        P("ep", None),
        P("ep", None, "tp"),
        P("ep", None, "tp"),
        P("ep", None, "tp"),
    )
    return jax.shard_map(
        shards,
        mesh=mesh,
        in_specs=placed,
        out_specs=(P("ep", "tp"), P("ep", "tp")),
        check_vma=False,
    )
```

```python
import jax
import jax.numpy as jnp
from jax import lax
from jax.experimental import pallas as pl
from jax.experimental.pallas import tpu as pltpu
from jax.sharding import PartitionSpec as P


EXPERTS = 32
GROUPS = 4
GROUP_SIZE = 8
CAP = 16
BLOCK = 128
HEAD = 64
SLOTS = EXPERTS * CAP
ROWS = SLOTS // 2
MSG = 144
WIDTH = 4

epsilon = 1e-06
f32 = jnp.float32
bf16 = jnp.bfloat16
i32 = jnp.int32

SMEM = pl.BlockSpec(memory_space=pltpu.SMEM)


def call(body, n_scalar, n_in, outs, flops, mib=16, hbm=(), **more):
    def run(*args):
        args = [
            pltpu.with_memory_space_constraint(a, pltpu.HBM) if k in hbm else a
            for k, a in enumerate(args)
        ]
        return kernel(*args)

    kernel = pl.pallas_call(
        body,
        out_shape=outs,
        in_specs=[SMEM] * n_scalar + [pl.BlockSpec()] * n_in,
        cost_estimate=pl.CostEstimate(flops=flops, bytes_accessed=1 << 20, transcendentals=0),
        compiler_params=pltpu.CompilerParams(vmem_limit_bytes=mib << 20),
        **more,
    )
    return run


def call_out(body, n_scalar, n_in, out, flops, scratch, copies):
    copies = [pltpu.SemaphoreType.DMA((copies,))]
    more = {"out_specs": pl.BlockSpec(memory_space=pltpu.HBM), "scratch_shapes": scratch + copies}
    return call(body, n_scalar, n_in, pltpu.HBM(out.shape, out.dtype), flops, **more)


def nn(a, b):
    return lax.dot_general(a, b, (((1,), (0,)), ((), ())), preferred_element_type=f32)


def nt(a, b):
    return lax.dot_general(a, b, (((1,), (1,)), ((), ())), preferred_element_type=f32)


def iota(shape, dim):
    return lax.broadcasted_iota(i32, shape, dim)


def ones_where(mask):
    return jnp.where(mask, 1.0, 0.0).astype(f32)


def places(first, second):
    expert = iota((EXPERTS, BLOCK), 0)
    mark0 = ones_where(first == expert)
    mark1 = ones_where(second == expert)
    earlier = ones_where(iota((BLOCK, BLOCK), 0) < iota((BLOCK, BLOCK), 1)).astype(bf16)
    before = nn((mark0 + mark1).astype(bf16), earlier)
    place0 = jnp.sum(mark0 * before, axis=0, keepdims=True)
    place1 = jnp.sum(mark1 * before, axis=0, keepdims=True)
    return place0.astype(i32), place1.astype(i32)


def dispatch_body(tp_ref, rows_ref, gain_ref, ids_ref, out_ref):
    x = rows_ref[...].astype(f32)
    inv = lax.rsqrt(jnp.mean(x * x, axis=-1, keepdims=True) + epsilon)
    at = pl.multiple_of(tp_ref[0] * BLOCK, BLOCK)
    own = rows_ref[:, pl.ds(at, BLOCK)].astype(f32)
    own = (own * inv * gain_ref[:, pl.ds(at, BLOCK)]).astype(bf16)
    ids = ids_ref[...]
    first, second = ids[0:1, :], ids[1:2, :]
    place0, place1 = places(first, second)
    slot = iota((SLOTS, BLOCK), 0)
    hit = (slot == first * CAP + place0) | (slot == second * CAP + place1)
    out_ref[...] = nn(ones_where(hit).astype(bf16), own).astype(bf16)


def project_body(rows_ref, gain_ref, wq_ref, wk_ref, wv_ref, bias_ref, q_ref, msg_ref):
    x = rows_ref[...].astype(f32)
    inv = lax.rsqrt(jnp.mean(x * x, axis=-1, keepdims=True) + epsilon)
    normed = (x * inv * gain_ref[...]).astype(bf16)
    q = nt(normed, wq_ref[...]).astype(bf16)
    q_ref[...] = (q.astype(f32) * (HEAD**-0.5)).astype(bf16)
    kv = jnp.concatenate([wk_ref[...], wv_ref[...]], axis=0)
    msg_ref[0:BLOCK, :] = nt(kv, normed).astype(bf16)
    msg_ref[BLOCK:MSG, :] = jnp.broadcast_to(bias_ref[...], (MSG - BLOCK, BLOCK))


def halves_body(x_ref, out_ref, sems):
    copies = []
    for k in range(out_ref.shape[0]):
        half = k % 2
        source = x_ref.at[half * ROWS : (half + 1) * ROWS, :]
        copies.append(pltpu.make_async_copy(source, out_ref.at[k], sems.at[k]))
        copies[-1].start()
    for copy in copies:
        copy.wait()


def hidden_body(tp_ref, x_ref, g0_ref, u0_ref, g1_ref, u1_ref, out_ref, hidden_ref, sems):
    parts = x_ref.shape[0]
    even = tp_ref[0] % 2 == 0
    own_weights = jnp.concatenate([g0_ref[...], u0_ref[...]], axis=1)
    other_weights = jnp.concatenate([g1_ref[...], u1_ref[...]], axis=1)

    def gated(both):
        gate, up = both[:, :BLOCK], both[:, BLOCK:]
        return gate * jax.nn.sigmoid(gate) * up

    copies = []
    for m in range(2):
        x = [x_ref[k, m * BLOCK : (m + 1) * BLOCK, :] for k in range(parts)]
        x = jnp.concatenate(x, axis=1)
        own, other = gated(nn(x, own_weights)), gated(nn(x, other_weights))
        span = slice(m * ROWS, (m + 1) * ROWS)
        hidden_ref[m * ROWS : m * ROWS + BLOCK, :] = jnp.where(even, own, other).astype(bf16)
        hidden_ref[m * ROWS + BLOCK : (m + 1) * ROWS, :] = jnp.where(even, other, own).astype(bf16)
        for k in range(parts):
            target = out_ref.at[k, span, :]
            copies.append(
                pltpu.make_async_copy(hidden_ref.at[span, :], target, sems.at[m * parts + k])
            )
            copies[-1].start()
    for copy in copies:
        copy.wait()


def down_body(x_ref, w_ref, out_ref):
    parts = x_ref.shape[0]
    rows = []
    for half in range(2):
        for m in range(2):
            at = m * ROWS
            pieces = [
                x_ref[k, at + e * BLOCK : at + (e + 1) * BLOCK, :]
                for k in range(half, parts, 2)
                for e in range(2)
            ]
            rows.append(jnp.concatenate(pieces, axis=1))
    out_ref[...] = nn(jnp.concatenate(rows, axis=0), w_ref[...]).astype(bf16)


def order_body(pos_ref, own_ref, other_ref, out_ref):
    core = pos_ref[0] % 2
    own, other = own_ref[...], other_ref[...]
    rows = own.shape[0]
    out_ref[0:rows, :] = jnp.where(core == 1, own, other)
    out_ref[rows:, :] = jnp.where(core == 1, other, own)


def attend_body(pos_ref, q_ref, near_ref, far_ref, far_other_ref, out_ref):
    here = pos_ref[0]
    core = here % 2
    rows = far_ref.shape[0]
    chips = 2 * rows // MSG
    odd = (here // 2) % 2
    q = q_ref[...]
    wide = (2 * BLOCK, 2 * BLOCK)
    row, col = iota(wide, 0), iota(wide, 1)
    row = jnp.where(row >= BLOCK, row - BLOCK, row)
    tail = ones_where((col >= BLOCK) | (row >= col)).astype(bf16)
    t, s = iota((BLOCK, BLOCK), 0), iota((BLOCK, BLOCK), 1)

    offset = s - t

    def step(k, carry):
        later, total = carry
        messages, starts = [], []
        for w in range(WIDTH):
            z = chips - 1 - (k * WIDTH + w)
            at = pl.multiple_of((z // 2) * MSG, 16)
            near = odd == (WIDTH - 1 - w) % 2
            far, other = far_ref[pl.ds(at, MSG), :], far_other_ref[pl.ds(at, MSG), :]
            upper = jnp.where(core == 1, far, other)
            lower = jnp.where(core == 1, other, far)
            messages.append(jnp.where(near, near_ref[pl.ds(at, MSG), :], upper))
            messages.append(jnp.where(near, near_ref[pl.ds(rows + at, MSG), :], lower))
            starts += [(here - 2 * z - 1) * BLOCK, (here - 2 * z) * BLOCK]
        scores = [nn(q, m[0:HEAD, :]) + m[BLOCK : BLOCK + 1, :].astype(f32) for m in messages]
        causal = [offset < start for start in starts]
        logs = [jnp.log(1.0 + jnp.exp(-jnp.abs(x))) for x in scores]
        keep = [-(jnp.maximum(x, 0.0) + y) for x, y in zip(scores, logs)]
        keep = [jnp.where(c, x, 0.0) for c, x in zip(causal, keep)]
        high = [x.astype(bf16) for x in keep]
        low = [(x - y.astype(f32)).astype(bf16) for x, y in zip(keep, high)]
        sums = [nn(jnp.concatenate([x, y], axis=1), tail) for x, y in zip(high, low)]
        weights = [jnp.exp(x + y[:, :BLOCK]) for x, y in zip(scores, sums)]
        weights = [jnp.where(c, x, 0.0).astype(bf16) for c, x in zip(causal, weights)]
        outs = [nt(x, m[HEAD:BLOCK, :]) for x, m in zip(weights, messages)]
        for x, y in zip(outs, sums):
            total = total + jnp.exp(later) * x
            later = later + y[:, BLOCK : BLOCK + HEAD]
        return later, total

    zeros = jnp.zeros((BLOCK, HEAD), f32)
    _, total = lax.fori_loop(0, chips // WIDTH, step, (zeros, zeros))
    out_ref[...] = jnp.transpose(total).astype(bf16)


def pack_body(*refs):
    for k, ref in enumerate(refs[:-1]):
        refs[-1][k * HEAD : (k + 1) * HEAD, :] = ref[...]


def mix_body(tp_ref, x_ref, w_ref, out_ref):
    column = tp_ref[0] % 4
    weights = []
    for k in range(x_ref.shape[0] // HEAD):
        head = k - k % 4 + jnp.bitwise_xor(column, k % 4)
        weights.append(w_ref[pl.ds(pl.multiple_of(head * HEAD, HEAD), HEAD), :])
    x = jnp.transpose(x_ref[...].astype(f32)).astype(bf16)
    out_ref[...] = nn(x, jnp.concatenate(weights, axis=0)).astype(bf16)


def plan_body(ids_ref, group_ref, pair_ref, pick_ref, table_ref):
    ids = ids_ref[...]
    first, second = ids[0:1, :], ids[1:2, :]
    place0, place1 = places(first, second)
    shares = jnp.exp(group_ref[...])
    shares = shares / jnp.sum(shares, axis=0, keepdims=True)
    group = iota((GROUPS, BLOCK), 0)
    chosen0 = jnp.sum(jnp.where(first // GROUP_SIZE == group, shares, 0.0), axis=0, keepdims=True)
    chosen1 = jnp.sum(jnp.where(second // GROUP_SIZE == group, shares, 0.0), axis=0, keepdims=True)
    spread = pair_ref[0:1, :] - pair_ref[1:2, :]
    weight0 = chosen0 * jax.nn.sigmoid(spread)
    weight1 = chosen1 * jax.nn.sigmoid(-spread)
    slots = [(first * CAP + place0).astype(f32), (second * CAP + place1).astype(f32)]
    table = jnp.concatenate(slots + [weight0, weight1], axis=0)
    table = jnp.concatenate([table, jnp.zeros((BLOCK - 4, BLOCK), f32)], axis=0)
    table = jnp.transpose(table)
    slot = iota((BLOCK, SLOTS), 1)
    for k in range(2):
        hit = ones_where(slot == table[:, k : k + 1].astype(i32))
        pick_ref[k * BLOCK : (k + 1) * BLOCK, :] = hit.astype(bf16)
    table_ref[...] = table


def combine_body(pick_ref, table_ref, back_ref, out_ref):
    both = nn(pick_ref[...], back_ref[...])
    out = table_ref[:, 2:3] * both[:BLOCK] + table_ref[:, 3:4] * both[BLOCK:]
    out_ref[...] = out.astype(bf16)


def shards(
    attn_rows,
    attn_gain,
    query_weight,
    key_weight,
    value_weight,
    key_bias,
    out_weight,
    expert_rows,
    expert_gain,
    expert_ids,
    group_logits,
    pair_logits,
    gate_weight,
    up_weight,
    down_weight,
):
    ep, tp = lax.axis_size("ep"), lax.axis_size("tp")
    chips = ep // 2
    here = lax.axis_index("ep")
    run = chips // 4
    strided = [[(m + 4 * k) * 2 + c for k in range(run)] for m in range(4) for c in range(2)]
    pairs = [[(z + 2 * b) * 2 + c for b in range(2)] for z in range(chips) if z % 4 < 2 for c in range(2)]
    side = tp // 4
    along_y = [[y * 4 + x for y in range(side)] for x in range(4)]
    struct = jax.ShapeDtypeStruct

    def exchange(x, axis):
        return lax.all_to_all(x, axis, split_axis=0, concat_axis=0, tiled=True)

    slots = struct((SLOTS, BLOCK), bf16)
    copies = struct((tp, SLOTS, BLOCK), bf16)
    square = struct((BLOCK, BLOCK), bf16)
    ids = expert_ids.T
    column = lax.axis_index("tp").reshape(1)

    send = call(dispatch_body, 1, 3, slots, 1 << 27, hbm=(1, 2, 3))(
        column, expert_rows, expert_gain[None, :], ids
    )
    routed = exchange(send.reshape(ep, CAP, BLOCK), "ep").reshape(SLOTS, BLOCK)
    outs = (struct((BLOCK, HEAD), bf16), struct((MSG, BLOCK), bf16))
    query, message = call(project_body, 0, 6, outs, 1 << 28, hbm=range(6))(
        attn_rows,
        attn_gain[None, :],
        query_weight.T,
        key_weight.T,
        value_weight.T,
        key_bias,
    )
    swaps = [(k, k ^ 1) for k in range(tp)]
    other_gate = lax.ppermute(gate_weight[0], "tp", swaps)
    other_up = lax.ppermute(up_weight[0], "tp", swaps)
    keys = lax.all_gather(message, "ep", axis=0, tiled=True, axis_index_groups=pairs)
    own = lax.all_gather(keys, "ep", axis=0, tiled=True, axis_index_groups=strided)
    far = lax.ppermute(own, "ep", [(e, e ^ 2) for e in range(ep)])
    routed = call_out(halves_body, 0, 1, struct((tp, ROWS, BLOCK), bf16), 1 << 24, [], tp)(routed)
    routed = exchange(routed, "tp")
    own_hidden = [pltpu.VMEM((SLOTS, BLOCK), bf16)]
    hidden = call_out(hidden_body, 1, 5, copies, 1 << 29, own_hidden, 2 * tp)(
        column, routed, gate_weight[0], up_weight[0], other_gate, other_up
    )
    hidden = exchange(hidden, "tp")
    cores = [(e, e ^ 1) for e in range(ep)]
    own_other = lax.ppermute(own, "ep", cores)
    ordered = struct((2 * own.shape[0], BLOCK), bf16)
    near = call(order_body, 1, 2, ordered, 1 << 22)(here.reshape(1), own, own_other)
    far_other = lax.ppermute(far, "ep", cores)
    attended = call(attend_body, 1, 4, struct((HEAD, BLOCK), bf16), 1 << 30)(
        here.reshape(1), query, near, far, far_other
    )
    far_heads = [lax.ppermute(attended, "tp", [(k ^ d, k) for k in range(tp)]) for d in range(2, 4)]
    heads = [attended, lax.ppermute(attended, "tp", [(k ^ 1, k) for k in range(tp)]), *far_heads]
    stacked = struct((len(heads) * HEAD, BLOCK), bf16)
    attended = call(pack_body, 0, len(heads), stacked, 1 << 20)(*heads)
    result = call(down_body, 0, 2, slots, 1 << 28)(hidden, down_weight[0])
    back = exchange(result.reshape(ep, CAP, BLOCK), "ep").reshape(SLOTS, BLOCK)
    tables = (struct((2 * BLOCK, SLOTS), bf16), struct((BLOCK, BLOCK), f32))
    picks, table = call(plan_body, 0, 3, tables, 1 << 26)(ids, group_logits.T, pair_logits.T)
    attended = lax.all_gather(attended, "tp", axis=0, tiled=True, axis_index_groups=along_y)
    mixed = call(mix_body, 1, 2, square, 1 << 26)(column, attended, out_weight)
    expert_out = call(combine_body, 0, 3, square, 1 << 27)(picks, table, back)
    return (mixed, expert_out)


def solution(mesh):
    placed = (
        P("ep", None),
        P(),
        P(None, "tp"),
        P(None, "tp"),
        P(None, "tp"),
        P("tp", "ep"),
        P(None, "tp"),
        P("ep", None),
        P(),
        P("ep", None),
        P("ep", None),
        P("ep", None),
        P("ep", None, "tp"),
        P("ep", None, "tp"),
        P("ep", None, "tp"),
    )
    return jax.shard_map(
        shards,
        mesh=mesh,
        in_specs=placed,
        out_specs=(P("ep", "tp"), P("ep", "tp")),
        check_vma=False,
    )
```

```python
import jax
import jax.numpy as jnp
from jax import lax
from jax.experimental import pallas as pl
from jax.experimental.pallas import tpu as pltpu
from jax.sharding import PartitionSpec as P


EXPERTS = 32
GROUPS = 4
GROUP_SIZE = 8
CAP = 16
BLOCK = 128
HEAD = 64
SLOTS = EXPERTS * CAP
ROWS = SLOTS // 2
MSG = 144
PAIR = 272
WIDTH = 4

epsilon = 1e-06
f32 = jnp.float32
bf16 = jnp.bfloat16
i32 = jnp.int32

SMEM = pl.BlockSpec(memory_space=pltpu.SMEM)


def call(body, n_scalar, n_in, outs, flops, mib=16, hbm=(), **more):
    def run(*args):
        args = [
            pltpu.with_memory_space_constraint(a, pltpu.HBM) if k in hbm else a
            for k, a in enumerate(args)
        ]
        return kernel(*args)

    kernel = pl.pallas_call(
        body,
        out_shape=outs,
        in_specs=[SMEM] * n_scalar + [pl.BlockSpec()] * n_in,
        cost_estimate=pl.CostEstimate(flops=flops, bytes_accessed=1 << 20, transcendentals=0),
        compiler_params=pltpu.CompilerParams(vmem_limit_bytes=mib << 20),
        **more,
    )
    return run


def call_out(body, n_scalar, n_in, out, flops, scratch, copies):
    copies = [pltpu.SemaphoreType.DMA((copies,))]
    more = {"out_specs": pl.BlockSpec(memory_space=pltpu.HBM), "scratch_shapes": scratch + copies}
    return call(body, n_scalar, n_in, pltpu.HBM(out.shape, out.dtype), flops, **more)


def nn(a, b):
    return lax.dot_general(a, b, (((1,), (0,)), ((), ())), preferred_element_type=f32)


def nt(a, b):
    return lax.dot_general(a, b, (((1,), (1,)), ((), ())), preferred_element_type=f32)


def iota(shape, dim):
    return lax.broadcasted_iota(i32, shape, dim)


def ones_where(mask):
    return jnp.where(mask, 1.0, 0.0).astype(f32)


def places(first, second):
    expert = iota((EXPERTS, BLOCK), 0)
    mark0 = ones_where(first == expert)
    mark1 = ones_where(second == expert)
    earlier = ones_where(iota((BLOCK, BLOCK), 0) < iota((BLOCK, BLOCK), 1)).astype(bf16)
    before = nn((mark0 + mark1).astype(bf16), earlier)
    place0 = jnp.sum(mark0 * before, axis=0, keepdims=True)
    place1 = jnp.sum(mark1 * before, axis=0, keepdims=True)
    return place0.astype(i32), place1.astype(i32)


def dispatch_body(tp_ref, rows_ref, gain_ref, ids_ref, out_ref):
    x = rows_ref[...].astype(f32)
    inv = lax.rsqrt(jnp.mean(x * x, axis=-1, keepdims=True) + epsilon)
    at = pl.multiple_of(tp_ref[0] * BLOCK, BLOCK)
    own = rows_ref[:, pl.ds(at, BLOCK)].astype(f32)
    own = (own * inv * gain_ref[:, pl.ds(at, BLOCK)]).astype(bf16)
    ids = ids_ref[...]
    first, second = ids[0:1, :], ids[1:2, :]
    place0, place1 = places(first, second)
    slot = iota((SLOTS, BLOCK), 0)
    hit = (slot == first * CAP + place0) | (slot == second * CAP + place1)
    out_ref[...] = nn(ones_where(hit).astype(bf16), own).astype(bf16)


def project_body(rows_ref, gain_ref, wq_ref, wk_ref, wv_ref, bias_ref, q_ref, msg_ref):
    x = rows_ref[...].astype(f32)
    inv = lax.rsqrt(jnp.mean(x * x, axis=-1, keepdims=True) + epsilon)
    normed = (x * inv * gain_ref[...]).astype(bf16)
    q = nt(normed, wq_ref[...]).astype(bf16)
    q_ref[...] = (q.astype(f32) * (HEAD**-0.5)).astype(bf16)
    kv = jnp.concatenate([wk_ref[...], wv_ref[...]], axis=0)
    msg_ref[0:BLOCK, :] = nt(kv, normed).astype(bf16)
    msg_ref[BLOCK:MSG, :] = jnp.broadcast_to(bias_ref[...], (MSG - BLOCK, BLOCK))


def halves_body(x_ref, out_ref, sems):
    copies = []
    for k in range(out_ref.shape[0]):
        half = k % 2
        source = x_ref.at[half * ROWS : (half + 1) * ROWS, :]
        copies.append(pltpu.make_async_copy(source, out_ref.at[k], sems.at[k]))
        copies[-1].start()
    for copy in copies:
        copy.wait()


def hidden_body(tp_ref, x_ref, g0_ref, u0_ref, g1_ref, u1_ref, out_ref, hidden_ref, sems):
    parts = x_ref.shape[0]
    even = tp_ref[0] % 2 == 0
    own_weights = jnp.concatenate([g0_ref[...], u0_ref[...]], axis=1)
    other_weights = jnp.concatenate([g1_ref[...], u1_ref[...]], axis=1)

    def gated(both):
        gate, up = both[:, :BLOCK], both[:, BLOCK:]
        return gate * jax.nn.sigmoid(gate) * up

    copies = []
    for m in range(2):
        x = [x_ref[k, m * BLOCK : (m + 1) * BLOCK, :] for k in range(parts)]
        x = jnp.concatenate(x, axis=1)
        own, other = gated(nn(x, own_weights)), gated(nn(x, other_weights))
        span = slice(m * ROWS, (m + 1) * ROWS)
        hidden_ref[m * ROWS : m * ROWS + BLOCK, :] = jnp.where(even, own, other).astype(bf16)
        hidden_ref[m * ROWS + BLOCK : (m + 1) * ROWS, :] = jnp.where(even, other, own).astype(bf16)
        for k in range(parts):
            target = out_ref.at[k, span, :]
            copies.append(
                pltpu.make_async_copy(hidden_ref.at[span, :], target, sems.at[m * parts + k])
            )
            copies[-1].start()
    for copy in copies:
        copy.wait()


def down_body(x_ref, w_ref, out_ref):
    parts = x_ref.shape[0]
    rows = []
    for half in range(2):
        for m in range(2):
            at = m * ROWS
            pieces = [
                x_ref[k, at + e * BLOCK : at + (e + 1) * BLOCK, :]
                for k in range(half, parts, 2)
                for e in range(2)
            ]
            rows.append(jnp.concatenate(pieces, axis=1))
    out_ref[...] = nn(jnp.concatenate(rows, axis=0), w_ref[...]).astype(bf16)


def trim_body(x_ref, out_ref):
    for b in range(2):
        out_ref[b * BLOCK : (b + 1) * BLOCK, :] = x_ref[b * MSG : b * MSG + BLOCK, :]
    bias = [x_ref[b * MSG + BLOCK : (b + 1) * MSG, :] for b in range(2)]
    first = iota((16, BLOCK), 0) < 8
    out_ref[2 * BLOCK : PAIR, :] = jnp.where(first, bias[0], bias[1])


def order_body(pos_ref, own_ref, other_ref, out_ref):
    core = pos_ref[0] % 2
    own, other = own_ref[...], other_ref[...]
    rows = own.shape[0]
    out_ref[0:rows, :] = jnp.where(core == 1, own, other)
    out_ref[rows:, :] = jnp.where(core == 1, other, own)


def attend_body(pos_ref, q_ref, near_ref, far_ref, far_other_ref, out_ref):
    here = pos_ref[0]
    core = here % 2
    rows = far_ref.shape[0]
    chips = 4 * rows // PAIR
    odd = (here // 2) % 2
    q = q_ref[...]
    wide = (2 * BLOCK, 2 * BLOCK)
    row, col = iota(wide, 0), iota(wide, 1)
    row = jnp.where(row >= BLOCK, row - BLOCK, row)
    tail = ones_where((col >= BLOCK) | (row >= col)).astype(bf16)
    t, s = iota((BLOCK, BLOCK), 0), iota((BLOCK, BLOCK), 1)

    offset = s - t

    def step(k, carry):
        later, total = carry
        messages, biases, starts = [], [], []
        for w in range(WIDTH):
            z = chips - 1 - (k * WIDTH + w)
            base = (z // 4) * PAIR
            which = (WIDTH - 1 - w) // 2
            near = odd == (WIDTH - 1 - w) % 2

            def piece(at, size):
                at = pl.multiple_of(base + at, 16)
                far, other = far_ref[pl.ds(at, size), :], far_other_ref[pl.ds(at, size), :]
                upper = jnp.where(core == 1, far, other)
                lower = jnp.where(core == 1, other, far)
                upper = jnp.where(near, near_ref[pl.ds(at, size), :], upper)
                return upper, jnp.where(near, near_ref[pl.ds(rows + at, size), :], lower)

            messages += piece(which * BLOCK, BLOCK)
            biases += [x[which * 8 : which * 8 + 1, :] for x in piece(2 * BLOCK, 16)]
            starts += [(here - 2 * z - 1) * BLOCK, (here - 2 * z) * BLOCK]
        scores = [nn(q, m[0:HEAD, :]) + x.astype(f32) for m, x in zip(messages, biases)]
        causal = [offset < start for start in starts]
        logs = [jnp.log(1.0 + jnp.exp(-jnp.abs(x))) for x in scores]
        keep = [-(jnp.maximum(x, 0.0) + y) for x, y in zip(scores, logs)]
        keep = [jnp.where(c, x, 0.0) for c, x in zip(causal, keep)]
        high = [x.astype(bf16) for x in keep]
        low = [(x - y.astype(f32)).astype(bf16) for x, y in zip(keep, high)]
        sums = [nn(jnp.concatenate([x, y], axis=1), tail) for x, y in zip(high, low)]
        weights = [jnp.exp(x + y[:, :BLOCK]) for x, y in zip(scores, sums)]
        weights = [jnp.where(c, x, 0.0).astype(bf16) for c, x in zip(causal, weights)]
        outs = [nt(x, m[HEAD:BLOCK, :]) for x, m in zip(weights, messages)]
        for x, y in zip(outs, sums):
            total = total + jnp.exp(later) * x
            later = later + y[:, BLOCK : BLOCK + HEAD]
        return later, total

    zeros = jnp.zeros((BLOCK, HEAD), f32)
    _, total = lax.fori_loop(0, chips // WIDTH, step, (zeros, zeros))
    out_ref[...] = jnp.transpose(total).astype(bf16)


def pack_body(*refs):
    for k, ref in enumerate(refs[:-1]):
        refs[-1][k * HEAD : (k + 1) * HEAD, :] = ref[...]


def mix_body(tp_ref, x_ref, w_ref, out_ref):
    column = tp_ref[0] % 4
    weights = []
    for k in range(x_ref.shape[0] // HEAD):
        head = k - k % 4 + jnp.bitwise_xor(column, k % 4)
        weights.append(w_ref[pl.ds(pl.multiple_of(head * HEAD, HEAD), HEAD), :])
    x = jnp.transpose(x_ref[...].astype(f32)).astype(bf16)
    out_ref[...] = nn(x, jnp.concatenate(weights, axis=0)).astype(bf16)


def plan_body(ids_ref, group_ref, pair_ref, pick_ref, table_ref):
    ids = ids_ref[...]
    first, second = ids[0:1, :], ids[1:2, :]
    place0, place1 = places(first, second)
    shares = jnp.exp(group_ref[...])
    shares = shares / jnp.sum(shares, axis=0, keepdims=True)
    group = iota((GROUPS, BLOCK), 0)
    chosen0 = jnp.sum(jnp.where(first // GROUP_SIZE == group, shares, 0.0), axis=0, keepdims=True)
    chosen1 = jnp.sum(jnp.where(second // GROUP_SIZE == group, shares, 0.0), axis=0, keepdims=True)
    spread = pair_ref[0:1, :] - pair_ref[1:2, :]
    weight0 = chosen0 * jax.nn.sigmoid(spread)
    weight1 = chosen1 * jax.nn.sigmoid(-spread)
    slots = [(first * CAP + place0).astype(f32), (second * CAP + place1).astype(f32)]
    table = jnp.concatenate(slots + [weight0, weight1], axis=0)
    table = jnp.concatenate([table, jnp.zeros((BLOCK - 4, BLOCK), f32)], axis=0)
    table = jnp.transpose(table)
    slot = iota((BLOCK, SLOTS), 1)
    for k in range(2):
        hit = ones_where(slot == table[:, k : k + 1].astype(i32))
        pick_ref[k * BLOCK : (k + 1) * BLOCK, :] = hit.astype(bf16)
    table_ref[...] = table


def combine_body(pick_ref, table_ref, back_ref, out_ref):
    both = nn(pick_ref[...], back_ref[...])
    out = table_ref[:, 2:3] * both[:BLOCK] + table_ref[:, 3:4] * both[BLOCK:]
    out_ref[...] = out.astype(bf16)


def shards(
    attn_rows,
    attn_gain,
    query_weight,
    key_weight,
    value_weight,
    key_bias,
    out_weight,
    expert_rows,
    expert_gain,
    expert_ids,
    group_logits,
    pair_logits,
    gate_weight,
    up_weight,
    down_weight,
):
    ep, tp = lax.axis_size("ep"), lax.axis_size("tp")
    chips = ep // 2
    here = lax.axis_index("ep")
    run = chips // 4
    strided = [[(m + 4 * k) * 2 + c for k in range(run)] for m in range(4) for c in range(2)]
    pairs = [[(z + 2 * b) * 2 + c for b in range(2)] for z in range(chips) if z % 4 < 2 for c in range(2)]
    side = tp // 4
    along_y = [[y * 4 + x for y in range(side)] for x in range(4)]
    struct = jax.ShapeDtypeStruct

    def exchange(x, axis):
        return lax.all_to_all(x, axis, split_axis=0, concat_axis=0, tiled=True)

    slots = struct((SLOTS, BLOCK), bf16)
    copies = struct((tp, SLOTS, BLOCK), bf16)
    square = struct((BLOCK, BLOCK), bf16)
    ids = expert_ids.T
    column = lax.axis_index("tp").reshape(1)

    send = call(dispatch_body, 1, 3, slots, 1 << 27, hbm=(1, 2, 3))(
        column, expert_rows, expert_gain[None, :], ids
    )
    routed = exchange(send.reshape(ep, CAP, BLOCK), "ep").reshape(SLOTS, BLOCK)
    outs = (struct((BLOCK, HEAD), bf16), struct((MSG, BLOCK), bf16))
    query, message = call(project_body, 0, 6, outs, 1 << 28, hbm=range(6))(
        attn_rows,
        attn_gain[None, :],
        query_weight.T,
        key_weight.T,
        value_weight.T,
        key_bias,
    )
    swaps = [(k, k ^ 1) for k in range(tp)]
    other_gate = lax.ppermute(gate_weight[0], "tp", swaps)
    other_up = lax.ppermute(up_weight[0], "tp", swaps)
    keys = lax.all_gather(message, "ep", axis=0, tiled=True, axis_index_groups=pairs)
    keys = call(trim_body, 0, 1, struct((PAIR, BLOCK), bf16), 1 << 20)(keys)
    own = lax.all_gather(keys, "ep", axis=0, tiled=True, axis_index_groups=strided)
    far = lax.ppermute(own, "ep", [(e, e ^ 2) for e in range(ep)])
    routed = call_out(halves_body, 0, 1, struct((tp, ROWS, BLOCK), bf16), 1 << 24, [], tp)(routed)
    routed = exchange(routed, "tp")
    own_hidden = [pltpu.VMEM((SLOTS, BLOCK), bf16)]
    hidden = call_out(hidden_body, 1, 5, copies, 1 << 29, own_hidden, 2 * tp)(
        column, routed, gate_weight[0], up_weight[0], other_gate, other_up
    )
    hidden = exchange(hidden, "tp")
    cores = [(e, e ^ 1) for e in range(ep)]
    own_other = lax.ppermute(own, "ep", cores)
    ordered = struct((2 * own.shape[0], BLOCK), bf16)
    near = call(order_body, 1, 2, ordered, 1 << 22)(here.reshape(1), own, own_other)
    far_other = lax.ppermute(far, "ep", cores)
    attended = call(attend_body, 1, 4, struct((HEAD, BLOCK), bf16), 1 << 30)(
        here.reshape(1), query, near, far, far_other
    )
    heads = [attended]
    for d in range(1, 4):
        heads.append(lax.ppermute(attended, "tp", [(k ^ d, k) for k in range(tp)]))
    stacked = struct((len(heads) * HEAD, BLOCK), bf16)
    attended = call(pack_body, 0, len(heads), stacked, 1 << 20)(*heads)
    result = call(down_body, 0, 2, slots, 1 << 28)(hidden, down_weight[0])
    back = exchange(result.reshape(ep, CAP, BLOCK), "ep").reshape(SLOTS, BLOCK)
    tables = (struct((2 * BLOCK, SLOTS), bf16), struct((BLOCK, BLOCK), f32))
    picks, table = call(plan_body, 0, 3, tables, 1 << 26)(ids, group_logits.T, pair_logits.T)
    attended = lax.all_gather(attended, "tp", axis=0, tiled=True, axis_index_groups=along_y)
    mixed = call(mix_body, 1, 2, square, 1 << 26)(column, attended, out_weight)
    expert_out = call(combine_body, 0, 3, square, 1 << 27)(picks, table, back)
    return (mixed, expert_out)


def solution(mesh):
    placed = (
        P("ep", None),
        P(),
        P(None, "tp"),
        P(None, "tp"),
        P(None, "tp"),
        P("tp", "ep"),
        P(None, "tp"),
        P("ep", None),
        P(),
        P("ep", None),
        P("ep", None),
        P("ep", None),
        P("ep", None, "tp"),
        P("ep", None, "tp"),
        P("ep", None, "tp"),
    )
    return jax.shard_map(
        shards,
        mesh=mesh,
        in_specs=placed,
        out_specs=(P("ep", "tp"), P("ep", "tp")),
        check_vma=False,
    )
```
